32 devices in a mesh: fs: 16 (over z, y, x), tp: 2 (over core).
Axes of the slice: x: 2, y: 2, z: 4, core: 2. Of those that a mesh axis runs over, the one named last changes fastest.
Arguments:
- tokens: bfloat16 [4096, 2048], P('fs', 'tp'), may hold values from -6 to 6
- mixer_norm_gain: bfloat16 [2048], replicated, may hold values from 0.099609375 to 1.8984375
- recurrence_branch_weight: bfloat16 [2048, 1024], P('fs', 'tp'), may hold values from -0.125 to 0.125
- output_gate_projection: bfloat16 [2048, 1024], P('fs', 'tp'), may hold values from -0.125 to 0.125
- recurrence_conv_taps: bfloat16 [4, 1024], P(None, 'tp'), may hold values from -3 to 3
- recurrence_gate_map: bfloat16 [16, 64, 64], P('tp'), may hold values from -0.75 to 0.75
- input_gate_map: bfloat16 [16, 64, 64], P('tp'), may hold values from -0.75 to 0.75
- channel_decay_rate: float32 [1024], P('tp'), may hold values from 0.001 to 0.03
- position_log_decay: float32 [4096, 1024], P('fs', 'tp'), may hold values from -0.69 to 0
- mixer_output_weight: bfloat16 [1024, 2048], P('tp', 'fs'), may hold values from -0.75 to 0.75
- feedforward_norm_gain: bfloat16 [2048], replicated, may hold values from 0.099609375 to 1.8984375
- gate_up_weight: bfloat16 [2048, 5632], P('fs', 'tp'), may hold values from -0.125 to 0.125
- value_up_weight: bfloat16 [2048, 5632], P('fs', 'tp'), may hold values from -0.125 to 0.125
- gate_conv_taps: bfloat16 [3, 5632], P(None, 'tp'), may hold values from -3 to 3
- value_conv_taps: bfloat16 [3, 5632], P(None, 'tp'), may hold values from -3 to 3
- down_projection_weight: bfloat16 [5632, 2048], P('tp', 'fs'), may hold values from -0.15625 to 0.15625
Outputs:
- result: bfloat16 [4096, 2048], P('fs', 'tp')
The draws below stay inside these ranges and needn't reach their ends.
All inputs are finite; a program needn't handle non-finite values.
Results may differ from the reference program's by a relative error of at most 0.024.
Values may be sent and summed in bfloat16 or wider, within the bound.
A program may use at most 128 MiB of HBM per device.

```python
import math
import jax
import jax.numpy as jnp
from jax import lax

D = 2048
HEADS = 16
HEAD_DIM = 64
W = 1024
FF = 5632
SEQ_LEN = 64
TOKENS = 4096
N_TP = 2


def draw_channel_decay_rate(key, part):
    base = jax.random.fold_in(key, 17)
    key_pick, key_slow, key_fast = jax.random.split(base, 3)
    limit = 5
    picked = jax.random.randint(key_pick, (W,), 0, 10) < limit
    slow_rate = jnp.exp(jax.random.uniform(key_slow, (W,), jnp.float32, math.log(0.001), math.log(0.004)))
    fast_rate = jnp.exp(jax.random.uniform(key_fast, (W,), jnp.float32, math.log(0.012), math.log(0.03)))
    return jnp.where(picked, slow_rate, fast_rate).astype(jnp.float32)


def draw_position_log_decay(key, part):
    base = jax.random.fold_in(key, 29)
    key_marks, key_depth = jax.random.split(base, 2)
    marks = (jax.random.randint(key_marks, (TOKENS, 1), 0, 32) == 0).astype(jnp.float32)
    depth = jax.random.uniform(key_depth, (TOKENS, W), jnp.float32, 0.22, 0.69)
    return (-marks * depth).astype(jnp.float32)


def steps_of(rng, extent, pieces, low, top_value):
    level, own = 1.0, jax.random.fold_in(rng, 6)
    for position, parts in pieces:
        steps = jnp.exp(jax.random.uniform(jax.random.fold_in(own, position), (parts,), jnp.float32, low / len(pieces), top_value / len(pieces)))
        level = level * jnp.repeat(steps, extent[position] // parts).reshape([-1 if axis == position else 1 for axis in range(len(extent))])
    return level


def normal_values(stream_key, extent, scale, most, shards=(), dtype=jnp.bfloat16):
    drawn = jax.random.normal(stream_key, extent, jnp.float32) * scale
    if len(shards) > 0:
        drawn = steps_of(stream_key, extent, shards, -0.22, 0.18) * drawn
    return jnp.clip(drawn, min=-most, max=most).astype(dtype)


def setup_inputs(seed: int = 0) -> dict:
    key_list = jax.random.split(jax.random.key(seed), 17)
    tokens = normal_values(key_list[0], (TOKENS, D), 1.0, 6.0, ((0, 16), (1, 2)))
    mixer_norm_gain = jnp.clip(1.0 + 0.18 * jax.random.normal(key_list[1], (D,), jnp.float32), 0.099609375, 1.8984375).astype(jnp.bfloat16)
    recurrence_branch_weight = normal_values(key_list[2], (D, W), D ** -0.5, 0.125, ((0, 16), (1, 2)))
    output_gate_projection = normal_values(key_list[3], (D, W), D ** -0.5, 0.125, ((0, 16), (1, 2)))
    recurrence_conv_taps = normal_values(key_list[4], (4, W), 0.5, 3.0, ((1, 2),))
    recurrence_gate_map = normal_values(key_list[5], (HEADS, HEAD_DIM, HEAD_DIM), HEAD_DIM ** -0.5, 0.75, ((0, 2),))
    input_gate_map = normal_values(key_list[6], (HEADS, HEAD_DIM, HEAD_DIM), HEAD_DIM ** -0.5, 0.75, ((0, 2),))
    channel_decay_rate = draw_channel_decay_rate(jax.random.fold_in(key_list[16], 71), 0)
    position_log_decay = draw_position_log_decay(jax.random.fold_in(key_list[16], 71), 0)
    mixer_output_weight = normal_values(key_list[9], (W, D), (W // 16) ** -0.5, 0.75, ((0, 2), (1, 16)))
    feedforward_norm_gain = jnp.clip(1.0 + 0.18 * jax.random.normal(key_list[10], (D,), jnp.float32), 0.099609375, 1.8984375).astype(jnp.bfloat16)
    gate_up_weight = normal_values(key_list[11], (D, FF), D ** -0.5, 0.125, ((0, 16), (1, 2)))
    value_up_weight = normal_values(key_list[12], (D, FF), D ** -0.5, 0.125, ((0, 16), (1, 2)))
    gate_conv_taps = normal_values(key_list[13], (3, FF), 0.6, 3.0, ((1, 2),))
    value_conv_taps = normal_values(key_list[14], (3, FF), 0.6, 3.0, ((1, 2),))
    down_projection_weight = normal_values(key_list[15], (FF, D), (FF // 4) ** -0.5, 0.15625, ((0, 2), (1, 16)))
    return {"tokens": tokens, "mixer_norm_gain": mixer_norm_gain, "recurrence_branch_weight": recurrence_branch_weight, "output_gate_projection": output_gate_projection, "recurrence_conv_taps": recurrence_conv_taps, "recurrence_gate_map": recurrence_gate_map, "input_gate_map": input_gate_map, "channel_decay_rate": channel_decay_rate, "position_log_decay": position_log_decay, "mixer_output_weight": mixer_output_weight, "feedforward_norm_gain": feedforward_norm_gain, "gate_up_weight": gate_up_weight, "value_up_weight": value_up_weight, "gate_conv_taps": gate_conv_taps, "value_conv_taps": value_conv_taps, "down_projection_weight": down_projection_weight}


EPS = 1e-06
DECAY_RATE_GAIN = 8.0

def rms_normed(values, gain):
    wide = values.astype(jnp.float32)
    factor = lax.rsqrt(lax.optimization_barrier(jnp.mean(wide * wide, axis=-1, keepdims=True)) + EPS)
    return (wide * factor * gain.astype(jnp.float32)).astype(jnp.bfloat16)

def causal_conv(values, kernel):
    width = kernel.shape[0]
    row_count, channels = values.shape
    grouped = values.astype(jnp.float32).reshape(row_count // SEQ_LEN, SEQ_LEN, channels)
    padded = jnp.pad(grouped, ((0, 0), (width - 1, 0), (0, 0)))
    summed = padded[:, 0:SEQ_LEN] * kernel[0].astype(jnp.float32)
    for offset in range(1, width):
        summed = summed + padded[:, offset:offset + SEQ_LEN] * kernel[offset].astype(jnp.float32)
    return summed.reshape(row_count, channels)

def combine(left, right):
    first_a, first_b = left
    second_a, second_b = right
    return (first_a * second_a, second_a * first_b + second_b)

def block_sums(left, weight, blocks):
    width = left.shape[1] // blocks
    summed = jnp.zeros((left.shape[0], weight.shape[1]), jnp.float32)
    for index in range(blocks):
        partial_sum = jnp.dot(left[:, index * width:(index + 1) * width], weight[index * width:(index + 1) * width], preferred_element_type=jnp.float32)
        summed = summed + partial_sum.astype(jnp.bfloat16).astype(jnp.float32)
    return summed

def reference(tokens, mixer_norm_gain, recurrence_branch_weight, output_gate_projection, recurrence_conv_taps, recurrence_gate_map, input_gate_map, channel_decay_rate, position_log_decay, mixer_output_weight, feedforward_norm_gain, gate_up_weight, value_up_weight, gate_conv_taps, value_conv_taps, down_projection_weight):
    row_count = tokens.shape[0]
    normed = rms_normed(tokens, mixer_norm_gain)
    branch = jnp.dot(normed, recurrence_branch_weight, preferred_element_type=jnp.float32).astype(jnp.bfloat16)
    outgate = jnp.dot(normed, output_gate_projection, preferred_element_type=jnp.float32).astype(jnp.bfloat16)
    conv = causal_conv(branch, recurrence_conv_taps).astype(jnp.bfloat16)
    grouped = conv.astype(jnp.float32).reshape(row_count, HEADS, HEAD_DIM)
    recurrence_scan = jax.nn.sigmoid(jnp.einsum('rhi,hij->rhj', grouped, recurrence_gate_map.astype(jnp.float32)).reshape(row_count, W))
    inner = jax.nn.sigmoid(jnp.einsum('rhi,hij->rhj', grouped, input_gate_map.astype(jnp.float32)).reshape(row_count, W))
    log_alpha = -DECAY_RATE_GAIN * recurrence_scan * channel_decay_rate[None, :] + position_log_decay
    drive = jnp.sqrt(-jnp.expm1(2.0 * log_alpha)) * inner * conv.astype(jnp.float32)
    shape3 = (row_count // SEQ_LEN, SEQ_LEN, W)
    unused, state = lax.associative_scan(combine, (jnp.exp(log_alpha).reshape(shape3), drive.reshape(shape3)), axis=1)
    state = state.reshape(row_count, W)
    mixed = (state * jax.nn.gelu(outgate.astype(jnp.float32))).astype(jnp.bfloat16)
    after = (tokens.astype(jnp.float32) + block_sums(mixed, mixer_output_weight, N_TP)).astype(jnp.bfloat16)
    normed2 = rms_normed(after, feedforward_norm_gain)
    gate_half = jnp.dot(normed2, gate_up_weight, preferred_element_type=jnp.float32).astype(jnp.bfloat16)
    value_half = jnp.dot(normed2, value_up_weight, preferred_element_type=jnp.float32).astype(jnp.bfloat16)
    hidden = (jax.nn.silu(causal_conv(gate_half, gate_conv_taps)) * causal_conv(value_half, value_conv_taps)).astype(jnp.bfloat16)
    return (after.astype(jnp.float32) + block_sums(hidden, down_projection_weight, N_TP)).astype(jnp.bfloat16)
```

```python
import functools

import jax
import jax.numpy as jnp
from jax import lax
from jax.experimental import pallas as pl
from jax.experimental.pallas import tpu as pltpu
from jax.sharding import PartitionSpec as P

SEQ_LEN = 64


EPS = 1e-06
DECAY_RATE_GAIN = 8.0


def rms_normed(values, gain):
    wide = values.astype(jnp.float32)
    factor = lax.rsqrt(jnp.mean(wide * wide, axis=-1, keepdims=True) + EPS)
    return (wide * factor * gain.astype(jnp.float32)).astype(jnp.bfloat16)


def causal_conv(values, kernel):
    width = kernel.shape[0]
    row_count, channels = values.shape
    grouped = values.astype(jnp.float32).reshape(row_count // SEQ_LEN, SEQ_LEN, channels)
    padded = jnp.pad(grouped, ((0, 0), (width - 1, 0), (0, 0)))
    summed = padded[:, 0:SEQ_LEN] * kernel[0].astype(jnp.float32)
    for offset in range(1, width):
        summed = summed + padded[:, offset : offset + SEQ_LEN] * kernel[offset].astype(jnp.float32)
    return summed.reshape(row_count, channels)


def combine(left, right):
    first_a, first_b = left
    second_a, second_b = right
    return (first_a * second_a, second_a * first_b + second_b)


def pair_folder(normed, pieces):
    return (
        jnp.dot(normed, pieces[0], preferred_element_type=jnp.float32),
        jnp.dot(normed, pieces[1], preferred_element_type=jnp.float32),
    )


def gathered_layer(
    tokens,
    mixer_norm_gain,
    recurrence_branch_weight,
    output_gate_projection,
    recurrence_conv_taps,
    recurrence_gate_map,
    input_gate_map,
    channel_decay_rate,
    position_log_decay,
    mixer_output_weight,
    feedforward_norm_gain,
    gate_up_weight,
    value_up_weight,
    gate_conv_taps,
    value_conv_taps,
    down_projection_weight,
):
    row_count = tokens.shape[0]
    local_width = recurrence_branch_weight.shape[1]
    local_heads = recurrence_gate_map.shape[0]
    head_size = recurrence_gate_map.shape[1]
    whole_rows = lax.all_gather(tokens, "tp", axis=1, tiled=True)
    normed = rms_normed(whole_rows, mixer_norm_gain)
    branch_sum, outgate_sum = pair_folder(
        normed,
        (
            lax.all_gather(recurrence_branch_weight, "fs", axis=0, tiled=True),
            lax.all_gather(output_gate_projection, "fs", axis=0, tiled=True),
        ),
    )
    branch = branch_sum.astype(jnp.bfloat16)
    outgate = outgate_sum.astype(jnp.bfloat16)
    conv = causal_conv(branch, recurrence_conv_taps).astype(jnp.bfloat16)
    grouped = conv.reshape(row_count, local_heads, head_size)
    recurrence_scan = jax.nn.sigmoid(
        jnp.einsum(
            "rhi,hij->rhj", grouped, recurrence_gate_map, preferred_element_type=jnp.float32
        ).reshape(row_count, local_width)
    )
    inner = jax.nn.sigmoid(
        jnp.einsum(
            "rhi,hij->rhj", grouped, input_gate_map, preferred_element_type=jnp.float32
        ).reshape(row_count, local_width)
    )
    log_alpha = (
        -DECAY_RATE_GAIN * recurrence_scan * channel_decay_rate[None, :] + position_log_decay
    )
    drive = jnp.sqrt(-jnp.expm1(2.0 * log_alpha)) * inner * conv.astype(jnp.float32)
    shape3 = (row_count // SEQ_LEN, SEQ_LEN, local_width)
    unused, state = lax.associative_scan(
        combine, (jnp.exp(log_alpha).reshape(shape3), drive.reshape(shape3)), axis=1
    )
    state = state.reshape(row_count, local_width)
    mixed = (state * jax.nn.gelu(outgate.astype(jnp.float32))).astype(jnp.bfloat16)
    mixer_terms = jnp.dot(
        mixed,
        lax.all_gather(mixer_output_weight, "fs", axis=1, tiled=True),
        preferred_element_type=jnp.float32,
    )
    mixer_terms = mixer_terms.astype(jnp.bfloat16).astype(jnp.float32)
    mixer_whole = lax.psum(mixer_terms.astype(jnp.bfloat16), "tp").astype(jnp.float32)
    whole_after = (whole_rows.astype(jnp.float32) + mixer_whole).astype(jnp.bfloat16)
    normed2 = rms_normed(whole_after, feedforward_norm_gain)
    gate_whole, value_whole = (
        lax.all_gather(gate_up_weight, "fs", axis=0, tiled=True),
        lax.all_gather(value_up_weight, "fs", axis=0, tiled=True),
    )
    gate_sum = jnp.dot(normed2, gate_whole, preferred_element_type=jnp.float32)
    value_sum = jnp.dot(normed2, value_whole, preferred_element_type=jnp.float32)
    gate_half = gate_sum.astype(jnp.bfloat16)
    value_half = value_sum.astype(jnp.bfloat16)
    hidden = (
        jax.nn.silu(causal_conv(gate_half, gate_conv_taps))
        * causal_conv(value_half, value_conv_taps)
    ).astype(jnp.bfloat16)
    channel_terms = jnp.dot(
        hidden,
        lax.all_gather(down_projection_weight, "fs", axis=1, tiled=True),
        preferred_element_type=jnp.float32,
    )
    channel_terms = channel_terms.astype(jnp.bfloat16).astype(jnp.float32)
    channel_share = lax.psum_scatter(
        channel_terms.astype(jnp.bfloat16), "tp", scatter_dimension=1, tiled=True
    ).astype(jnp.float32)
    share_width = channel_share.shape[1]
    residual_share = lax.dynamic_slice_in_dim(
        whole_after, lax.axis_index("tp") * share_width, share_width, 1
    )
    return (residual_share.astype(jnp.float32) + channel_share).astype(jnp.bfloat16)


PLANE = 4
LAYERS = 4
LANES = 128
ANY = pl.BlockSpec(memory_space=pl.ANY)
VMEM = pl.BlockSpec(memory_space=pltpu.VMEM)
F32, BF16 = jnp.float32, jnp.bfloat16
N_SMALL, N_BIG = 3, 5


def hop(src, dst, send, recv, target):
    return pltpu.make_async_remote_copy(
        src_ref=src,
        dst_ref=dst,
        send_sem=send,
        recv_sem=recv,
        device_id=target,
        device_id_type=pl.DeviceIdType.MESH,
    )


def greet(targets):
    barrier = pltpu.get_barrier_semaphore()
    for target in targets:
        pl.semaphore_signal(
            barrier, inc=1, device_id=target, device_id_type=pl.DeviceIdType.MESH
        )
    pl.semaphore_wait(barrier, len(targets))


def span(index, size):
    return pl.ds(pl.multiple_of(index * size, size), size)


def row_blocks(whole, deep, columns):
    def at(f, part=None):
        if part is None:
            return whole.at[span(f, deep), columns]
        return whole.at[span(f * 2 + part, deep // 2), columns]

    return at


def column_blocks(whole, rows, wide):
    def at(f, part=None):
        if part is None:
            return whole.at[pl.ds(0, rows), span(f, wide)]
        return whole.at[pl.ds(part * (rows // 2), rows // 2), span(f, wide)]

    return at


def position(shape):
    return lax.broadcasted_iota(jnp.int32, shape, 0) % SEQ_LEN


def shifted(values, distance, place, fill):
    return jnp.where(place >= distance, pltpu.roll(values, distance, 0), fill)


def rows_conv(values, taps, width, place):
    summed = shifted(values, width - 1, place, 0.0) * taps[0:1, :]
    for j in range(1, width - 1):
        summed = summed + shifted(values, width - 1 - j, place, 0.0) * taps[j : j + 1, :]
    return summed + values * taps[width - 1 : width, :]


def negative_expm1(x):
    near = 1.0 + x * (1.0 / 8.0)
    for n in range(7, 1, -1):
        near = 1.0 + x * (1.0 / n) * near
    return jnp.where(jnp.abs(x) < 0.4, -x * near, 1.0 - jnp.exp(x))


def normed_rows(values, gain):
    factor = lax.rsqrt(jnp.mean(values * values, axis=-1, keepdims=True) + EPS)
    return (values * factor * gain).astype(BF16)


def gelu(x):
    return 0.5 * x * (1.0 + jnp.tanh(0.7978845608028654 * (x + 0.044715 * (x * x * x))))


def layer_kernel(
    tok, gain1, rb, og, ctaps, rmap, imap, rate, pld, mo, gain2, gup, vup, gtaps, vtaps, dn,
    out,
    whole_tok, bo_all, mo_all, gup_v, vup_v, stage, gu_all, dn_all, taps, gmap, pld_v,
    normed, mixed, mine, theirs, after, n2, hidden, give, keep, pair, paired, own_part, arrive,
    send, recv, z_send, local, tok_sem, swap_send, swap_recv, n2_send, n2_recv,
    core_send, core_recv, pair_send, pair_recv, back_send, back_recv,
):
    fs, tp = lax.axis_index("fs"), lax.axis_index("tp")
    z, p = fs // PLANE, fs % PLANE
    y, x = p // 2, p % 2
    px, py = y * 2 + 1 - x, (1 - y) * 2 + x
    inner = ((z + 1) // 2) % 2
    layer = (z, z + 1 - 2 * (z % 2), 2 - z // 2, 3 - 3 * (z // 2))
    lands = (0, 1, 3 - inner, 3 - inner)
    line = [(zz * PLANE + p, tp) for zz in layer]
    x_target, y_target = (z * PLANE + px, tp), (z * PLANE + py, tp)
    core_target = (fs, 1 - tp)
    greet(line[1:] + [x_target, y_target, core_target])

    rows, half = tok.shape
    deep, local_width = rb.shape
    wide = mo.shape[1]
    units = dn.shape[0] // LAYERS
    full, rest = units // LANES, units % LANES
    cw = gmap.shape[1]
    heads, head = rmap.shape[:2]
    per = cw // head

    arrays = (
        (row_blocks(bo_all, deep, pl.ds(0, local_width)), rb),
        (row_blocks(bo_all, deep, pl.ds(local_width, local_width)), og),
        (column_blocks(mo_all, mo.shape[0], wide), mo),
        (row_blocks(gu_all, deep, slice(None)), None),
        (column_blocks(dn_all, units, wide), None),
    )

    def piece(a, zz):
        if a < N_SMALL:
            return arrays[a][1]
        return stage.at[zz] if a == 3 else dn.at[span(zz, units), :]

    pending = []
    inner_pending = []

    copy = hop(tok, whole_tok.at[:, span(tp, half)], tok_sem.at[0], tok_sem.at[1], core_target)
    copy.start()
    tok_copy = copy

    def z_hop(a, source, f, slot, land, to):
        return hop(source, arrays[a][0](f), z_send.at[a, slot], recv.at[a, 0, land], line[to])

    def sides(a, k):
        at = arrays[a][0]
        f = layer[k] * PLANE + p
        source = piece(a, z) if k == 0 else at(f)
        for kind, target in ((1, x_target), (2, y_target)):
            c = hop(source, at(f), send.at[a, kind, k], recv.at[a, kind, k], target)
            c.start()
            pending.append(c)

    def corners(a, k):
        at = arrays[a][0]
        base = layer[k] * PLANE
        for kind, part, owner, target in ((1, 0, px, y_target), (2, 1, py, x_target)):
            whole = at(base + owner)
            hop(whole, whole, send.at[a, kind, k], recv.at[a, kind, k], target).wait_recv()
            block = at(base + owner, part)
            c = hop(block, block, send.at[a, kind + 2, k], recv.at[a, kind + 2, k], target)
            c.start()
            pending.append(c)

    def corners_done(a, k):
        at = arrays[a][0]
        corner = layer[k] * PLANE + (PLANE - 1 - p)
        for kind, part, target in ((1, 0, y_target), (2, 1, x_target)):
            block = at(corner, part)
            hop(block, block, send.at[a, kind + 2, k], recv.at[a, kind + 2, k], target).wait_recv()

    def z_done(a, k):
        block = arrays[a][0](layer[k] * PLANE + p)
        hop(block, block, z_send.at[a, 0], recv.at[a, 0, k], line[k]).wait_recv()

    @pl.when(inner == 1)
    def _():
        for a in range(N_SMALL):
            z_hop(a, piece(a, z), fs, 1, 2, 2).start()

    for a in range(N_SMALL):
        c = z_hop(a, piece(a, z), fs, 0, 1, 1)
        c.start()
        pending.append(c)
    inner_pending += [(a, 1) for a in range(N_SMALL)]
    for a in range(N_SMALL):
        sides(a, 0)

    own = [
        pltpu.make_async_copy(gup, gup_v, local.at[0]),
        pltpu.make_async_copy(vup, vup_v, local.at[1]),
        pltpu.make_async_copy(tok, whole_tok.at[:, span(tp, half)], local.at[2]),
        pltpu.make_async_copy(pld, pld_v, local.at[3]),
        pltpu.make_async_copy(rb, arrays[0][0](fs), local.at[4]),
        pltpu.make_async_copy(og, arrays[1][0](fs), local.at[5]),
        pltpu.make_async_copy(mo, arrays[2][0](fs), local.at[6]),
        pltpu.make_async_copy(piece(4, z), arrays[4][0](fs), local.at[7]),
    ]
    for c in own:
        c.start()

    own[0].wait()
    own[1].wait()

    def arrange(gate, value, zz, store):
        for j in range(full):
            at = zz * units + j * LANES
            store(2 * j * LANES, gate[:, at : at + LANES])
            store((2 * j + 1) * LANES, value[:, at : at + LANES])
        if rest:
            at = zz * units + full * LANES
            store(2 * full * LANES, gate[:, at : at + rest])
            store(2 * full * LANES + rest, value[:, at : at + rest])

    for zz in range(LAYERS):

        def put(at, v, zz=zz):
            stage[zz, :, at : at + v.shape[1]] = v

        def put_taps(at, v, zz=zz):
            taps[zz, 0 : v.shape[0], at : at + v.shape[1]] = v.astype(F32)

        arrange(gup_v, vup_v, zz, put)
        arrange(gtaps, vtaps, zz, put_taps)
    gu_all[span(fs, deep), :] = stage[z]
    dn_all[units:, :] = jnp.zeros((dn_all.shape[0] - units, dn_all.shape[1]), BF16)
    gmap[...] = jnp.zeros(gmap.shape, BF16)
    for c in range(heads // per):
        for h in range(per):
            r = slice(h * head, (h + 1) * head)
            gmap[c, r, h * head : (h + 1) * head] = rmap[c * per + h]
            gmap[c, r, cw + h * head : cw + (h + 1) * head] = imap[c * per + h]

    def relay(k, to, land, slot):
        @pl.when(inner == 1)
        def _():
            for a in range(N_SMALL):
                f = layer[k] * PLANE + p
                z_hop(a, arrays[a][0](f), f, slot, land, to).start()

        inner_pending.extend((a, slot) for a in range(N_SMALL))

    for k, to, land in ((1, 2, 3), (2, 1, 2), (3, 1, 3)):
        for a in range(N_SMALL):
            z_done(a, k)
        relay(k, to, land, k + 1)
        for a in range(N_SMALL):
            sides(a, k)
        for a in range(N_SMALL):
            corners(a, k - 1)
    for a in range(N_SMALL, N_BIG):
        for k in range(1, LAYERS):
            c = z_hop(a, piece(a, layer[k]), fs, k, lands[k], k)
            c.start()
            pending.append(c)
    for a in range(N_SMALL):
        corners(a, LAYERS - 1)
    sides(3, 0)
    z_done(3, 1)
    sides(3, 1)

    tok_copy.wait_recv()
    own[2].wait()
    wide_tok = whole_tok[...].astype(F32)
    normed[...] = normed_rows(wide_tok, gain1[...].astype(F32))
    for c in own[3:]:
        c.wait()
    for k in range(LAYERS):
        for a in range(N_SMALL):
            corners_done(a, k)

    def mixer_chunk(c, _):
        at = span(c, cw)
        place = position((rows, cw))
        branch = jnp.dot(normed[...], bo_all[:, at], preferred_element_type=F32)
        branch = branch.astype(BF16).astype(F32)
        conv = rows_conv(branch, ctaps[:, at].astype(F32), ctaps.shape[0], place).astype(BF16)
        gates = jax.nn.sigmoid(jnp.dot(conv, gmap[c], preferred_element_type=F32))
        la = -DECAY_RATE_GAIN * gates[:, :cw] * rate[:, at] + pld_v[:, at]
        d = jnp.sqrt(negative_expm1(2.0 * la)) * gates[:, cw:] * conv.astype(F32)
        a = jnp.exp(la)
        step = 1
        while step < SEQ_LEN:
            d = a * shifted(d, step, place, 0.0) + d
            if step * 2 < SEQ_LEN:
                a = a * shifted(a, step, place, 1.0)
            step *= 2
        outgate = jnp.dot(
            normed[...],
            bo_all[:, pl.ds(pl.multiple_of(local_width + c * cw, cw), cw)],
            preferred_element_type=F32,
        )
        outgate = outgate.astype(BF16).astype(F32)
        mixed[:, at] = (d * gelu(outgate)).astype(BF16)
        return 0

    lax.fori_loop(0, local_width // cw, mixer_chunk, 0)
    z_done(3, 2)
    sides(3, 2)
    mix_wide = mine.shape[2]
    swaps = []
    for c in range(mine.shape[0]):
        mine[c] = jnp.dot(
            mixed[...], mo_all[:, c * mix_wide : (c + 1) * mix_wide], preferred_element_type=F32
        ).astype(BF16)
        s = hop(mine.at[c], theirs.at[c], swap_send.at[c], swap_recv.at[c], core_target)
        s.start()
        swaps.append(s)
    z_done(3, 3)
    sides(3, 3)
    square = jnp.zeros((rows, 1), F32)
    for c in range(mine.shape[0]):
        at = slice(c * mix_wide, (c + 1) * mix_wide)
        swaps[c].wait_recv()
        both = mine[c].astype(F32) + theirs[c].astype(F32)
        total = (whole_tok[:, at].astype(F32) + both).astype(BF16)
        after[:, at] = total
        total = total.astype(F32)
        square = square + jnp.sum(total * total, axis=-1, keepdims=True)
    factor = lax.rsqrt(square * (1.0 / after.shape[1]) + EPS)
    n2[0] = (after[...].astype(F32) * factor * gain2[...].astype(F32)).astype(BF16)

    mine_half = span(tp, half)

    def rows_hop(k, land, slot, to):
        return hop(
            n2.at[k, :, mine_half], n2.at[land, :, mine_half], n2_send.at[slot], n2_recv.at[land], line[to]
        )

    @pl.when(inner == 1)
    def _():
        rows_hop(0, 2, 1, 2).start()

    c = rows_hop(0, 1, 0, 1)
    c.start()
    pending.append(c)
    across = {}

    def rows_arrived(k, to, land):
        rows_hop(k, k, 0, 1).wait_recv()

        @pl.when(inner == 1)
        def _():
            rows_hop(k, land, k + 1, to).start()

        block = n2.at[k, :, mine_half]
        across[k] = hop(block, block, core_send.at[k], core_recv.at[k], core_target)
        across[k].start()

    for k in range(LAYERS):
        corners(3, k)
    dn_order = (0, 2, 1, 3)
    sides(4, 0)
    for k in dn_order[1:]:
        z_done(4, k)
        sides(4, k)
    rows_arrived(1, 2, 3)
    rows_arrived(2, 1, 2)

    def up(k):
        place = position((rows, 4 * LANES))
        layer_taps = taps.at[z]
        width = gtaps.shape[0]
        j = 0
        while j < 2 * full * LANES:
            n = min(4 * LANES, 2 * full * LANES - j)
            s = jnp.dot(n2[k], gu_all[:, j : j + n], preferred_element_type=F32)
            s = rows_conv(s.astype(BF16).astype(F32), layer_taps[0:width, j : j + n], width, place[:, :n])
            for i in range(0, n, 2 * LANES):
                g, v = s[:, i : i + LANES], s[:, i + LANES : i + 2 * LANES]
                h = (j + i) // 2
                hidden[k, :, h : h + LANES] = (g * jax.nn.sigmoid(g) * v).astype(BF16)
            j += n
        if rest:
            s = jnp.dot(n2[k], gu_all[:, j:], preferred_element_type=F32)
            s = rows_conv(s.astype(BF16).astype(F32), layer_taps[0:width, j:], width, place[:, :LANES])
            h = s * jax.nn.sigmoid(s) * pltpu.roll(s, rest, 1)
            lane = lax.broadcasted_iota(jnp.int32, h.shape, 1)
            hidden[k, :, full * LANES : (full + 1) * LANES] = jnp.where(lane < rest, h, 0.0).astype(BF16)

    def up_step(k, _):
        up(k)
        return 0

    for k in range(LAYERS):
        corners_done(3, k)
    lax.fori_loop(0, 1, up_step, 0)
    corners(4, 0)
    corners(4, 2)
    across[1].wait_recv()
    across[2].wait_recv()
    rows_arrived(3, 1, 3)
    lax.fori_loop(1, 3, up_step, 0)
    corners(4, 1)
    corners(4, 3)
    across[3].wait_recv()
    lax.fori_loop(3, 4, up_step, 0)

    turn = (tp + z // 2) % 2
    chunk = PLANE * wide
    backs = []
    for i in range(LAYERS // 2):
        first, second = layer[i], layer[i + 2]
        kept = first * (1 - turn) + second * turn
        given = first * turn + second * (1 - turn)
        corners_done(4, i)
        corners_done(4, i + 2)

        def give_step(k, _):
            give[i, k] = jnp.dot(
                hidden[k], dn_all[:, span(given, chunk)], preferred_element_type=F32
            ).astype(BF16)
            return 0

        def keep_step(k, _):
            keep[k] = jnp.dot(
                hidden[k], dn_all[:, span(kept, chunk)], preferred_element_type=F32
            ).astype(BF16)
            return 0

        lax.fori_loop(0, LAYERS, give_step, 0)
        s = hop(give.at[i], pair.at[i], pair_send.at[i], pair_recv.at[i], core_target)
        s.start()
        pending.append(s)
        lax.fori_loop(0, LAYERS, keep_step, 0)
        s.wait_recv()
        place_at = span(kept % 2, chunk)

        def pair_step(k, _):
            paired[i, k] = (keep[k].astype(F32) + pair[i, k].astype(F32)).astype(BF16)
            return 0

        lax.fori_loop(0, LAYERS, pair_step, 0)
        own_part[:, place_at] = paired[i, 0]
        for k in range(1, LAYERS):
            c = hop(
                paired.at[i, k], arrive.at[lands[k] - 1, :, place_at],
                back_send.at[i, k], back_recv.at[i, lands[k]], line[k],
            )
            c.start()
            pending.append(c)
            block = arrive.at[k - 1, :, place_at]
            backs.append(hop(paired.at[i, k], block, back_send.at[i, k], back_recv.at[i, k], line[k]))

    for c in backs:
        c.wait_recv()
    total = own_part[...].astype(F32)
    for k in range(LAYERS - 1):
        total = total + arrive[k].astype(F32)
    out[...] = (after[:, mine_half].astype(F32) + total).astype(BF16)

    for c in pending + swaps + list(across.values()) + [tok_copy]:
        c.wait_send()

    @pl.when(inner == 1)
    def _():
        for a, slot in inner_pending:
            z_hop(a, arrays[a][0](fs), fs, slot, 0, 1).wait_send()
        for slot in range(1, LAYERS + 1):
            rows_hop(0, 0, slot, 1).wait_send()


def fused_layer(
    tokens,
    mixer_norm_gain,
    recurrence_branch_weight,
    output_gate_projection,
    recurrence_conv_taps,
    recurrence_gate_map,
    input_gate_map,
    channel_decay_rate,
    position_log_decay,
    mixer_output_weight,
    feedforward_norm_gain,
    gate_up_weight,
    value_up_weight,
    gate_conv_taps,
    value_conv_taps,
    down_projection_weight,
):
    rows, half = tokens.shape
    deep, local_width = recurrence_branch_weight.shape
    wide = mixer_output_weight.shape[1]
    n_fs = LAYERS * PLANE
    features = 2 * half
    local_units = gate_up_weight.shape[1]
    units = local_units // LAYERS
    padded = -(-units // (2 * LANES)) * 2 * LANES
    head = recurrence_gate_map.shape[1]
    cw = min(local_width, 4 * head)
    chunk = PLANE * wide
    dma = pltpu.SemaphoreType.DMA
    scratch = [
        pltpu.VMEM((rows, features), BF16),
        pltpu.VMEM((n_fs * deep, 2 * local_width), BF16),
        pltpu.VMEM((local_width, n_fs * wide), BF16),
        pltpu.VMEM((deep, local_units), BF16),
        pltpu.VMEM((deep, local_units), BF16),
        pltpu.VMEM((LAYERS, deep, 2 * units), BF16),
        pltpu.VMEM((n_fs * deep, 2 * units), BF16),
        pltpu.VMEM((padded, n_fs * wide), BF16),
        pltpu.VMEM((LAYERS, 8, 2 * units), F32),
        pltpu.VMEM((local_width // cw, cw, 2 * cw), BF16),
        pltpu.VMEM((rows, local_width), F32),
        pltpu.VMEM((rows, features), BF16),
        pltpu.VMEM((rows, local_width), BF16),
        pltpu.VMEM((LAYERS, rows, chunk), BF16),
        pltpu.VMEM((LAYERS, rows, chunk), BF16),
        pltpu.VMEM((rows, features), BF16),
        pltpu.VMEM((LAYERS, rows, features), BF16),
        pltpu.VMEM((LAYERS, rows, padded), BF16),
        pltpu.VMEM((2, LAYERS, rows, chunk), BF16),
        pltpu.VMEM((LAYERS, rows, chunk), BF16),
        pltpu.VMEM((2, LAYERS, rows, chunk), BF16),
        pltpu.VMEM((2, LAYERS, rows, chunk), BF16),
        pltpu.VMEM((rows, half), BF16),
        pltpu.VMEM((LAYERS - 1, rows, half), BF16),
        dma((N_BIG, 5, LAYERS)),
        dma((N_BIG, 5, LAYERS)),
        dma((N_BIG, LAYERS + 1)),
        dma((8,)),
        dma((2,)),
        dma((LAYERS,)),
        dma((LAYERS,)),
        dma((LAYERS + 1,)),
        dma((LAYERS,)),
        dma((LAYERS,)),
        dma((LAYERS,)),
        dma((2,)),
        dma((2,)),
        dma((2, LAYERS)),
        dma((2, LAYERS)),
    ]
    return pl.pallas_call(
        layer_kernel,
        out_shape=jax.ShapeDtypeStruct((rows, half), BF16),
        in_specs=[ANY, VMEM, ANY, ANY, VMEM, VMEM, VMEM, VMEM, ANY, ANY, VMEM, ANY, ANY, VMEM, VMEM, ANY],
        out_specs=VMEM,
        scratch_shapes=scratch,
        compiler_params=pltpu.CompilerParams(
            collective_id=0, has_side_effects=True, vmem_limit_bytes=62 * 2**20
        ),
        name="layer",
    )(
        tokens,
        mixer_norm_gain.reshape(1, -1),
        recurrence_branch_weight,
        output_gate_projection,
        recurrence_conv_taps,
        recurrence_gate_map,
        input_gate_map,
        channel_decay_rate.reshape(1, -1),
        position_log_decay,
        mixer_output_weight,
        feedforward_norm_gain.reshape(1, -1),
        gate_up_weight,
        value_up_weight,
        gate_conv_taps,
        value_conv_taps,
        down_projection_weight,
    )


def solution(mesh):
    placed = (
        P("fs", "tp"),
        P(),
        P("fs", "tp"),
        P("fs", "tp"),
        P(None, "tp"),
        P("tp", None, None),
        P("tp", None, None),
        P("tp"),
        P("fs", "tp"),
        P("tp", "fs"),
        P(),
        P("fs", "tp"),
        P("fs", "tp"),
        P(None, "tp"),
        P(None, "tp"),
        P("tp", "fs"),
    )
    fused = mesh.shape["tp"] == 2 and mesh.shape["fs"] == LAYERS * PLANE
    body = fused_layer if fused else gathered_layer
    return jax.shard_map(
        body, mesh=mesh, in_specs=placed, out_specs=P("fs", "tp"), check_vma=False
    )
```

```python
import functools

import jax
import jax.numpy as jnp
from jax import lax
from jax.experimental import pallas as pl
from jax.experimental.pallas import tpu as pltpu
from jax.sharding import PartitionSpec as P

SEQ_LEN = 64


EPS = 1e-06
DECAY_RATE_GAIN = 8.0


def rms_normed(values, gain):
    wide = values.astype(jnp.float32)
    factor = lax.rsqrt(jnp.mean(wide * wide, axis=-1, keepdims=True) + EPS)
    return (wide * factor * gain.astype(jnp.float32)).astype(jnp.bfloat16)


def causal_conv(values, kernel):
    width = kernel.shape[0]
    row_count, channels = values.shape
    grouped = values.astype(jnp.float32).reshape(row_count // SEQ_LEN, SEQ_LEN, channels)
    padded = jnp.pad(grouped, ((0, 0), (width - 1, 0), (0, 0)))
    summed = padded[:, 0:SEQ_LEN] * kernel[0].astype(jnp.float32)
    for offset in range(1, width):
        summed = summed + padded[:, offset : offset + SEQ_LEN] * kernel[offset].astype(jnp.float32)
    return summed.reshape(row_count, channels)


def combine(left, right):
    first_a, first_b = left
    second_a, second_b = right
    return (first_a * second_a, second_a * first_b + second_b)


def pair_folder(normed, pieces):
    return (
        jnp.dot(normed, pieces[0], preferred_element_type=jnp.float32),
        jnp.dot(normed, pieces[1], preferred_element_type=jnp.float32),
    )


def gathered_layer(
    tokens,
    mixer_norm_gain,
    recurrence_branch_weight,
    output_gate_projection,
    recurrence_conv_taps,
    recurrence_gate_map,
    input_gate_map,
    channel_decay_rate,
    position_log_decay,
    mixer_output_weight,
    feedforward_norm_gain,
    gate_up_weight,
    value_up_weight,
    gate_conv_taps,
    value_conv_taps,
    down_projection_weight,
):
    row_count = tokens.shape[0]
    local_width = recurrence_branch_weight.shape[1]
    local_heads = recurrence_gate_map.shape[0]
    head_size = recurrence_gate_map.shape[1]
    whole_rows = lax.all_gather(tokens, "tp", axis=1, tiled=True)
    normed = rms_normed(whole_rows, mixer_norm_gain)
    branch_sum, outgate_sum = pair_folder(
        normed,
        (
            lax.all_gather(recurrence_branch_weight, "fs", axis=0, tiled=True),
            lax.all_gather(output_gate_projection, "fs", axis=0, tiled=True),
        ),
    )
    branch = branch_sum.astype(jnp.bfloat16)
    outgate = outgate_sum.astype(jnp.bfloat16)
    conv = causal_conv(branch, recurrence_conv_taps).astype(jnp.bfloat16)
    grouped = conv.reshape(row_count, local_heads, head_size)
    recurrence_scan = jax.nn.sigmoid(
        jnp.einsum(
            "rhi,hij->rhj", grouped, recurrence_gate_map, preferred_element_type=jnp.float32
        ).reshape(row_count, local_width)
    )
    inner = jax.nn.sigmoid(
        jnp.einsum(
            "rhi,hij->rhj", grouped, input_gate_map, preferred_element_type=jnp.float32
        ).reshape(row_count, local_width)
    )
    log_alpha = (
        -DECAY_RATE_GAIN * recurrence_scan * channel_decay_rate[None, :] + position_log_decay
    )
    drive = jnp.sqrt(-jnp.expm1(2.0 * log_alpha)) * inner * conv.astype(jnp.float32)
    shape3 = (row_count // SEQ_LEN, SEQ_LEN, local_width)
    unused, state = lax.associative_scan(
        combine, (jnp.exp(log_alpha).reshape(shape3), drive.reshape(shape3)), axis=1
    )
    state = state.reshape(row_count, local_width)
    mixed = (state * jax.nn.gelu(outgate.astype(jnp.float32))).astype(jnp.bfloat16)
    mixer_terms = jnp.dot(
        mixed,
        lax.all_gather(mixer_output_weight, "fs", axis=1, tiled=True),
        preferred_element_type=jnp.float32,
    )
    mixer_terms = mixer_terms.astype(jnp.bfloat16).astype(jnp.float32)
    mixer_whole = lax.psum(mixer_terms.astype(jnp.bfloat16), "tp").astype(jnp.float32)
    whole_after = (whole_rows.astype(jnp.float32) + mixer_whole).astype(jnp.bfloat16)
    normed2 = rms_normed(whole_after, feedforward_norm_gain)
    gate_whole, value_whole = (
        lax.all_gather(gate_up_weight, "fs", axis=0, tiled=True),
        lax.all_gather(value_up_weight, "fs", axis=0, tiled=True),
    )
    gate_sum = jnp.dot(normed2, gate_whole, preferred_element_type=jnp.float32)
    value_sum = jnp.dot(normed2, value_whole, preferred_element_type=jnp.float32)
    gate_half = gate_sum.astype(jnp.bfloat16)
    value_half = value_sum.astype(jnp.bfloat16)
    hidden = (
        jax.nn.silu(causal_conv(gate_half, gate_conv_taps))
        * causal_conv(value_half, value_conv_taps)
    ).astype(jnp.bfloat16)
    channel_terms = jnp.dot(
        hidden,
        lax.all_gather(down_projection_weight, "fs", axis=1, tiled=True),
        preferred_element_type=jnp.float32,
    )
    channel_terms = channel_terms.astype(jnp.bfloat16).astype(jnp.float32)
    channel_share = lax.psum_scatter(
        channel_terms.astype(jnp.bfloat16), "tp", scatter_dimension=1, tiled=True
    ).astype(jnp.float32)
    share_width = channel_share.shape[1]
    residual_share = lax.dynamic_slice_in_dim(
        whole_after, lax.axis_index("tp") * share_width, share_width, 1
    )
    return (residual_share.astype(jnp.float32) + channel_share).astype(jnp.bfloat16)


PLANE = 4
LAYERS = 4
LANES = 128
ANY = pl.BlockSpec(memory_space=pl.ANY)
VMEM = pl.BlockSpec(memory_space=pltpu.VMEM)
F32, BF16 = jnp.float32, jnp.bfloat16
N_SMALL, N_BIG = 3, 5


def hop(src, dst, send, recv, target):
    return pltpu.make_async_remote_copy(
        src_ref=src,
        dst_ref=dst,
        send_sem=send,
        recv_sem=recv,
        device_id=target,
        device_id_type=pl.DeviceIdType.MESH,
    )


def greet(targets):
    barrier = pltpu.get_barrier_semaphore()
    for target in targets:
        pl.semaphore_signal(
            barrier, inc=1, device_id=target, device_id_type=pl.DeviceIdType.MESH
        )
    pl.semaphore_wait(barrier, len(targets))


def span(index, size):
    return pl.ds(pl.multiple_of(index * size, size), size)


def row_blocks(whole, deep, columns):
    def at(f, part=None):
        if part is None:
            return whole.at[span(f, deep), columns]
        return whole.at[span(f * 2 + part, deep // 2), columns]

    return at


def column_blocks(whole, rows, wide):
    def at(f, part=None):
        if part is None:
            return whole.at[pl.ds(0, rows), span(f, wide)]
        return whole.at[pl.ds(part * (rows // 2), rows // 2), span(f, wide)]

    return at


def position(shape):
    return lax.broadcasted_iota(jnp.int32, shape, 0) % SEQ_LEN


def shifted(values, distance, place, fill):
    return jnp.where(place >= distance, pltpu.roll(values, distance, 0), fill)


def rows_conv(values, taps, width, place):
    summed = shifted(values, width - 1, place, 0.0) * taps[0:1, :]
    for j in range(1, width - 1):
        summed = summed + shifted(values, width - 1 - j, place, 0.0) * taps[j : j + 1, :]
    return summed + values * taps[width - 1 : width, :]


def negative_expm1(x):
    near = 1.0 + x * (1.0 / 8.0)
    for n in range(7, 1, -1):
        near = 1.0 + x * (1.0 / n) * near
    return jnp.where(jnp.abs(x) < 0.4, -x * near, 1.0 - jnp.exp(x))


def normed_rows(values, gain):
    factor = lax.rsqrt(jnp.mean(values * values, axis=-1, keepdims=True) + EPS)
    return (values * factor * gain).astype(BF16)


def gelu(x):
    return 0.5 * x * (1.0 + jnp.tanh(0.7978845608028654 * (x + 0.044715 * (x * x * x))))


def layer_kernel(
    tok, gain1, rb, og, ctaps, rmap, imap, rate, pld, mo, gain2, gup, vup, gtaps, vtaps, dn,
    out,
    whole_tok, bo_all, mo_all, gup_v, vup_v, stage, gu_all, dn_all, taps, gmap, pld_v,
    normed, mixed, mine, theirs, after, n2, hidden, give, keep, pair, paired, own_part, arrive, joint,
    send, recv, z_send, local, tok_sem, swap_send, swap_recv, n2_send, n2_recv,
    core_send, core_recv, pair_send, pair_recv, back_send, back_recv, joint_send,
):
    fs, tp = lax.axis_index("fs"), lax.axis_index("tp")
    z, p = fs // PLANE, fs % PLANE
    y, x = p // 2, p % 2
    px, py = y * 2 + 1 - x, (1 - y) * 2 + x
    inner = ((z + 1) // 2) % 2
    layer = (z, z + 1 - 2 * (z % 2), 2 - z // 2, 3 - 3 * (z // 2))
    lands = (0, 1, 3 - inner, 3 - inner)
    down = (
        ((inner, 3 * (z // 2)), (2, layer[2])),
        ((1 - inner, 1 + z // 2), (3, layer[3])),
    )
    line = [(zz * PLANE + p, tp) for zz in layer]
    x_target, y_target = (z * PLANE + px, tp), (z * PLANE + py, tp)
    core_target = (fs, 1 - tp)
    with jax.named_scope("greet"):
        greet(line[1:] + [x_target, y_target, core_target])

    rows, half = tok.shape
    deep, local_width = rb.shape
    wide = mo.shape[1]
    units = dn.shape[0] // LAYERS
    full, rest = units // LANES, units % LANES
    cw = gmap.shape[1]
    heads, head = rmap.shape[:2]
    per = cw // head

    arrays = (
        (row_blocks(bo_all, deep, pl.ds(0, local_width)), rb),
        (row_blocks(bo_all, deep, pl.ds(local_width, local_width)), og),
        (column_blocks(mo_all, mo.shape[0], wide), mo),
        (row_blocks(gu_all, deep, slice(None)), None),
        (column_blocks(dn_all, units, wide), None),
    )

    def piece(a, zz):
        if a < N_SMALL:
            return arrays[a][1]
        return stage.at[zz] if a == 3 else dn.at[span(zz, units), :]

    pending = []
    inner_pending = []

    copy = hop(tok, whole_tok.at[:, span(tp, half)], tok_sem.at[0], tok_sem.at[1], core_target)
    copy.start()
    tok_copy = copy

    def z_hop(a, source, f, slot, land, to):
        return hop(source, arrays[a][0](f), z_send.at[a, slot], recv.at[a, 0, land], line[to])

    def sides(a, k, of=None):
        at = arrays[a][0]
        f = (layer[k] if of is None else of) * PLANE + p
        source = piece(a, z) if of is None and k == 0 else at(f)
        for kind, target in ((1, x_target), (2, y_target)):
            c = hop(source, at(f), send.at[a, kind, k], recv.at[a, kind, k], target)
            c.start()
            pending.append(c)

    def corners(a, k, of=None):
        at = arrays[a][0]
        base = (layer[k] if of is None else of) * PLANE
        for kind, part, owner, target in ((1, 0, px, y_target), (2, 1, py, x_target)):
            whole = at(base + owner)
            with jax.named_scope(f"side{a}{k if of is None else 9}{kind}"):
                hop(whole, whole, send.at[a, kind, k], recv.at[a, kind, k], target).wait_recv()
            block = at(base + owner, part)
            c = hop(block, block, send.at[a, kind + 2, k], recv.at[a, kind + 2, k], target)
            c.start()
            pending.append(c)

    def corners_done(a, k, of=None):
        at = arrays[a][0]
        corner = (layer[k] if of is None else of) * PLANE + (PLANE - 1 - p)
        for kind, part, target in ((1, 0, y_target), (2, 1, x_target)):
            block = at(corner, part)
            with jax.named_scope(f"corner{a}{k if of is None else 9}{kind}"):
                hop(block, block, send.at[a, kind + 2, k], recv.at[a, kind + 2, k], target).wait_recv()

    def z_done(a, k):
        block = arrays[a][0](layer[k] * PLANE + p)
        with jax.named_scope(f"z{a}{k}"):
            hop(block, block, z_send.at[a, 0], recv.at[a, 0, k], line[k]).wait_recv()

    @pl.when(inner == 1)
    def _():
        for a in range(N_SMALL):
            z_hop(a, piece(a, z), fs, 1, 2, 2).start()

    for a in range(N_SMALL):
        c = z_hop(a, piece(a, z), fs, 0, 1, 1)
        c.start()
        pending.append(c)
    inner_pending += [(a, 1) for a in range(N_SMALL)]
    for a in range(N_SMALL):
        sides(a, 0)

    own = [
        pltpu.make_async_copy(gup, gup_v, local.at[0]),
        pltpu.make_async_copy(vup, vup_v, local.at[1]),
        pltpu.make_async_copy(tok, whole_tok.at[:, span(tp, half)], local.at[2]),
        pltpu.make_async_copy(pld, pld_v, local.at[3]),
        pltpu.make_async_copy(rb, arrays[0][0](fs), local.at[4]),
        pltpu.make_async_copy(og, arrays[1][0](fs), local.at[5]),
        pltpu.make_async_copy(mo, arrays[2][0](fs), local.at[6]),
        pltpu.make_async_copy(piece(4, z), arrays[4][0](fs), local.at[7]),
    ]
    for c in own:
        c.start()

    own[0].wait()
    own[1].wait()

    def arrange(gate, value, zz, store):
        for j in range(full):
            at = zz * units + j * LANES
            store(2 * j * LANES, gate[:, at : at + LANES])
            store((2 * j + 1) * LANES, value[:, at : at + LANES])
        if rest:
            at = zz * units + full * LANES
            store(2 * full * LANES, gate[:, at : at + rest])
            store(2 * full * LANES + rest, value[:, at : at + rest])

    for zz in range(LAYERS):

        def put(at, v, zz=zz):
            stage[zz, :, at : at + v.shape[1]] = v

        def put_taps(at, v, zz=zz):
            taps[zz, 0 : v.shape[0], at : at + v.shape[1]] = v.astype(F32)

        arrange(gup_v, vup_v, zz, put)
        arrange(gtaps, vtaps, zz, put_taps)
    gu_all[span(fs, deep), :] = stage[z]
    dn_all[units:, :] = jnp.zeros((dn_all.shape[0] - units, dn_all.shape[1]), BF16)
    gmap[...] = jnp.zeros(gmap.shape, BF16)
    for c in range(heads // per):
        for h in range(per):
            r = slice(h * head, (h + 1) * head)
            gmap[c, r, h * head : (h + 1) * head] = rmap[c * per + h]
            gmap[c, r, cw + h * head : cw + (h + 1) * head] = imap[c * per + h]

    def relay(k, to, land, slot):
        @pl.when(inner == 1)
        def _():
            for a in range(N_SMALL):
                f = layer[k] * PLANE + p
                z_hop(a, arrays[a][0](f), f, slot, land, to).start()

        inner_pending.extend((a, slot) for a in range(N_SMALL))

    def ffn_along_z(where):
        @pl.when(inner == where)
        def _():
            for a in range(N_SMALL, N_BIG):
                for k in range(1, LAYERS):
                    z_hop(a, piece(a, layer[k]), fs, k, lands[k], k).start()

    for k, to, land in ((1, 2, 3), (2, 1, 2), (3, 1, 3)):
        for a in range(N_SMALL):
            z_done(a, k)
        relay(k, to, land, k + 1)
        if k > 1:
            ffn_along_z(k - 2)
        for a in range(N_SMALL):
            sides(a, k)
        if k == 2:
            for a in range(N_SMALL):
                corners(a, 0)
    for k in range(1, LAYERS):
        for a in range(N_SMALL):
            corners(a, k)
    sides(3, 0)
    z_done(3, 1)
    sides(3, 1)

    with jax.named_scope("tokens"):
        tok_copy.wait_recv()
        own[2].wait()
    wide_tok = whole_tok[...].astype(F32)
    normed[...] = normed_rows(wide_tok, gain1[...].astype(F32)[None, :])
    for c in own[3:]:
        c.wait()
    for k in range(LAYERS):
        for a in range(N_SMALL):
            corners_done(a, k)

    def mixer_chunk(c, _):
        at = span(c, cw)
        place = position((rows, cw))
        branch = jnp.dot(normed[...], bo_all[:, at], preferred_element_type=F32)
        branch = branch.astype(BF16).astype(F32)
        conv = rows_conv(branch, ctaps[:, at].astype(F32), ctaps.shape[0], place).astype(BF16)
        gates = jax.nn.sigmoid(jnp.dot(conv, gmap[c], preferred_element_type=F32))
        la = -DECAY_RATE_GAIN * gates[:, :cw] * rate[:, at] + pld_v[:, at]
        d = jnp.sqrt(negative_expm1(2.0 * la)) * gates[:, cw:] * conv.astype(F32)
        a = jnp.exp(la)
        step = 1
        while step < SEQ_LEN:
            d = a * shifted(d, step, place, 0.0) + d
            if step * 2 < SEQ_LEN:
                a = a * shifted(a, step, place, 1.0)
            step *= 2
        outgate = jnp.dot(
            normed[...],
            bo_all[:, pl.ds(pl.multiple_of(local_width + c * cw, cw), cw)],
            preferred_element_type=F32,
        )
        outgate = outgate.astype(BF16).astype(F32)
        mixed[:, at] = (d * gelu(outgate)).astype(BF16)
        return 0

    with jax.named_scope("mixer"):
        lax.fori_loop(0, local_width // cw, mixer_chunk, 0)
    mix_wide = mine.shape[2]
    swaps = []
    for c in range(mine.shape[0]):
        mine[c] = jnp.dot(
            mixed[...], mo_all[:, c * mix_wide : (c + 1) * mix_wide], preferred_element_type=F32
        ).astype(BF16)
        s = hop(mine.at[c], theirs.at[c], swap_send.at[c], swap_recv.at[c], core_target)
        s.start()
        swaps.append(s)
    square = jnp.zeros((rows, 1), F32)
    for c in range(mine.shape[0]):
        at = slice(c * mix_wide, (c + 1) * mix_wide)
        with jax.named_scope(f"swap{c}"):
            swaps[c].wait_recv()
        both = mine[c].astype(F32) + theirs[c].astype(F32)
        total = (whole_tok[:, at].astype(F32) + both).astype(BF16)
        after[:, at] = total
        total = total.astype(F32)
        square = square + jnp.sum(total * total, axis=-1, keepdims=True)
    factor = lax.rsqrt(square * (1.0 / after.shape[1]) + EPS)
    n2[0] = (after[...].astype(F32) * factor * gain2[...].astype(F32)[None, :]).astype(BF16)

    mine_half = span(tp, half)

    def rows_hop(k, land, slot, to):
        return hop(
            n2.at[k, :, mine_half], n2.at[land, :, mine_half], n2_send.at[slot], n2_recv.at[land], line[to]
        )

    @pl.when(inner == 1)
    def _():
        rows_hop(0, 2, 1, 2).start()

    c = rows_hop(0, 1, 0, 1)
    c.start()
    pending.append(c)

    def rows_arrived(k, to, land):
        with jax.named_scope(f"rows{k}"):
            rows_hop(k, k, 0, 1).wait_recv()

        @pl.when(inner == 1)
        def _():
            rows_hop(k, land, k + 1, to).start()

        core_hop(k).start()

    def core_hop(k):
        block = n2.at[k, :, mine_half]
        return hop(block, block, core_send.at[k], core_recv.at[k], core_target)

    for k in (2, 3):
        z_done(3, k)
        sides(3, k)
    corners(3, 0)
    corners(3, 1)
    rows_arrived(1, 2, 3)
    corners(3, 2)
    rows_arrived(2, 1, 2)
    corners(3, 3)
    z_done(4, 1)
    z_done(4, 2)
    down_a, down_b = down[0]
    sides(4, *down_a)
    sides(4, *down_b)

    @pl.when(inner == 1)
    def _():
        rows_arrived(3, 1, 3)

    def up(k):
        place = position((rows, 4 * LANES))
        layer_taps = taps.at[z]
        width = gtaps.shape[0]
        j = 0
        while j < 2 * full * LANES:
            n = min(4 * LANES, 2 * full * LANES - j)
            s = jnp.dot(n2[k], gu_all[:, j : j + n], preferred_element_type=F32)
            s = rows_conv(s.astype(BF16).astype(F32), layer_taps[0:width, j : j + n], width, place[:, :n])
            for i in range(0, n, 2 * LANES):
                g, v = s[:, i : i + LANES], s[:, i + LANES : i + 2 * LANES]
                h = (j + i) // 2
                hidden[k, :, h : h + LANES] = (g * jax.nn.sigmoid(g) * v).astype(BF16)
            j += n
        if rest:
            s = jnp.dot(n2[k], gu_all[:, j:], preferred_element_type=F32)
            s = rows_conv(s.astype(BF16).astype(F32), layer_taps[0:width, j:], width, place[:, :LANES])
            h = s * jax.nn.sigmoid(s) * pltpu.roll(s, rest, 1)
            lane = lax.broadcasted_iota(jnp.int32, h.shape, 1)
            hidden[k, :, full * LANES : (full + 1) * LANES] = jnp.where(lane < rest, h, 0.0).astype(BF16)

    def up_step(k, _):
        with jax.named_scope("up"):
            up(k)
        return 0

    for k in range(LAYERS):
        corners_done(3, k)
    lax.fori_loop(0, 1, up_step, 0)
    with jax.named_scope("across12"):
        core_hop(1).wait_recv()
        core_hop(2).wait_recv()
    lax.fori_loop(1, 2, up_step, 0)
    corners(4, *down_a)
    lax.fori_loop(2, 3, up_step, 0)
    corners(4, *down_b)
    z_done(4, 3)
    for block in down[1]:
        sides(4, *block)

    @pl.when(inner == 0)
    def _():
        rows_arrived(3, 1, 3)

    with jax.named_scope("across3"):
        core_hop(3).wait_recv()
    lax.fori_loop(3, 4, up_step, 0)

    turn = (tp + z // 2) % 2
    chunk = PLANE * wide
    step_count = LAYERS // 2

    def chunk_sum(i):
        first, second = down[i][0][1], down[i][1][1]
        kept = first * (1 - turn) + second * turn
        given = first * turn + second * (1 - turn)
        for block in down[i]:
            corners_done(4, *block)

        def give_step(k, _):
            give[i, k] = jnp.dot(
                hidden[k], dn_all[:, span(given, chunk)], preferred_element_type=F32
            ).astype(BF16)
            return 0

        def keep_step(k, _):
            keep[k] = jnp.dot(
                hidden[k], dn_all[:, span(kept, chunk)], preferred_element_type=F32
            ).astype(BF16)
            return 0

        lax.fori_loop(0, LAYERS, give_step, 0)
        s = hop(give.at[i], pair.at[i], pair_send.at[i], pair_recv.at[i], core_target)
        s.start()
        pending.append(s)
        lax.fori_loop(0, LAYERS, keep_step, 0)
        with jax.named_scope(f"pair{i}"):
            s.wait_recv()

        def pair_step(k, _):
            paired[i, k] = (keep[k].astype(F32) + pair[i, k].astype(F32)).astype(BF16)
            return 0

        lax.fori_loop(0, LAYERS, pair_step, 0)
        return span(kept % 2, chunk)

    def to_partner(i, k, place):
        landing = arrive.at[0, :, place] if k == 1 else joint.at[i, k - 2]
        return hop(paired.at[i, k], landing, back_send.at[i, k], back_recv.at[i, k], line[1])

    def to_layer(i, k, place):
        return hop(joint.at[i, k], arrive.at[1, :, place], joint_send.at[i, k], back_recv.at[i, 0], line[k + 2])

    places = []
    for i in range(step_count):
        place = chunk_sum(i)
        places.append(place)
        own_part[:, place] = paired[i, 0]

        @pl.when(inner == 0)
        def _():
            for k in (2, 3):
                to_partner(i, k, place).start()

        to_partner(i, 1, place).start()
        if i == 0:
            for block in down[1]:
                corners(4, *block)
    for i in range(step_count):
        place = places[i]

        @pl.when(inner == 1)
        def _():
            for k in range(2):
                with jax.named_scope(f"joint{i}{k}"):
                    to_partner(i, k + 2, place).wait_recv()
                joint[i, k] = (joint[i, k].astype(F32) + paired[i, k + 2].astype(F32)).astype(BF16)
                to_layer(i, k, place).start()

    for i in range(step_count):
        with jax.named_scope(f"near{i}"):
            to_partner(i, 1, places[i]).wait_recv()
    for i in range(step_count):
        with jax.named_scope(f"far{i}"):
            to_layer(i, 0, places[i]).wait_recv()
    total = own_part[...].astype(F32) + arrive[0].astype(F32) + arrive[1].astype(F32)
    out[...] = (after[:, mine_half].astype(F32) + total).astype(BF16)

    for c in pending + swaps + [core_hop(k) for k in range(1, LAYERS)] + [tok_copy]:
        c.wait_send()
    for a in range(N_SMALL, N_BIG):
        for k in range(1, LAYERS):
            z_hop(a, piece(a, z), fs, k, 1, k).wait_send()
    for i in range(step_count):
        to_partner(i, 1, places[i]).wait_send()

    @pl.when(inner == 0)
    def _():
        for i in range(step_count):
            for k in (2, 3):
                to_partner(i, k, places[i]).wait_send()

    @pl.when(inner == 1)
    def _():
        for a, slot in inner_pending:
            z_hop(a, arrays[a][0](fs), fs, slot, 0, 1).wait_send()
        for slot in range(1, LAYERS + 1):
            rows_hop(0, 0, slot, 1).wait_send()
        for i in range(step_count):
            for k in range(2):
                to_layer(i, k, places[i]).wait_send()


def fused_layer(
    tokens,
    mixer_norm_gain,
    recurrence_branch_weight,
    output_gate_projection,
    recurrence_conv_taps,
    recurrence_gate_map,
    input_gate_map,
    channel_decay_rate,
    position_log_decay,
    mixer_output_weight,
    feedforward_norm_gain,
    gate_up_weight,
    value_up_weight,
    gate_conv_taps,
    value_conv_taps,
    down_projection_weight,
):
    rows, half = tokens.shape
    deep, local_width = recurrence_branch_weight.shape
    wide = mixer_output_weight.shape[1]
    n_fs = LAYERS * PLANE
    features = 2 * half
    local_units = gate_up_weight.shape[1]
    units = local_units // LAYERS
    padded = -(-units // (2 * LANES)) * 2 * LANES
    head = recurrence_gate_map.shape[1]
    cw = min(local_width, 4 * head)
    chunk = PLANE * wide
    dma = pltpu.SemaphoreType.DMA
    scratch = [
        pltpu.VMEM((rows, features), BF16),
        pltpu.VMEM((n_fs * deep, 2 * local_width), BF16),
        pltpu.VMEM((local_width, n_fs * wide), BF16),
        pltpu.VMEM((deep, local_units), BF16),
        pltpu.VMEM((deep, local_units), BF16),
        pltpu.VMEM((LAYERS, deep, 2 * units), BF16),
        pltpu.VMEM((n_fs * deep, 2 * units), BF16),
        pltpu.VMEM((padded, n_fs * wide), BF16),
        pltpu.VMEM((LAYERS, 8, 2 * units), F32),
        pltpu.VMEM((local_width // cw, cw, 2 * cw), BF16),
        pltpu.VMEM((rows, local_width), F32),
        pltpu.VMEM((rows, features), BF16),
        pltpu.VMEM((rows, local_width), BF16),
        pltpu.VMEM((LAYERS, rows, chunk), BF16),
        pltpu.VMEM((LAYERS, rows, chunk), BF16),
        pltpu.VMEM((rows, features), BF16),
        pltpu.VMEM((LAYERS, rows, features), BF16),
        pltpu.VMEM((LAYERS, rows, padded), BF16),
        pltpu.VMEM((2, LAYERS, rows, chunk), BF16),
        pltpu.VMEM((LAYERS, rows, chunk), BF16),
        pltpu.VMEM((2, LAYERS, rows, chunk), BF16),
        pltpu.VMEM((2, LAYERS, rows, chunk), BF16),
        pltpu.VMEM((rows, half), BF16),
        pltpu.VMEM((2, rows, half), BF16),
        pltpu.VMEM((2, 2, rows, chunk), BF16),
        dma((N_BIG, 5, LAYERS)),
        dma((N_BIG, 5, LAYERS)),
        dma((N_BIG, LAYERS + 1)),
        dma((8,)),
        dma((2,)),
        dma((LAYERS,)),
        dma((LAYERS,)),
        dma((LAYERS + 1,)),
        dma((LAYERS,)),
        dma((LAYERS,)),
        dma((LAYERS,)),
        dma((2,)),
        dma((2,)),
        dma((2, LAYERS)),
        dma((2, LAYERS)),
        dma((2, 2)),
    ]
    return pl.pallas_call(
        layer_kernel,
        out_shape=jax.ShapeDtypeStruct((rows, half), BF16),
        in_specs=[ANY, VMEM, ANY, ANY, VMEM, VMEM, VMEM, VMEM, ANY, ANY, VMEM, ANY, ANY, VMEM, VMEM, ANY],
        out_specs=VMEM,
        scratch_shapes=scratch,
        compiler_params=pltpu.CompilerParams(
            collective_id=0, has_side_effects=True, vmem_limit_bytes=62 * 2**20
        ),
        name="layer",
    )(
        tokens,
        mixer_norm_gain,
        recurrence_branch_weight,
        output_gate_projection,
        recurrence_conv_taps,
        recurrence_gate_map,
        input_gate_map,
        channel_decay_rate.reshape(1, -1),
        position_log_decay,
        mixer_output_weight,
        feedforward_norm_gain,
        gate_up_weight,
        value_up_weight,
        gate_conv_taps,
        value_conv_taps,
        down_projection_weight,
    )


def solution(mesh):
    placed = (
        P("fs", "tp"),
        P(),
        P("fs", "tp"),
        P("fs", "tp"),
        P(None, "tp"),
        P("tp", None, None),
        P("tp", None, None),
        P("tp"),
        P("fs", "tp"),
        P("tp", "fs"),
        P(),
        P("fs", "tp"),
        P("fs", "tp"),
        P(None, "tp"),
        P(None, "tp"),
        P("tp", "fs"),
    )
    fused = mesh.shape["tp"] == 2 and mesh.shape["fs"] == LAYERS * PLANE
    body = fused_layer if fused else gathered_layer
    return jax.shard_map(
        body, mesh=mesh, in_specs=placed, out_specs=P("fs", "tp"), check_vma=False
    )
```

```python
import functools

import jax
import jax.numpy as jnp
from jax import lax
from jax.experimental import pallas as pl
from jax.experimental.pallas import tpu as pltpu
from jax.sharding import PartitionSpec as P

SEQ_LEN = 64


EPS = 1e-06
DECAY_RATE_GAIN = 8.0


def rms_normed(values, gain):
    wide = values.astype(jnp.float32)
    factor = lax.rsqrt(jnp.mean(wide * wide, axis=-1, keepdims=True) + EPS)
    return (wide * factor * gain.astype(jnp.float32)).astype(jnp.bfloat16)


def causal_conv(values, kernel):
    width = kernel.shape[0]
    row_count, channels = values.shape
    grouped = values.astype(jnp.float32).reshape(row_count // SEQ_LEN, SEQ_LEN, channels)
    padded = jnp.pad(grouped, ((0, 0), (width - 1, 0), (0, 0)))
    summed = padded[:, 0:SEQ_LEN] * kernel[0].astype(jnp.float32)
    for offset in range(1, width):
        summed = summed + padded[:, offset : offset + SEQ_LEN] * kernel[offset].astype(jnp.float32)
    return summed.reshape(row_count, channels)


def combine(left, right):
    first_a, first_b = left
    second_a, second_b = right
    return (first_a * second_a, second_a * first_b + second_b)


def pair_folder(normed, pieces):
    return (
        jnp.dot(normed, pieces[0], preferred_element_type=jnp.float32),
        jnp.dot(normed, pieces[1], preferred_element_type=jnp.float32),
    )


def gathered_layer(
    tokens,
    mixer_norm_gain,
    recurrence_branch_weight,
    output_gate_projection,
    recurrence_conv_taps,
    recurrence_gate_map,
    input_gate_map,
    channel_decay_rate,
    position_log_decay,
    mixer_output_weight,
    feedforward_norm_gain,
    gate_up_weight,
    value_up_weight,
    gate_conv_taps,
    value_conv_taps,
    down_projection_weight,
):
    row_count = tokens.shape[0]
    local_width = recurrence_branch_weight.shape[1]
    local_heads = recurrence_gate_map.shape[0]
    head_size = recurrence_gate_map.shape[1]
    whole_rows = lax.all_gather(tokens, "tp", axis=1, tiled=True)
    normed = rms_normed(whole_rows, mixer_norm_gain)
    branch_sum, outgate_sum = pair_folder(
        normed,
        (
            lax.all_gather(recurrence_branch_weight, "fs", axis=0, tiled=True),
            lax.all_gather(output_gate_projection, "fs", axis=0, tiled=True),
        ),
    )
    branch = branch_sum.astype(jnp.bfloat16)
    outgate = outgate_sum.astype(jnp.bfloat16)
    conv = causal_conv(branch, recurrence_conv_taps).astype(jnp.bfloat16)
    grouped = conv.reshape(row_count, local_heads, head_size)
    recurrence_scan = jax.nn.sigmoid(
        jnp.einsum(
            "rhi,hij->rhj", grouped, recurrence_gate_map, preferred_element_type=jnp.float32
        ).reshape(row_count, local_width)
    )
    inner = jax.nn.sigmoid(
        jnp.einsum(
            "rhi,hij->rhj", grouped, input_gate_map, preferred_element_type=jnp.float32
        ).reshape(row_count, local_width)
    )
    log_alpha = (
        -DECAY_RATE_GAIN * recurrence_scan * channel_decay_rate[None, :] + position_log_decay
    )
    drive = jnp.sqrt(-jnp.expm1(2.0 * log_alpha)) * inner * conv.astype(jnp.float32)
    shape3 = (row_count // SEQ_LEN, SEQ_LEN, local_width)
    unused, state = lax.associative_scan(
        combine, (jnp.exp(log_alpha).reshape(shape3), drive.reshape(shape3)), axis=1
    )
    state = state.reshape(row_count, local_width)
    mixed = (state * jax.nn.gelu(outgate.astype(jnp.float32))).astype(jnp.bfloat16)
    mixer_terms = jnp.dot(
        mixed,
        lax.all_gather(mixer_output_weight, "fs", axis=1, tiled=True),
        preferred_element_type=jnp.float32,
    )
    mixer_terms = mixer_terms.astype(jnp.bfloat16).astype(jnp.float32)
    mixer_whole = lax.psum(mixer_terms.astype(jnp.bfloat16), "tp").astype(jnp.float32)
    whole_after = (whole_rows.astype(jnp.float32) + mixer_whole).astype(jnp.bfloat16)
    normed2 = rms_normed(whole_after, feedforward_norm_gain)
    gate_whole, value_whole = (
        lax.all_gather(gate_up_weight, "fs", axis=0, tiled=True),
        lax.all_gather(value_up_weight, "fs", axis=0, tiled=True),
    )
    gate_sum = jnp.dot(normed2, gate_whole, preferred_element_type=jnp.float32)
    value_sum = jnp.dot(normed2, value_whole, preferred_element_type=jnp.float32)
    gate_half = gate_sum.astype(jnp.bfloat16)
    value_half = value_sum.astype(jnp.bfloat16)
    hidden = (
        jax.nn.silu(causal_conv(gate_half, gate_conv_taps))
        * causal_conv(value_half, value_conv_taps)
    ).astype(jnp.bfloat16)
    channel_terms = jnp.dot(
        hidden,
        lax.all_gather(down_projection_weight, "fs", axis=1, tiled=True),
        preferred_element_type=jnp.float32,
    )
    channel_terms = channel_terms.astype(jnp.bfloat16).astype(jnp.float32)
    channel_share = lax.psum_scatter(
        channel_terms.astype(jnp.bfloat16), "tp", scatter_dimension=1, tiled=True
    ).astype(jnp.float32)
    share_width = channel_share.shape[1]
    residual_share = lax.dynamic_slice_in_dim(
        whole_after, lax.axis_index("tp") * share_width, share_width, 1
    )
    return (residual_share.astype(jnp.float32) + channel_share).astype(jnp.bfloat16)


PLANE = 4
LAYERS = 4
LANES = 128
ANY = pl.BlockSpec(memory_space=pl.ANY)
VMEM = pl.BlockSpec(memory_space=pltpu.VMEM)
F32, BF16 = jnp.float32, jnp.bfloat16
N_SMALL, N_BIG = 3, 5


def hop(src, dst, send, recv, target):
    return pltpu.make_async_remote_copy(
        src_ref=src,
        dst_ref=dst,
        send_sem=send,
        recv_sem=recv,
        device_id=target,
        device_id_type=pl.DeviceIdType.MESH,
    )


def greet(targets):
    barrier = pltpu.get_barrier_semaphore()
    for target in targets:
        pl.semaphore_signal(
            barrier, inc=1, device_id=target, device_id_type=pl.DeviceIdType.MESH
        )
    pl.semaphore_wait(barrier, len(targets))


def span(index, size):
    return pl.ds(pl.multiple_of(index * size, size), size)


def row_blocks(whole, deep, columns):
    cut = deep * 3 // 4 // 16 * 16

    def at(f, part=None):
        if part is None:
            return whole.at[span(f, deep), columns]
        start, size = ((0, cut), (cut, deep - cut))[part]
        return whole.at[pl.ds(pl.multiple_of(f * deep + start, 16), size), columns]

    return at


def column_blocks(whole, rows, wide):
    cut = rows // 2 // 16 * 16

    def at(f, part=None):
        start, size = ((0, rows) if part is None else ((0, cut), (cut, rows - cut))[part])
        return whole.at[pl.ds(start, size), span(f, wide)]

    return at


def position(shape):
    return lax.broadcasted_iota(jnp.int32, shape, 0) % SEQ_LEN


def shifted(values, distance, place, fill):
    return jnp.where(place >= distance, pltpu.roll(values, distance, 0), fill)


def rows_conv(values, taps, width, place):
    summed = shifted(values, width - 1, place, 0.0) * taps[0:1, :]
    for j in range(1, width - 1):
        summed = summed + shifted(values, width - 1 - j, place, 0.0) * taps[j : j + 1, :]
    return summed + values * taps[width - 1 : width, :]


def negative_expm1(x):
    near = 1.0 + x * (1.0 / 8.0)
    for n in range(7, 1, -1):
        near = 1.0 + x * (1.0 / n) * near
    return jnp.where(jnp.abs(x) < 0.4, -x * near, 1.0 - jnp.exp(x))


def normed_rows(values, gain):
    factor = lax.rsqrt(jnp.mean(values * values, axis=-1, keepdims=True) + EPS)
    return (values * factor * gain).astype(BF16)


def gelu(x):
    return 0.5 * x * (1.0 + jnp.tanh(0.7978845608028654 * (x + 0.044715 * (x * x * x))))


def layer_kernel(
    tok, gain1, rb, og, ctaps, rmap, imap, rate, pld, mo, gain2, gup, vup, gtaps, vtaps, dn,
    out,
    tok2, bo_all, mo_all, gup_v, vup_v, stage, gu_all, dn_all, taps, gmap, pld_v,
    normed, mix_give, mix_keep, mix_pair, mix_out, mix_in, after, n2, hidden, give, pair, paired, arrive, joint, out_v,
    send, recv, z_send, local, misc, n2_send, n2_recv,
    core_send, core_recv, pair_send, pair_recv, back_send, back_recv, joint_send,
):
    fs, tp = lax.axis_index("fs"), lax.axis_index("tp")
    z, p = fs // PLANE, fs % PLANE
    y, x = p // 2, p % 2
    px, py = y * 2 + 1 - x, (1 - y) * 2 + x
    inner = ((z + 1) // 2) % 2
    layer = (z, z + 1 - 2 * (z % 2), 2 - z // 2, 3 - 3 * (z // 2))
    lands = (0, 1, 3 - inner, 3 - inner)
    down = (
        ((1 - inner, 1 + z // 2), (2, layer[2])),
        ((inner, 3 * (z // 2)), (3, layer[3])),
    )
    line = [(zz * PLANE + p, tp) for zz in layer]
    x_target, y_target = (z * PLANE + px, tp), (z * PLANE + py, tp)
    core_target = (fs, 1 - tp)
    with jax.named_scope("greet"):
        greet(line[1:] + [x_target, y_target, core_target])

    rows, half = tok.shape
    deep, local_width = rb.shape
    wide = mo.shape[1]
    units = dn.shape[0] // LAYERS
    full, rest = units // LANES, units % LANES
    cw = gmap.shape[1]
    mine_half, their_half, channels = span(tp, half), span(1 - tp, half), span(x, cw)
    heads, head = rmap.shape[:2]
    per = cw // head

    arrays = (
        (row_blocks(bo_all, deep, pl.ds(0, local_width)), rb),
        (row_blocks(bo_all, deep, pl.ds(local_width, local_width)), og),
        (column_blocks(mo_all, mo.shape[0], wide), mo),
        (row_blocks(gu_all, deep, slice(None)), None),
        (column_blocks(dn_all, units, wide), None),
    )

    def piece(a, zz):
        if a < N_SMALL:
            return arrays[a][1]
        return stage.at[zz] if a == 3 else dn.at[span(zz, units), :]

    pending = []
    inner_pending = []

    def misc_hop(n, source, to, target):
        return hop(source, to, misc.at[2 * n], misc.at[2 * n + 1], target)

    def mixer_part(a, f, h):
        if a < 2:
            columns = pl.ds(pl.multiple_of(a * local_width + h * cw, cw), cw)
            return bo_all.at[span(f, deep), columns]
        return mo_all.at[span(h, cw), span(f, wide)]

    def own_part_of(a, h):
        return mo.at[span(h, cw), :] if a == 2 else arrays[a][1].at[:, span(h, cw)]

    def z_hop(a, source, f, slot, land, to):
        return hop(source, arrays[a][0](f), z_send.at[a, slot], recv.at[a, 0, land], line[to])

    def sides(a, k, of=None):
        at = arrays[a][0]
        f = (layer[k] if of is None else of) * PLANE + p
        source = piece(a, z) if of is None and k == 0 else at(f)
        for kind, target in ((1, x_target), (2, y_target)):
            c = hop(source, at(f), send.at[a, kind, k], recv.at[a, kind, k], target)
            c.start()
            pending.append(c)

    def mixer_sides(a, k):
        f = layer[k] * PLANE + p
        for kind, h, target in ((1, 1 - x, x_target), (2, x, y_target)):
            to = mixer_part(a, f, h)
            c = hop(own_part_of(a, h) if k == 0 else to, to, send.at[a, kind, k], recv.at[a, kind, k], target)
            c.start()
            pending.append(c)

    def mixer_hop(a, k, kind, owner, target):
        block = mixer_part(a, layer[k] * PLANE + owner, x)
        return hop(block, block, send.at[a, kind, k], recv.at[a, kind, k], target)

    def mixer_corner(a, k):
        with jax.named_scope(f"side{a}{k}"):
            mixer_hop(a, k, 1, px, x_target).wait_recv()
        c = mixer_hop(a, k, 3, px, y_target)
        c.start()
        pending.append(c)

    def mixer_done(a, k):
        with jax.named_scope(f"corner{a}{k}"):
            mixer_hop(a, k, 2, py, y_target).wait_recv()
            mixer_hop(a, k, 3, PLANE - 1 - p, y_target).wait_recv()

    def corners(a, k, of=None):
        at = arrays[a][0]
        base = (layer[k] if of is None else of) * PLANE
        for kind, part, owner, target in ((1, 0, px, y_target), (2, 1, py, x_target)):
            whole = at(base + owner)
            with jax.named_scope(f"side{a}{k if of is None else 9}{kind}"):
                hop(whole, whole, send.at[a, kind, k], recv.at[a, kind, k], target).wait_recv()
            block = at(base + owner, part)
            c = hop(block, block, send.at[a, kind + 2, k], recv.at[a, kind + 2, k], target)
            c.start()
            pending.append(c)

    def corners_done(a, k, of=None):
        at = arrays[a][0]
        corner = (layer[k] if of is None else of) * PLANE + (PLANE - 1 - p)
        for kind, part, target in ((1, 0, y_target), (2, 1, x_target)):
            block = at(corner, part)
            with jax.named_scope(f"corner{a}{k if of is None else 9}{kind}"):
                hop(block, block, send.at[a, kind + 2, k], recv.at[a, kind + 2, k], target).wait_recv()

    def z_done(a, k):
        block = arrays[a][0](layer[k] * PLANE + p)
        with jax.named_scope(f"z{a}{k}"):
            hop(block, block, z_send.at[a, 0], recv.at[a, 0, k], line[k]).wait_recv()

    @pl.when(inner == 1)
    def _():
        for a in range(N_SMALL):
            z_hop(a, piece(a, z), fs, 1, 2, 2).start()

    for a in range(N_SMALL):
        c = z_hop(a, piece(a, z), fs, 0, 1, 1)
        c.start()
        pending.append(c)
    inner_pending += [(a, 1) for a in range(N_SMALL)]
    for a in range(N_SMALL):
        mixer_sides(a, 0)
    tok_swap = misc_hop(0, tok, tok2.at[0, :, mine_half], core_target)
    tok_x = misc_hop(1, tok, tok2.at[1, :, mine_half], x_target)
    pld_x = misc_hop(2, pld.at[:, span(1 - x, cw)], pld_v.at[1], x_target)
    tok_swap.start()
    pld_x.start()
    pending += [tok_swap, tok_x, pld_x]

    own = [
        pltpu.make_async_copy(gup, gup_v, local.at[0]),
        pltpu.make_async_copy(vup, vup_v, local.at[1]),
        pltpu.make_async_copy(tok, tok2.at[0, :, mine_half], local.at[2]),
        pltpu.make_async_copy(pld.at[:, channels], pld_v.at[0], local.at[3]),
        pltpu.make_async_copy(rb, arrays[0][0](fs), local.at[4]),
        pltpu.make_async_copy(og, arrays[1][0](fs), local.at[5]),
        pltpu.make_async_copy(mo, arrays[2][0](fs), local.at[6]),
        pltpu.make_async_copy(piece(4, z), arrays[4][0](fs), local.at[7]),
    ]
    for c in own:
        c.start()

    own[0].wait()
    own[1].wait()

    def arrange(gate, value, zz, store):
        for j in range(full):
            at = zz * units + j * LANES
            store(2 * j * LANES, gate[:, at : at + LANES])
            store((2 * j + 1) * LANES, value[:, at : at + LANES])
        if rest:
            at = zz * units + full * LANES
            store(2 * full * LANES, gate[:, at : at + rest])
            store(2 * full * LANES + rest, value[:, at : at + rest])

    for zz in range(LAYERS):

        def put(at, v, zz=zz):
            stage[zz, :, at : at + v.shape[1]] = v

        def put_taps(at, v, zz=zz):
            taps[zz, 0 : v.shape[0], at : at + v.shape[1]] = v.astype(F32)

        arrange(gup_v, vup_v, zz, put)
        arrange(gtaps, vtaps, zz, put_taps)
    gu_all[span(fs, deep), :] = stage[z]
    dn_all[units:, :] = jnp.zeros((dn_all.shape[0] - units, dn_all.shape[1]), BF16)
    gmap[...] = jnp.zeros(gmap.shape, BF16)
    for c in range(heads // per):
        for h in range(per):
            r = slice(h * head, (h + 1) * head)
            gmap[c, r, h * head : (h + 1) * head] = rmap[c * per + h]
            gmap[c, r, cw + h * head : cw + (h + 1) * head] = imap[c * per + h]

    def relay(k, to, land, slot):
        @pl.when(inner == 1)
        def _():
            for a in range(N_SMALL):
                f = layer[k] * PLANE + p
                z_hop(a, arrays[a][0](f), f, slot, land, to).start()

        inner_pending.extend((a, slot) for a in range(N_SMALL))

    def ffn_along_z(where):
        @pl.when(inner == where)
        def _():
            for a in range(N_SMALL, N_BIG):
                for k in range(1, LAYERS):
                    z_hop(a, piece(a, layer[k]), fs, k, lands[k], k).start()

    for k, to, land in ((1, 2, 3), (2, 1, 2), (3, 1, 3)):
        for a in range(N_SMALL):
            z_done(a, k)
        relay(k, to, land, k + 1)
        if k > 1:
            ffn_along_z(k - 2)
        for a in range(N_SMALL):
            mixer_sides(a, k)
        if k == 1:
            tok_x.start()
        for a in range(N_SMALL):
            mixer_corner(a, k - 1)
    with jax.named_scope("tok_x"):
        tok_x.wait_recv()
    block = tok2.at[1, :, mine_half]
    tok_core = misc_hop(3, block, block, core_target)
    tok_core.start()
    pending.append(tok_core)
    for a in range(N_SMALL):
        mixer_corner(a, LAYERS - 1)
    sides(3, 0)

    with jax.named_scope("tokens"):
        tok_swap.wait_recv()
        tok_core.wait_recv()
        pld_x.wait_recv()
        own[2].wait()

    def norm_step(r, _):
        normed[r] = normed_rows(tok2[r].astype(F32), gain1[...].astype(F32)[None, :])
        return 0

    lax.fori_loop(0, 2, norm_step, 0)
    for c in own[3:]:
        c.wait()
    for k in range(LAYERS):
        for a in range(N_SMALL):
            mixer_done(a, k)

    def mixer_rows(r, _):
        place = position((rows, cw))
        branch = jnp.dot(normed[r], bo_all[:, channels], preferred_element_type=F32)
        branch = branch.astype(BF16).astype(F32)
        conv = rows_conv(branch, ctaps[:, channels].astype(F32), ctaps.shape[0], place).astype(BF16)
        gates = jax.nn.sigmoid(jnp.dot(conv, gmap[x], preferred_element_type=F32))
        la = -DECAY_RATE_GAIN * gates[:, :cw] * rate[:, channels] + pld_v[r]
        d = jnp.sqrt(negative_expm1(2.0 * la)) * gates[:, cw:] * conv.astype(F32)
        a = jnp.exp(la)
        step = 1
        while step < SEQ_LEN:
            d = a * shifted(d, step, place, 0.0) + d
            if step * 2 < SEQ_LEN:
                a = a * shifted(a, step, place, 1.0)
            step *= 2
        outgate = jnp.dot(
            normed[r],
            bo_all[:, pl.ds(pl.multiple_of(local_width + x * cw, cw), cw)],
            preferred_element_type=F32,
        )
        outgate = outgate.astype(BF16).astype(F32)
        mixed = (d * gelu(outgate)).astype(BF16)
        mix_give[r] = jnp.dot(mixed, mo_all[channels, their_half], preferred_element_type=F32).astype(BF16)
        mix_keep[r] = jnp.dot(mixed, mo_all[channels, mine_half], preferred_element_type=F32)
        return 0

    def mix_hop(r):
        return misc_hop(4 + r, mix_give.at[r], mix_pair.at[r], core_target)

    with jax.named_scope("mixer1"):
        lax.fori_loop(1, 2, mixer_rows, 0)
    mix_hop(1).start()
    with jax.named_scope("mixer0"):
        lax.fori_loop(0, 1, mixer_rows, 0)
    mix_hop(0).start()
    with jax.named_scope("swap1"):
        mix_hop(1).wait_recv()
    mix_out[...] = (mix_keep[1] + mix_pair[1].astype(F32)).astype(BF16)
    mix_x = misc_hop(6, mix_out, mix_in, x_target)
    mix_x.start()
    for k in range(1, LAYERS):
        z_done(3, k)
        sides(3, k)
    with jax.named_scope("swap0"):
        mix_hop(0).wait_recv()
    mix_keep[0] = mix_keep[0] + mix_pair[0].astype(F32) + tok2[0, :, mine_half].astype(F32)
    with jax.named_scope("mix_x"):
        mix_x.wait_recv()
    after[:, mine_half] = (mix_keep[0] + mix_in[...].astype(F32)).astype(BF16)
    after_core = misc_hop(7, after.at[:, mine_half], after.at[:, mine_half], core_target)
    after_core.start()
    pending += [mix_hop(0), mix_hop(1), mix_x, after_core]
    corners(3, 0)
    with jax.named_scope("after"):
        after_core.wait_recv()
    n2[0] = normed_rows(after[...].astype(F32), gain2[...].astype(F32)[None, :])


    def rows_hop(k, land, slot, to):
        return hop(
            n2.at[k, :, mine_half], n2.at[land, :, mine_half], n2_send.at[slot], n2_recv.at[land], line[to]
        )

    @pl.when(inner == 1)
    def _():
        rows_hop(0, 2, 1, 2).start()

    c = rows_hop(0, 1, 0, 1)
    c.start()
    pending.append(c)

    def rows_arrived(k, to, land):
        with jax.named_scope(f"rows{k}"):
            rows_hop(k, k, 0, 1).wait_recv()

        @pl.when(inner == 1)
        def _():
            rows_hop(k, land, k + 1, to).start()

        core_hop(k).start()

    def core_hop(k):
        block = n2.at[k, :, mine_half]
        return hop(block, block, core_send.at[k], core_recv.at[k], core_target)

    corners(3, 1)
    rows_arrived(1, 2, 3)
    corners(3, 2)
    rows_arrived(2, 1, 2)
    corners(3, 3)
    z_done(4, 1)
    z_done(4, 2)
    down_a, down_b = down[0]

    @pl.when(inner == 1)
    def _():
        rows_arrived(3, 1, 3)

    sides(4, *down_a)
    sides(4, *down_b)

    def up(k):
        place = position((rows, 4 * LANES))
        layer_taps = taps.at[z]
        width = gtaps.shape[0]
        j = 0
        while j < 2 * full * LANES:
            n = min(4 * LANES, 2 * full * LANES - j)
            s = jnp.dot(n2[k], gu_all[:, j : j + n], preferred_element_type=F32)
            s = rows_conv(s.astype(BF16).astype(F32), layer_taps[0:width, j : j + n], width, place[:, :n])
            for i in range(0, n, 2 * LANES):
                g, v = s[:, i : i + LANES], s[:, i + LANES : i + 2 * LANES]
                h = (j + i) // 2
                hidden[k, :, h : h + LANES] = (g * jax.nn.sigmoid(g) * v).astype(BF16)
            j += n
        if rest:
            s = jnp.dot(n2[k], gu_all[:, j:], preferred_element_type=F32)
            s = rows_conv(s.astype(BF16).astype(F32), layer_taps[0:width, j:], width, place[:, :LANES])
            h = s * jax.nn.sigmoid(s) * pltpu.roll(s, rest, 1)
            lane = lax.broadcasted_iota(jnp.int32, h.shape, 1)
            hidden[k, :, full * LANES : (full + 1) * LANES] = jnp.where(lane < rest, h, 0.0).astype(BF16)

    def up_step(k, _):
        with jax.named_scope("up"):
            up(k)
        return 0

    turn = (tp + z // 2) % 2
    quarter = PLANE * wide // 2

    def columns_of(j, mine):
        first, second = down[j // 2][0][1], down[j // 2][1][1]
        side = turn if mine else 1 - turn
        block = first * (1 - side) + second * side
        return block * 2 + (y if j % 2 == 0 else 1 - y)

    def place_of(j):
        return columns_of(j, True) % (half // quarter)

    def pair_hop(j, k):
        return hop(give.at[j, k], pair.at[j, k], pair_send.at[j, k], pair_recv.at[j, k], core_target)

    def to_partner(j, k):
        landing = arrive.at[0, j] if k == 1 else joint.at[j, k - 2]
        return hop(paired.at[j, k], landing, back_send.at[j, k], back_recv.at[j, k], line[1])

    def to_layer(j, k):
        return hop(joint.at[j, k], arrive.at[1, j], joint_send.at[j, k], back_recv.at[j, 0], line[k + 2])

    def part_sums(j, slots):
        given, kept = span(columns_of(j, False), quarter), span(columns_of(j, True), quarter)
        for k in slots:
            give[j, k] = jnp.dot(hidden[k], dn_all[:, given], preferred_element_type=F32).astype(BF16)
            pair_hop(j, k).start()
        for k in slots:
            keep = jnp.dot(hidden[k], dn_all[:, kept], preferred_element_type=F32)
            with jax.named_scope(f"pair{j}{k}"):
                pair_hop(j, k).wait_recv()
            paired[j, k] = (keep + pair[j, k].astype(F32)).astype(BF16)
            if k > 1:

                @pl.when(inner == 0)
                def _():
                    to_partner(j, k).start()

            elif k == 1:
                to_partner(j, 1).start()

    def joint_sums(j, k):
        @pl.when(inner == 1)
        def _():
            with jax.named_scope(f"joint{j}{k}"):
                to_partner(j, k + 2).wait_recv()
            joint[j, k] = (joint[j, k].astype(F32) + paired[j, k + 2].astype(F32)).astype(BF16)
            to_layer(j, k).start()

    for k in range(LAYERS):
        corners_done(3, k)
    with jax.named_scope("across12"):
        core_hop(1).wait_recv()
        core_hop(2).wait_recv()
    lax.fori_loop(1, 3, up_step, 0)
    corners(4, *down_a)
    corners(4, *down_b)
    z_done(4, 3)
    for block in down[1]:
        sides(4, *block)
    part_sums(0, (2, 1))
    for block in down[0]:
        corners_done(4, *block)
    part_sums(1, (2, 1))

    @pl.when(inner == 0)
    def _():
        rows_arrived(3, 1, 3)

    with jax.named_scope("across3"):
        core_hop(3).wait_recv()
    lax.fori_loop(3, 4, up_step, 0)
    part_sums(0, (3,))
    part_sums(1, (3,))
    corners(4, *down[1][0])
    joint_sums(0, 0)
    lax.fori_loop(0, 1, up_step, 0)
    corners(4, *down[1][1])
    joint_sums(1, 0)
    part_sums(2, (3, 2, 1))
    joint_sums(0, 1)
    for block in down[1]:
        corners_done(4, *block)
    part_sums(3, (3, 2, 1))
    joint_sums(1, 1)
    for j in range(LAYERS):
        part_sums(j, (0,))
    for j in (2, 3):
        for k in (1, 0):
            joint_sums(j, k)

    stores = []
    for j in range(LAYERS):
        with jax.named_scope(f"near{j}"):
            to_partner(j, 1).wait_recv()
        with jax.named_scope(f"far{j}"):
            to_layer(j, 0).wait_recv()
        total = paired[j, 0].astype(F32) + arrive[0, j].astype(F32) + arrive[1, j].astype(F32)
        first = pl.multiple_of(tp * half + place_of(j) * quarter, quarter)
        out_v[j] = (after[:, pl.ds(first, quarter)].astype(F32) + total).astype(BF16)
        stores.append(pltpu.make_async_copy(out_v.at[j], out.at[:, span(place_of(j), quarter)], local.at[j]))
        stores[j].start()

    for c in pending + [core_hop(k) for k in range(1, LAYERS)]:
        c.wait_send()
    for a in range(N_SMALL, N_BIG):
        for k in range(1, LAYERS):
            z_hop(a, piece(a, z), fs, k, 1, k).wait_send()
    for j in range(LAYERS):
        to_partner(j, 1).wait_send()
        for k in range(LAYERS):
            pair_hop(j, k).wait_send()

    @pl.when(inner == 0)
    def _():
        for j in range(LAYERS):
            for k in (2, 3):
                to_partner(j, k).wait_send()

    @pl.when(inner == 1)
    def _():
        for a, slot in inner_pending:
            z_hop(a, arrays[a][0](fs), fs, slot, 0, 1).wait_send()
        for slot in range(1, LAYERS + 1):
            rows_hop(0, 0, slot, 1).wait_send()
        for j in range(LAYERS):
            for k in range(2):
                to_layer(j, k).wait_send()

    for c in stores:
        c.wait()


def fused_layer(
    tokens,
    mixer_norm_gain,
    recurrence_branch_weight,
    output_gate_projection,
    recurrence_conv_taps,
    recurrence_gate_map,
    input_gate_map,
    channel_decay_rate,
    position_log_decay,
    mixer_output_weight,
    feedforward_norm_gain,
    gate_up_weight,
    value_up_weight,
    gate_conv_taps,
    value_conv_taps,
    down_projection_weight,
):
    rows, half = tokens.shape
    deep, local_width = recurrence_branch_weight.shape
    wide = mixer_output_weight.shape[1]
    n_fs = LAYERS * PLANE
    features = 2 * half
    local_units = gate_up_weight.shape[1]
    units = local_units // LAYERS
    padded = -(-units // (2 * LANES)) * 2 * LANES
    cw = local_width // 2
    quarter = PLANE * wide // 2
    dma = pltpu.SemaphoreType.DMA
    scratch = [
        pltpu.VMEM((2, rows, features), BF16),
        pltpu.VMEM((n_fs * deep, 2 * local_width), BF16),
        pltpu.VMEM((local_width, n_fs * wide), BF16),
        pltpu.VMEM((deep, local_units), BF16),
        pltpu.VMEM((deep, local_units), BF16),
        pltpu.VMEM((LAYERS, deep, 2 * units), BF16),
        pltpu.VMEM((n_fs * deep, 2 * units), BF16),
        pltpu.VMEM((padded, n_fs * wide), BF16),
        pltpu.VMEM((LAYERS, 8, 2 * units), F32),
        pltpu.VMEM((local_width // cw, cw, 2 * cw), BF16),
        pltpu.VMEM((2, rows, cw), F32),
        pltpu.VMEM((2, rows, features), BF16),
        pltpu.VMEM((2, rows, half), BF16),
        pltpu.VMEM((2, rows, half), F32),
        pltpu.VMEM((2, rows, half), BF16),
        pltpu.VMEM((rows, half), BF16),
        pltpu.VMEM((rows, half), BF16),
        pltpu.VMEM((rows, features), BF16),
        pltpu.VMEM((LAYERS, rows, features), BF16),
        pltpu.VMEM((LAYERS, rows, padded), BF16),
        pltpu.VMEM((LAYERS, LAYERS, rows, quarter), BF16),
        pltpu.VMEM((LAYERS, LAYERS, rows, quarter), BF16),
        pltpu.VMEM((LAYERS, LAYERS, rows, quarter), BF16),
        pltpu.VMEM((2, LAYERS, rows, quarter), BF16),
        pltpu.VMEM((LAYERS, 2, rows, quarter), BF16),
        pltpu.VMEM((LAYERS, rows, quarter), BF16),
        dma((N_BIG, 5, LAYERS)),
        dma((N_BIG, 5, LAYERS)),
        dma((N_BIG, LAYERS + 1)),
        dma((8,)),
        dma((16,)),
        dma((LAYERS + 1,)),
        dma((LAYERS,)),
        dma((LAYERS,)),
        dma((LAYERS,)),
        dma((LAYERS, LAYERS)),
        dma((LAYERS, LAYERS)),
        dma((LAYERS, LAYERS)),
        dma((LAYERS, LAYERS)),
        dma((LAYERS, 2)),
    ]
    return pl.pallas_call(
        layer_kernel,
        out_shape=jax.ShapeDtypeStruct((rows, half), BF16),
        in_specs=[ANY, VMEM, ANY, ANY, VMEM, VMEM, VMEM, VMEM, ANY, ANY, VMEM, ANY, ANY, VMEM, VMEM, ANY],
        out_specs=ANY,
        scratch_shapes=scratch,
        compiler_params=pltpu.CompilerParams(
            collective_id=0, has_side_effects=True, vmem_limit_bytes=62 * 2**20
        ),
        name="layer",
    )(
        tokens,
        mixer_norm_gain,
        recurrence_branch_weight,
        output_gate_projection,
        recurrence_conv_taps,
        recurrence_gate_map,
        input_gate_map,
        channel_decay_rate.reshape(1, -1),
        position_log_decay,
        mixer_output_weight,
        feedforward_norm_gain,
        gate_up_weight,
        value_up_weight,
        gate_conv_taps,
        value_conv_taps,
        down_projection_weight,
    )


def solution(mesh):
    placed = (
        P("fs", "tp"),
        P(),
        P("fs", "tp"),
        P("fs", "tp"),
        P(None, "tp"),
        P("tp", None, None),
        P("tp", None, None),
        P("tp"),
        P("fs", "tp"),
        P("tp", "fs"),
        P(),
        P("fs", "tp"),
        P("fs", "tp"),
        P(None, "tp"),
        P(None, "tp"),
        P("tp", "fs"),
    )
    fused = mesh.shape["tp"] == 2 and mesh.shape["fs"] == LAYERS * PLANE
    body = fused_layer if fused else gathered_layer
    return jax.shard_map(
        body, mesh=mesh, in_specs=placed, out_specs=P("fs", "tp"), check_vma=False
    )
```

```python
import functools

import jax
import jax.numpy as jnp
from jax import lax
from jax.experimental import pallas as pl
from jax.experimental.pallas import tpu as pltpu
from jax.sharding import PartitionSpec as P

SEQ_LEN = 64


EPS = 1e-06
DECAY_RATE_GAIN = 8.0


def rms_normed(values, gain):
    wide = values.astype(jnp.float32)
    factor = lax.rsqrt(jnp.mean(wide * wide, axis=-1, keepdims=True) + EPS)
    return (wide * factor * gain.astype(jnp.float32)).astype(jnp.bfloat16)


def causal_conv(values, kernel):
    width = kernel.shape[0]
    row_count, channels = values.shape
    grouped = values.astype(jnp.float32).reshape(row_count // SEQ_LEN, SEQ_LEN, channels)
    padded = jnp.pad(grouped, ((0, 0), (width - 1, 0), (0, 0)))
    summed = padded[:, 0:SEQ_LEN] * kernel[0].astype(jnp.float32)
    for offset in range(1, width):
        summed = summed + padded[:, offset : offset + SEQ_LEN] * kernel[offset].astype(jnp.float32)
    return summed.reshape(row_count, channels)


def combine(left, right):
    first_a, first_b = left
    second_a, second_b = right
    return (first_a * second_a, second_a * first_b + second_b)


def pair_folder(normed, pieces):
    return (
        jnp.dot(normed, pieces[0], preferred_element_type=jnp.float32),
        jnp.dot(normed, pieces[1], preferred_element_type=jnp.float32),
    )


def gathered_layer(
    tokens,
    mixer_norm_gain,
    recurrence_branch_weight,
    output_gate_projection,
    recurrence_conv_taps,
    recurrence_gate_map,
    input_gate_map,
    channel_decay_rate,
    position_log_decay,
    mixer_output_weight,
    feedforward_norm_gain,
    gate_up_weight,
    value_up_weight,
    gate_conv_taps,
    value_conv_taps,
    down_projection_weight,
):
    row_count = tokens.shape[0]
    local_width = recurrence_branch_weight.shape[1]
    local_heads = recurrence_gate_map.shape[0]
    head_size = recurrence_gate_map.shape[1]
    whole_rows = lax.all_gather(tokens, "tp", axis=1, tiled=True)
    normed = rms_normed(whole_rows, mixer_norm_gain)
    branch_sum, outgate_sum = pair_folder(
        normed,
        (
            lax.all_gather(recurrence_branch_weight, "fs", axis=0, tiled=True),
            lax.all_gather(output_gate_projection, "fs", axis=0, tiled=True),
        ),
    )
    branch = branch_sum.astype(jnp.bfloat16)
    outgate = outgate_sum.astype(jnp.bfloat16)
    conv = causal_conv(branch, recurrence_conv_taps).astype(jnp.bfloat16)
    grouped = conv.reshape(row_count, local_heads, head_size)
    recurrence_scan = jax.nn.sigmoid(
        jnp.einsum(
            "rhi,hij->rhj", grouped, recurrence_gate_map, preferred_element_type=jnp.float32
        ).reshape(row_count, local_width)
    )
    inner = jax.nn.sigmoid(
        jnp.einsum(
            "rhi,hij->rhj", grouped, input_gate_map, preferred_element_type=jnp.float32
        ).reshape(row_count, local_width)
    )
    log_alpha = (
        -DECAY_RATE_GAIN * recurrence_scan * channel_decay_rate[None, :] + position_log_decay
    )
    drive = jnp.sqrt(-jnp.expm1(2.0 * log_alpha)) * inner * conv.astype(jnp.float32)
    shape3 = (row_count // SEQ_LEN, SEQ_LEN, local_width)
    unused, state = lax.associative_scan(
        combine, (jnp.exp(log_alpha).reshape(shape3), drive.reshape(shape3)), axis=1
    )
    state = state.reshape(row_count, local_width)
    mixed = (state * jax.nn.gelu(outgate.astype(jnp.float32))).astype(jnp.bfloat16)
    mixer_terms = jnp.dot(
        mixed,
        lax.all_gather(mixer_output_weight, "fs", axis=1, tiled=True),
        preferred_element_type=jnp.float32,
    )
    mixer_terms = mixer_terms.astype(jnp.bfloat16).astype(jnp.float32)
    mixer_whole = lax.psum(mixer_terms.astype(jnp.bfloat16), "tp").astype(jnp.float32)
    whole_after = (whole_rows.astype(jnp.float32) + mixer_whole).astype(jnp.bfloat16)
    normed2 = rms_normed(whole_after, feedforward_norm_gain)
    gate_whole, value_whole = (
        lax.all_gather(gate_up_weight, "fs", axis=0, tiled=True),
        lax.all_gather(value_up_weight, "fs", axis=0, tiled=True),
    )
    gate_sum = jnp.dot(normed2, gate_whole, preferred_element_type=jnp.float32)
    value_sum = jnp.dot(normed2, value_whole, preferred_element_type=jnp.float32)
    gate_half = gate_sum.astype(jnp.bfloat16)
    value_half = value_sum.astype(jnp.bfloat16)
    hidden = (
        jax.nn.silu(causal_conv(gate_half, gate_conv_taps))
        * causal_conv(value_half, value_conv_taps)
    ).astype(jnp.bfloat16)
    channel_terms = jnp.dot(
        hidden,
        lax.all_gather(down_projection_weight, "fs", axis=1, tiled=True),
        preferred_element_type=jnp.float32,
    )
    channel_terms = channel_terms.astype(jnp.bfloat16).astype(jnp.float32)
    channel_share = lax.psum_scatter(
        channel_terms.astype(jnp.bfloat16), "tp", scatter_dimension=1, tiled=True
    ).astype(jnp.float32)
    share_width = channel_share.shape[1]
    residual_share = lax.dynamic_slice_in_dim(
        whole_after, lax.axis_index("tp") * share_width, share_width, 1
    )
    return (residual_share.astype(jnp.float32) + channel_share).astype(jnp.bfloat16)


PLANE = 4
LAYERS = 4
LANES = 128
ANY = pl.BlockSpec(memory_space=pl.ANY)
VMEM = pl.BlockSpec(memory_space=pltpu.VMEM)
F32, BF16 = jnp.float32, jnp.bfloat16
N_SMALL, N_BIG = 3, 5
ROWS_CUT = 6
MISC_HALVES = 15
N_SENT = 13
AT_Z = 0
AT_MIX = AT_Z + N_BIG * LAYERS
AT_MIX_DONE = AT_MIX + N_SMALL * LAYERS
AT_SIDE = AT_MIX_DONE + 2
AT_CORNER = AT_SIDE + 2 * 2 * LAYERS
AT_MISC = AT_CORNER + 2 * 2 * 2
AT_ROWS = AT_MISC + 8
AT_CORE = AT_ROWS + LAYERS
AT_PAIR = AT_CORE + LAYERS
AT_BACK = AT_PAIR + LAYERS * LAYERS


def hop(src, dst, send, recv, target):
    return pltpu.make_async_remote_copy(
        src_ref=src,
        dst_ref=dst,
        send_sem=send,
        recv_sem=recv,
        device_id=target,
        device_id_type=pl.DeviceIdType.MESH,
    )


def greet(targets):
    barrier = pltpu.get_barrier_semaphore()
    for target in targets:
        pl.semaphore_signal(
            barrier, inc=1, device_id=target, device_id_type=pl.DeviceIdType.MESH
        )
    pl.semaphore_wait(barrier, len(targets))


def span(index, size):
    return pl.ds(pl.multiple_of(index * size, size), size)


def row_blocks(whole, deep, columns):
    cut = ROWS_CUT * deep // 8

    def at(f, part=None):
        if part is None:
            return whole.at[span(f, deep), columns]
        start, size = ((0, cut), (cut, deep - cut))[part]
        return whole.at[pl.ds(pl.multiple_of(f * deep + start, 16), size), columns]

    return at


def column_blocks(whole, rows, wide):
    cut = rows // 2 // 16 * 16

    def at(f, part=None):
        start, size = ((0, rows) if part is None else ((0, cut), (cut, rows - cut))[part])
        return whole.at[pl.ds(start, size), span(f, wide)]

    return at


def position(shape):
    return lax.broadcasted_iota(jnp.int32, shape, 0) % SEQ_LEN


def shifted(values, distance, place, fill):
    return jnp.where(place >= distance, pltpu.roll(values, distance, 0), fill)


def rows_conv(values, taps, width, place):
    summed = shifted(values, width - 1, place, 0.0) * taps[0:1, :]
    for j in range(1, width - 1):
        summed = summed + shifted(values, width - 1 - j, place, 0.0) * taps[j : j + 1, :]
    return summed + values * taps[width - 1 : width, :]


def negative_expm1(x):
    near = 1.0 + x * (1.0 / 8.0)
    for n in range(7, 1, -1):
        near = 1.0 + x * (1.0 / n) * near
    return jnp.where(jnp.abs(x) < 0.4, -x * near, 1.0 - jnp.exp(x))


def normed_rows(values, gain):
    factor = lax.rsqrt(jnp.mean(values * values, axis=-1, keepdims=True) + EPS)
    return (values * factor * gain).astype(BF16)


def gelu(x):
    return 0.5 * x * (1.0 + jnp.tanh(0.7978845608028654 * (x + 0.044715 * (x * x * x))))


def layer_kernel(
    tok, gain1, rb, og, ctaps, rmap, imap, rate, pld, mo, gain2, gup, vup, gtaps, vtaps, dn,
    out,
    tok2, bo_all, mo_all, gup_v, vup_v, stage, gu_all, dn_all, taps, gmap, pld_v,
    normed, mix_give, mix_keep, mix_pair, mix_out, mix_in, after, n2, hidden, give, pair, paired, arrive, joint, out_v, part,
    sent, got, local,
):
    fs, tp = lax.axis_index("fs"), lax.axis_index("tp")
    z, p = fs // PLANE, fs % PLANE
    y, x = p // 2, p % 2
    px, py = y * 2 + 1 - x, (1 - y) * 2 + x
    inner = ((z + 1) // 2) % 2
    layer = (z, z + 1 - 2 * (z % 2), 2 - z // 2, 3 - 3 * (z // 2))
    lands = (0, 1, 3 - inner, 3 - inner)
    down = (
        ((1 - inner, 1 + z // 2), (2, layer[2])),
        ((inner, 3 * (z // 2)), (3, layer[3])),
    )
    line = [(zz * PLANE + p, tp) for zz in layer]
    x_target, y_target = (z * PLANE + px, tp), (z * PLANE + py, tp)
    core_target = (fs, 1 - tp)
    with jax.named_scope("greet"):
        greet(line[1:] + [x_target, y_target, core_target])

    rows, half = tok.shape
    deep, local_width = rb.shape
    wide = mo.shape[1]
    units = dn.shape[0] // LAYERS
    full, rest = units // LANES, units % LANES
    cw = gmap.shape[1]
    mine_half, their_half, channels = span(tp, half), span(1 - tp, half), span(x, cw)
    heads, head = rmap.shape[:2]
    per = cw // head

    arrays = (
        (row_blocks(bo_all, deep, pl.ds(0, local_width)), rb),
        (row_blocks(bo_all, deep, pl.ds(local_width, local_width)), og),
        (column_blocks(mo_all, mo.shape[0], wide), mo),
        (row_blocks(gu_all, deep, slice(None)), None),
        (column_blocks(dn_all, units, wide), None),
    )

    def piece(a, zz):
        if a < N_SMALL:
            return arrays[a][1]
        return stage.at[zz] if a == 3 else dn.at[span(zz, units), :]

    MIX, UP, DOWN, MIX_Z, MIX_RELAY, UP_Z, DOWN_Z, ROWS, ROWS_RELAY, MISC, PAIR, NEAR, FAR = range(N_SENT)

    def misc_hop(n, source, to, target):
        return hop(source, to, sent.at[MISC], got.at[AT_MISC + n], target)

    def arrival(block, n):
        return hop(block, block, sent.at[MISC], got.at[n], core_target)

    def mixer_part(a, f, h):
        if a < 2:
            columns = pl.ds(pl.multiple_of(a * local_width + h * cw, cw), cw)
            return bo_all.at[span(f, deep), columns]
        return mo_all.at[span(h, cw), span(f, wide)]

    def own_part_of(a, h):
        return mo.at[span(h, cw), :] if a == 2 else arrays[a][1].at[:, span(h, cw)]

    def z_hop(a, source, f, slot, land, to):
        group = (UP_Z, DOWN_Z)[a - N_SMALL] if a >= N_SMALL else MIX_RELAY if slot else MIX_Z
        return hop(source, arrays[a][0](f), sent.at[group], got.at[AT_Z + a * LAYERS + land], line[to])

    def side_at(a, k, kind):
        return AT_SIDE + ((a - N_SMALL) * 2 + kind - 1) * LAYERS + k

    def corner_at(a, late, kind):
        return AT_CORNER + ((a - N_SMALL) * 2 + late) * 2 + kind - 1

    def sides(a, k, of=None, kinds=(1, 2)):
        at = arrays[a][0]
        f = (layer[k] if of is None else of) * PLANE + p
        source = piece(a, z) if of is None and k == 0 else at(f)
        for kind in kinds:
            target = (x_target, y_target)[kind - 1]
            hop(source, at(f), sent.at[UP + a - N_SMALL], got.at[side_at(a, k, kind)], target).start()

    def mixer_sides(a, k):
        copies = []
        f = layer[k] * PLANE + p
        for kind, h, target in ((1, 1 - x, x_target), (2, x, y_target)):
            to = mixer_part(a, f, h)
            source = own_part_of(a, h) if k == 0 else to
            n = AT_MIX + a * LAYERS + k if kind == 1 else AT_MIX_DONE
            copies.append(hop(source, to, sent.at[MIX], got.at[n], target))
        return copies

    def mixer_corner(a, k):
        block = mixer_part(a, layer[k] * PLANE + px, x)
        with jax.named_scope(f"side{a}{k}"):
            arrival(block, AT_MIX + a * LAYERS + k).wait_recv()
        hop(block, block, sent.at[MIX], got.at[AT_MIX_DONE + 1], y_target).start()

    def mixer_done():
        block = bo_all.at[pl.ds(0, N_SMALL * LAYERS * deep // 4), :]
        for n in range(2):
            with jax.named_scope(f"mixer_done{n}"):
                arrival(block, AT_MIX_DONE + n).wait_recv()

    def corners(a, k, of=None, kinds=(1, 2)):
        at = arrays[a][0]
        base = (layer[k] if of is None else of) * PLANE
        late = k == LAYERS - 1 if a == N_SMALL else of is down[1][0][1] or of is down[1][1][1]
        for kind, part, owner, target in ((1, 0, px, y_target), (2, 1, py, x_target)):
            if kind not in kinds:
                continue
            with jax.named_scope(f"side{a}{k if of is None else 9}{kind}"):
                arrival(at(base + owner), side_at(a, k, kind)).wait_recv()
            block = at(base + owner, part)
            hop(block, block, sent.at[UP + a - N_SMALL], got.at[corner_at(a, late, kind)], target).start()

    def corners_done(a, late):
        count = (1 if late else LAYERS - 1) if a == N_SMALL else 2
        for kind in (1, 2):
            if a == N_SMALL:
                block = gu_all.at[pl.ds(0, count * (ROWS_CUT * deep // 8 if kind == 1 else deep - ROWS_CUT * deep // 8)), :]
            else:
                block = dn_all.at[pl.ds(0, units // 2), pl.ds(0, count * wide)]
            with jax.named_scope(f"corner{a}{int(late)}{kind}"):
                arrival(block, corner_at(a, late, kind)).wait_recv()

    def z_done(a, k):
        block = arrays[a][0](layer[k] * PLANE + p)
        with jax.named_scope(f"z{a}{k}"):
            arrival(block, AT_Z + a * LAYERS + k).wait_recv()

    @pl.when(inner == 1)
    def _():
        for a in range(N_SMALL):
            z_hop(a, piece(a, z), fs, 1, 2, 2).start()

    for a in range(N_SMALL):
        z_hop(a, piece(a, z), fs, 0, 1, 1).start()
    mixer_copies = [[c for a in range(N_SMALL) for c in mixer_sides(a, k)] for k in range(LAYERS)]
    for c in mixer_copies[0]:
        c.start()
    tok_swap = misc_hop(0, tok, tok2.at[0, :, mine_half], core_target)

    def tok_hop(n, target):
        piece_rows = pl.ds(n % 2 * (rows // 2), rows // 2)
        block = tok2.at[1, piece_rows, mine_half]
        return misc_hop(1 + n if n < 2 else 0, tok.at[piece_rows, :] if n < 2 else block, block, target)

    tok_x = [tok_hop(n, x_target) for n in range(2)]
    tok_core = [tok_hop(n, core_target) for n in (2, 3)]
    pld_x = misc_hop(3, pld.at[:, span(1 - x, cw)], pld_v.at[1], x_target)
    tok_swap.start()

    own = [
        pltpu.make_async_copy(gup, gup_v, local.at[0]),
        pltpu.make_async_copy(vup, vup_v, local.at[1]),
        pltpu.make_async_copy(tok, tok2.at[0, :, mine_half], local.at[2]),
        pltpu.make_async_copy(pld.at[:, channels], pld_v.at[0], local.at[3]),
        pltpu.make_async_copy(rb, arrays[0][0](fs), local.at[4]),
        pltpu.make_async_copy(og, arrays[1][0](fs), local.at[5]),
        pltpu.make_async_copy(mo, arrays[2][0](fs), local.at[6]),
        pltpu.make_async_copy(piece(4, z), arrays[4][0](fs), local.at[7]),
    ]
    for c in own:
        c.start()

    own[0].wait()
    own[1].wait()

    def arrange(gate, value, zz, store):
        for j in range(full):
            at = zz * units + j * LANES
            store(2 * j * LANES, gate[:, at : at + LANES])
            store((2 * j + 1) * LANES, value[:, at : at + LANES])
        if rest:
            at = zz * units + full * LANES
            store(2 * full * LANES, gate[:, at : at + rest])
            store(2 * full * LANES + rest, value[:, at : at + rest])

    for zz in range(LAYERS):

        def put(at, v, zz=zz):
            stage[zz, :, at : at + v.shape[1]] = v

        def put_taps(at, v, zz=zz):
            taps[zz, 0 : v.shape[0], at : at + v.shape[1]] = v.astype(F32)

        arrange(gup_v, vup_v, zz, put)
        arrange(gtaps, vtaps, zz, put_taps)
    gu_all[span(fs, deep), :] = stage[z]
    dn_all[units:, :] = jnp.zeros((dn_all.shape[0] - units, dn_all.shape[1]), BF16)
    gmap[...] = jnp.zeros(gmap.shape, BF16)
    for c in range(heads // per):
        for h in range(per):
            r = slice(h * head, (h + 1) * head)
            gmap[c, r, h * head : (h + 1) * head] = rmap[c * per + h]
            gmap[c, r, cw + h * head : cw + (h + 1) * head] = imap[c * per + h]

    def relay(k, to, land, slot):
        @pl.when(inner == 1)
        def _():
            for a in range(N_SMALL):
                f = layer[k] * PLANE + p
                z_hop(a, arrays[a][0](f), f, slot, land, to).start()


    def ffn_along_z(a):
        for k in range(1, LAYERS):
            z_hop(a, piece(a, layer[k]), fs, k, lands[k], k).start()

    def mixer_step(k, to, land):
        for a in range(N_SMALL):
            z_done(a, k)
        relay(k, to, land, k + 1)
        for c in mixer_copies[k]:
            c.start()

    def mixer_corners(k):
        for a in range(N_SMALL):
            mixer_corner(a, k)

    mixer_corners(0)
    pld_x.start()
    mixer_step(1, 2, 3)

    @pl.when(inner == 1)
    def _():
        mixer_step(2, 1, 2)

    mixer_corners(1)
    tok_x[0].start()

    @pl.when(inner == 0)
    def _():
        mixer_step(2, 1, 2)
        ffn_along_z(3)

    mixer_corners(2)
    tok_x[1].start()
    mixer_step(3, 1, 3)

    @pl.when(inner == 1)
    def _():
        ffn_along_z(3)

    for n in range(2):
        with jax.named_scope("tok_x"):
            tok_x[n].wait_recv()
        tok_core[n].start()
    for a in range(N_SMALL):
        mixer_corner(a, LAYERS - 1)
    sides(3, 0)

    with jax.named_scope("tokens"):
        arrival(tok2.at[0], AT_MISC).wait_recv()
        pld_x.wait_recv()
        own[2].wait()

    def norm_step(r, _):
        normed[r] = normed_rows(tok2[r].astype(F32), gain1[...].astype(F32)[None, :])
        return 0

    lax.fori_loop(0, 2, norm_step, 0)
    for c in own[3:]:
        c.wait()
    mixer_done()

    def mixer_rows(r, _):
        place = position((rows, cw))
        branch = jnp.dot(normed[r], bo_all[:, channels], preferred_element_type=F32)
        branch = branch.astype(BF16).astype(F32)
        conv = rows_conv(branch, ctaps[:, channels].astype(F32), ctaps.shape[0], place).astype(BF16)
        gates = jax.nn.sigmoid(jnp.dot(conv, gmap[x], preferred_element_type=F32))
        la = -DECAY_RATE_GAIN * gates[:, :cw] * rate[:, channels] + pld_v[r]
        d = jnp.sqrt(negative_expm1(2.0 * la)) * gates[:, cw:] * conv.astype(F32)
        a = jnp.exp(la)
        step = 1
        while step < SEQ_LEN:
            d = a * shifted(d, step, place, 0.0) + d
            if step * 2 < SEQ_LEN:
                a = a * shifted(a, step, place, 1.0)
            step *= 2
        outgate = jnp.dot(
            normed[r],
            bo_all[:, pl.ds(pl.multiple_of(local_width + x * cw, cw), cw)],
            preferred_element_type=F32,
        )
        outgate = outgate.astype(BF16).astype(F32)
        mixed = (d * gelu(outgate)).astype(BF16)
        mix_give[r] = jnp.dot(mixed, mo_all[channels, their_half], preferred_element_type=F32).astype(BF16)
        mix_keep[r] = jnp.dot(mixed, mo_all[channels, mine_half], preferred_element_type=F32)
        return 0

    def mix_hop(r):
        return misc_hop(4 + r, mix_give.at[r], mix_pair.at[r], core_target)

    with jax.named_scope("mixer1"):
        lax.fori_loop(1, 2, mixer_rows, 0)
    mix_hop(1).start()
    with jax.named_scope("mixer0"):
        lax.fori_loop(0, 1, mixer_rows, 0)
    mix_hop(0).start()
    with jax.named_scope("swap1"):
        mix_hop(1).wait_recv()
    mix_out[...] = (mix_keep[1] + mix_pair[1].astype(F32)).astype(BF16)
    mix_x = misc_hop(6, mix_out, mix_in, x_target)
    mix_x.start()
    ffn_along_z(4)
    z_done(3, 1)
    sides(3, 1)
    corners(3, 0)
    for k in range(2, LAYERS):
        z_done(3, k)
        sides(3, k)
    with jax.named_scope("swap0"):
        mix_hop(0).wait_recv()
    mix_keep[0] = mix_keep[0] + mix_pair[0].astype(F32) + tok2[0, :, mine_half].astype(F32)
    with jax.named_scope("mix_x"):
        mix_x.wait_recv()
    after[:, mine_half] = (mix_keep[0] + mix_in[...].astype(F32)).astype(BF16)
    after_core = misc_hop(7, after.at[:, mine_half], after.at[:, mine_half], core_target)
    after_core.start()
    with jax.named_scope("after"):
        after_core.wait_recv()
    n2[0] = normed_rows(after[...].astype(F32), gain2[...].astype(F32)[None, :])


    def rows_hop(k, land, slot, to):
        return hop(
            n2.at[k, :, mine_half],
            n2.at[land, :, mine_half],
            sent.at[ROWS_RELAY if slot else ROWS],
            got.at[AT_ROWS + land],
            line[to],
        )

    @pl.when(inner == 1)
    def _():
        rows_hop(0, 2, 1, 2).start()

    rows_hop(0, 1, 0, 1).start()

    def rows_arrived(k, to, land):
        with jax.named_scope(f"rows{k}"):
            rows_hop(k, k, 0, 1).wait_recv()

        @pl.when(inner == 1)
        def _():
            rows_hop(k, land, k + 1, to).start()

        core_hop(k).start()

    def core_hop(k):
        block = n2.at[k, :, mine_half]
        return hop(block, block, sent.at[ROWS], got.at[AT_CORE + k], core_target)

    corners(3, 1)
    rows_arrived(1, 2, 3)
    corners(3, 2)

    @pl.when(inner == 1)
    def _():
        rows_arrived(2, 1, 2)

    corners(3, 3)
    z_done(4, 1)
    z_done(4, 2)
    down_a, down_b = down[0]
    for block in down[0]:
        sides(4, *block, kinds=(1,))

    @pl.when(inner == 1)
    def _():
        rows_arrived(3, 1, 3)

    @pl.when(inner == 0)
    def _():
        rows_arrived(2, 1, 2)

    block_rows = PLANE * deep

    def up_dot(k, at, blocks):
        total = None
        for of in blocks:
            where = span(layer[of], block_rows)
            s = jnp.dot(n2[k, :, where], gu_all[where, at], preferred_element_type=F32)
            total = s if total is None else total + s
        return total

    def up_early(k, _):
        with jax.named_scope("up_early"):
            for j in range(0, 2 * units, 4 * LANES):
                at = slice(j, min(j + 4 * LANES, 2 * units))
                part[k - 1, :, at] = up_dot(k, at, range(LAYERS - 1))
        return 0

    def up(k, late):
        place = position((rows, 4 * LANES))
        layer_taps = taps.at[z]
        width = gtaps.shape[0]

        def halves(j, n):
            at = slice(j, j + n)
            if late:
                s = part[k - 1, :, at] + up_dot(k, at, (LAYERS - 1,))
            else:
                s = jnp.dot(n2[k], gu_all[:, at], preferred_element_type=F32)
            return rows_conv(s.astype(BF16).astype(F32), layer_taps[0:width, at], width, place[:, :n])

        j = 0
        while j < 2 * full * LANES:
            n = min(4 * LANES, 2 * full * LANES - j)
            s = halves(j, n)
            for i in range(0, n, 2 * LANES):
                g, v = s[:, i : i + LANES], s[:, i + LANES : i + 2 * LANES]
                h = (j + i) // 2
                hidden[k, :, h : h + LANES] = (g * jax.nn.sigmoid(g) * v).astype(BF16)
            j += n
        if rest:
            s = halves(j, 2 * rest)
            h = s * jax.nn.sigmoid(s) * pltpu.roll(s, rest, 1)
            lane = lax.broadcasted_iota(jnp.int32, h.shape, 1)
            hidden[k, :, full * LANES : (full + 1) * LANES] = jnp.where(lane < rest, h, 0.0).astype(BF16)

    def up_step(k, _):
        with jax.named_scope("up"):
            up(k, False)
        return 0

    def up_late(k, _):
        with jax.named_scope("up_late"):
            up(k, True)
        return 0

    turn = (tp + z // 2) % 2
    quarter = PLANE * wide // 2

    def columns_of(j, mine):
        first, second = down[j // 2][0][1], down[j // 2][1][1]
        side = turn if mine else 1 - turn
        block = first * (1 - side) + second * side
        return block * 2 + (y if j % 2 == 0 else 1 - y)

    def place_of(j):
        return columns_of(j, True) % (half // quarter)

    def pair_hop(j, k):
        return hop(give.at[j, k], pair.at[j, k], sent.at[PAIR], got.at[AT_PAIR + j * LAYERS + k], core_target)

    def to_partner(j, k):
        landing = arrive.at[0, j] if k == 1 else joint.at[j, k - 2]
        group = NEAR if k == 1 else FAR
        return hop(paired.at[j, k], landing, sent.at[group], got.at[AT_BACK + j * LAYERS + k], line[1])

    def to_layer(j, k):
        return hop(joint.at[j, k], arrive.at[1, j], sent.at[FAR], got.at[AT_BACK + j * LAYERS], line[k + 2])

    def part_sums(*parts):
        for j, k in parts:
            given = span(columns_of(j, False), quarter)
            give[j, k] = jnp.dot(hidden[k], dn_all[:, given], preferred_element_type=F32).astype(BF16)
            pair_hop(j, k).start()
        for j, k in parts:
            kept = span(columns_of(j, True), quarter)
            keep = jnp.dot(hidden[k], dn_all[:, kept], preferred_element_type=F32)
            with jax.named_scope(f"pair{j}{k}"):
                pair_hop(j, k).wait_recv()
            paired[j, k] = (keep + pair[j, k].astype(F32)).astype(BF16)
            if k > 1:

                @pl.when(inner == 0)
                def _():
                    to_partner(j, k).start()

            elif k == 1:
                to_partner(j, 1).start()

    def joint_sums(j, k):
        @pl.when(inner == 1)
        def _():
            with jax.named_scope(f"joint{j}{k}"):
                to_partner(j, k + 2).wait_recv()
            joint[j, k] = (joint[j, k].astype(F32) + paired[j, k + 2].astype(F32)).astype(BF16)
            to_layer(j, k).start()

    corners_done(3, False)
    for block in down[0]:
        sides(4, *block, kinds=(2,))
    with jax.named_scope("across12"):
        core_hop(1).wait_recv()
        core_hop(2).wait_recv()
    lax.fori_loop(1, 3, up_early, 0)
    corners_done(3, True)
    lax.fori_loop(1, 3, up_late, 0)
    corners(4, *down_a)
    corners(4, *down_b, kinds=(1,))
    part_sums((0, 2), (0, 1))
    corners(4, *down_b, kinds=(2,))
    z_done(4, 3)
    for block in down[1]:
        sides(4, *block)

    @pl.when(inner == 0)
    def _():
        rows_arrived(3, 1, 3)

    corners_done(4, False)
    part_sums((1, 2), (1, 1))
    with jax.named_scope("across3"):
        core_hop(3).wait_recv()
    lax.fori_loop(3, 4, up_step, 0)
    part_sums((0, 3), (1, 3))
    joint_sums(0, 0)
    corners(4, *down[1][0])
    joint_sums(1, 0)
    corners(4, *down[1][1], kinds=(1,))
    part_sums((2, 3), (2, 2), (2, 1))
    corners(4, *down[1][1], kinds=(2,))
    joint_sums(0, 1)
    corners_done(4, True)
    part_sums((3, 3), (3, 2), (3, 1))
    joint_sums(1, 1)
    lax.fori_loop(0, 1, up_step, 0)
    part_sums((0, 0), (1, 0))
    joint_sums(2, 1)
    joint_sums(2, 0)
    part_sums((2, 0), (3, 0))
    joint_sums(3, 1)
    joint_sums(3, 0)

    stores = []
    for j in range(LAYERS):
        with jax.named_scope(f"near{j}"):
            to_partner(j, 1).wait_recv()
        with jax.named_scope(f"far{j}"):
            to_layer(j, 0).wait_recv()
        total = paired[j, 0].astype(F32) + arrive[0, j].astype(F32) + arrive[1, j].astype(F32)
        first = pl.multiple_of(tp * half + place_of(j) * quarter, quarter)
        out_v[j] = (after[:, pl.ds(first, quarter)].astype(F32) + total).astype(BF16)
        stores.append(pltpu.make_async_copy(out_v.at[j], out.at[:, span(place_of(j), quarter)], local.at[j]))
        stores[j].start()

    def all_sent(group, block):
        hop(block, block, sent.at[group], got.at[0], core_target).wait_send()

    with jax.named_scope("sent"):
        every = slice(None)
        all_sent(MIX, bo_all.at[pl.ds(0, 3 * N_SMALL * LAYERS * deep // 4), :])
        all_sent(UP, gu_all.at[pl.ds(0, 3 * LAYERS * deep), :])
        all_sent(DOWN, dn_all.at[pl.ds(0, units), pl.ds(0, 3 * LAYERS * wide)])
        all_sent(MIX_Z, bo_all.at[pl.ds(0, N_SMALL * deep // 2), :])
        all_sent(UP_Z, gu_all.at[pl.ds(0, 3 * deep), :])
        all_sent(DOWN_Z, dn_all.at[pl.ds(0, units), pl.ds(0, 3 * wide)])
        all_sent(ROWS, n2.at[pl.ds(0, 2)])
        all_sent(MISC, bo_all.at[pl.ds(0, MISC_HALVES * rows * half // bo_all.shape[1] // 2), :])
        all_sent(PAIR, give)
        all_sent(NEAR, arrive.at[0])
        all_sent(FAR, joint)

        @pl.when(inner == 1)
        def _():
            all_sent(MIX_RELAY, bo_all.at[pl.ds(0, LAYERS * N_SMALL * deep // 2), :])
            all_sent(ROWS_RELAY, n2.at[pl.ds(0, 2)])

    with jax.named_scope("stores"):
        for c in stores:
            c.wait()


def fused_layer(
    tokens,
    mixer_norm_gain,
    recurrence_branch_weight,
    output_gate_projection,
    recurrence_conv_taps,
    recurrence_gate_map,
    input_gate_map,
    channel_decay_rate,
    position_log_decay,
    mixer_output_weight,
    feedforward_norm_gain,
    gate_up_weight,
    value_up_weight,
    gate_conv_taps,
    value_conv_taps,
    down_projection_weight,
):
    rows, half = tokens.shape
    deep, local_width = recurrence_branch_weight.shape
    wide = mixer_output_weight.shape[1]
    n_fs = LAYERS * PLANE
    features = 2 * half
    local_units = gate_up_weight.shape[1]
    units = local_units // LAYERS
    padded = -(-units // (2 * LANES)) * 2 * LANES
    cw = local_width // 2
    quarter = PLANE * wide // 2
    dma = pltpu.SemaphoreType.DMA
    scratch = [
        pltpu.VMEM((2, rows, features), BF16),
        pltpu.VMEM((n_fs * deep, 2 * local_width), BF16),
        pltpu.VMEM((local_width, n_fs * wide), BF16),
        pltpu.VMEM((deep, local_units), BF16),
        pltpu.VMEM((deep, local_units), BF16),
        pltpu.VMEM((LAYERS, deep, 2 * units), BF16),
        pltpu.VMEM((n_fs * deep, 2 * units), BF16),
        pltpu.VMEM((padded, n_fs * wide), BF16),
        pltpu.VMEM((LAYERS, 8, 2 * units), F32),
        pltpu.VMEM((local_width // cw, cw, 2 * cw), BF16),
        pltpu.VMEM((2, rows, cw), F32),
        pltpu.VMEM((2, rows, features), BF16),
        pltpu.VMEM((2, rows, half), BF16),
        pltpu.VMEM((2, rows, half), F32),
        pltpu.VMEM((2, rows, half), BF16),
        pltpu.VMEM((rows, half), BF16),
        pltpu.VMEM((rows, half), BF16),
        pltpu.VMEM((rows, features), BF16),
        pltpu.VMEM((LAYERS, rows, features), BF16),
        pltpu.VMEM((LAYERS, rows, padded), BF16),
        pltpu.VMEM((LAYERS, LAYERS, rows, quarter), BF16),
        pltpu.VMEM((LAYERS, LAYERS, rows, quarter), BF16),
        pltpu.VMEM((LAYERS, LAYERS, rows, quarter), BF16),
        pltpu.VMEM((2, LAYERS, rows, quarter), BF16),
        pltpu.VMEM((LAYERS, 2, rows, quarter), BF16),
        pltpu.VMEM((LAYERS, rows, quarter), BF16),
        pltpu.VMEM((2, rows, 2 * units), F32),
        dma((N_SENT,)),
        dma((AT_BACK + LAYERS * LAYERS,)),
        dma((8,)),
    ]
    return pl.pallas_call(
        layer_kernel,
        out_shape=jax.ShapeDtypeStruct((rows, half), BF16),
        in_specs=[ANY, VMEM, ANY, ANY, VMEM, VMEM, VMEM, VMEM, ANY, ANY, VMEM, ANY, ANY, VMEM, VMEM, ANY],
        out_specs=ANY,
        scratch_shapes=scratch,
        compiler_params=pltpu.CompilerParams(
            collective_id=0, has_side_effects=True, vmem_limit_bytes=62 * 2**20
        ),
        name="layer",
    )(
        tokens,
        mixer_norm_gain,
        recurrence_branch_weight,
        output_gate_projection,
        recurrence_conv_taps,
        recurrence_gate_map,
        input_gate_map,
        channel_decay_rate.reshape(1, -1),
        position_log_decay,
        mixer_output_weight,
        feedforward_norm_gain,
        gate_up_weight,
        value_up_weight,
        gate_conv_taps,
        value_conv_taps,
        down_projection_weight,
    )


def solution(mesh):
    placed = (
        P("fs", "tp"),
        P(),
        P("fs", "tp"),
        P("fs", "tp"),
        P(None, "tp"),
        P("tp", None, None),
        P("tp", None, None),
        P("tp"),
        P("fs", "tp"),
        P("tp", "fs"),
        P(),
        P("fs", "tp"),
        P("fs", "tp"),
        P(None, "tp"),
        P(None, "tp"),
        P("tp", "fs"),
    )
    fused = mesh.shape["tp"] == 2 and mesh.shape["fs"] == LAYERS * PLANE
    body = fused_layer if fused else gathered_layer
    return jax.shard_map(
        body, mesh=mesh, in_specs=placed, out_specs=P("fs", "tp"), check_vma=False
    )
```

```python
import functools

import jax
import jax.numpy as jnp
from jax import lax
from jax.experimental import pallas as pl
from jax.experimental.pallas import tpu as pltpu
from jax.sharding import PartitionSpec as P

SEQ_LEN = 64


EPS = 1e-06
DECAY_RATE_GAIN = 8.0


def rms_normed(values, gain):
    wide = values.astype(jnp.float32)
    factor = lax.rsqrt(jnp.mean(wide * wide, axis=-1, keepdims=True) + EPS)
    return (wide * factor * gain.astype(jnp.float32)).astype(jnp.bfloat16)


def causal_conv(values, kernel):
    width = kernel.shape[0]
    row_count, channels = values.shape
    grouped = values.astype(jnp.float32).reshape(row_count // SEQ_LEN, SEQ_LEN, channels)
    padded = jnp.pad(grouped, ((0, 0), (width - 1, 0), (0, 0)))
    summed = padded[:, 0:SEQ_LEN] * kernel[0].astype(jnp.float32)
    for offset in range(1, width):
        summed = summed + padded[:, offset : offset + SEQ_LEN] * kernel[offset].astype(jnp.float32)
    return summed.reshape(row_count, channels)


def combine(left, right):
    first_a, first_b = left
    second_a, second_b = right
    return (first_a * second_a, second_a * first_b + second_b)


def pair_folder(normed, pieces):
    return (
        jnp.dot(normed, pieces[0], preferred_element_type=jnp.float32),
        jnp.dot(normed, pieces[1], preferred_element_type=jnp.float32),
    )


def gathered_layer(
    tokens,
    mixer_norm_gain,
    recurrence_branch_weight,
    output_gate_projection,
    recurrence_conv_taps,
    recurrence_gate_map,
    input_gate_map,
    channel_decay_rate,
    position_log_decay,
    mixer_output_weight,
    feedforward_norm_gain,
    gate_up_weight,
    value_up_weight,
    gate_conv_taps,
    value_conv_taps,
    down_projection_weight,
):
    row_count = tokens.shape[0]
    local_width = recurrence_branch_weight.shape[1]
    local_heads = recurrence_gate_map.shape[0]
    head_size = recurrence_gate_map.shape[1]
    whole_rows = lax.all_gather(tokens, "tp", axis=1, tiled=True)
    normed = rms_normed(whole_rows, mixer_norm_gain)
    branch_sum, outgate_sum = pair_folder(
        normed,
        (
            lax.all_gather(recurrence_branch_weight, "fs", axis=0, tiled=True),
            lax.all_gather(output_gate_projection, "fs", axis=0, tiled=True),
        ),
    )
    branch = branch_sum.astype(jnp.bfloat16)
    outgate = outgate_sum.astype(jnp.bfloat16)
    conv = causal_conv(branch, recurrence_conv_taps).astype(jnp.bfloat16)
    grouped = conv.reshape(row_count, local_heads, head_size)
    recurrence_scan = jax.nn.sigmoid(
        jnp.einsum(
            "rhi,hij->rhj", grouped, recurrence_gate_map, preferred_element_type=jnp.float32
        ).reshape(row_count, local_width)
    )
    inner = jax.nn.sigmoid(
        jnp.einsum(
            "rhi,hij->rhj", grouped, input_gate_map, preferred_element_type=jnp.float32
        ).reshape(row_count, local_width)
    )
    log_alpha = (
        -DECAY_RATE_GAIN * recurrence_scan * channel_decay_rate[None, :] + position_log_decay
    )
    drive = jnp.sqrt(-jnp.expm1(2.0 * log_alpha)) * inner * conv.astype(jnp.float32)
    shape3 = (row_count // SEQ_LEN, SEQ_LEN, local_width)
    unused, state = lax.associative_scan(
        combine, (jnp.exp(log_alpha).reshape(shape3), drive.reshape(shape3)), axis=1
    )
    state = state.reshape(row_count, local_width)
    mixed = (state * jax.nn.gelu(outgate.astype(jnp.float32))).astype(jnp.bfloat16)
    mixer_terms = jnp.dot(
        mixed,
        lax.all_gather(mixer_output_weight, "fs", axis=1, tiled=True),
        preferred_element_type=jnp.float32,
    )
    mixer_terms = mixer_terms.astype(jnp.bfloat16).astype(jnp.float32)
    mixer_whole = lax.psum(mixer_terms.astype(jnp.bfloat16), "tp").astype(jnp.float32)
    whole_after = (whole_rows.astype(jnp.float32) + mixer_whole).astype(jnp.bfloat16)
    normed2 = rms_normed(whole_after, feedforward_norm_gain)
    gate_whole, value_whole = (
        lax.all_gather(gate_up_weight, "fs", axis=0, tiled=True),
        lax.all_gather(value_up_weight, "fs", axis=0, tiled=True),
    )
    gate_sum = jnp.dot(normed2, gate_whole, preferred_element_type=jnp.float32)
    value_sum = jnp.dot(normed2, value_whole, preferred_element_type=jnp.float32)
    gate_half = gate_sum.astype(jnp.bfloat16)
    value_half = value_sum.astype(jnp.bfloat16)
    hidden = (
        jax.nn.silu(causal_conv(gate_half, gate_conv_taps))
        * causal_conv(value_half, value_conv_taps)
    ).astype(jnp.bfloat16)
    channel_terms = jnp.dot(
        hidden,
        lax.all_gather(down_projection_weight, "fs", axis=1, tiled=True),
        preferred_element_type=jnp.float32,
    )
    channel_terms = channel_terms.astype(jnp.bfloat16).astype(jnp.float32)
    channel_share = lax.psum_scatter(
        channel_terms.astype(jnp.bfloat16), "tp", scatter_dimension=1, tiled=True
    ).astype(jnp.float32)
    share_width = channel_share.shape[1]
    residual_share = lax.dynamic_slice_in_dim(
        whole_after, lax.axis_index("tp") * share_width, share_width, 1
    )
    return (residual_share.astype(jnp.float32) + channel_share).astype(jnp.bfloat16)


PLANE = 4
LAYERS = 4
LANES = 128
ANY = pl.BlockSpec(memory_space=pl.ANY)
VMEM = pl.BlockSpec(memory_space=pltpu.VMEM)
F32, BF16 = jnp.float32, jnp.bfloat16
N_SMALL, N_BIG = 3, 5
ROWS_CUT = 6
MISC_QUARTERS = 29
N_SENT = 13
AT_Z = 0
AT_MIX = AT_Z + N_BIG * LAYERS
AT_MIX_DONE = AT_MIX + N_SMALL * LAYERS
AT_SIDE = AT_MIX_DONE + 2
AT_CORNER = AT_SIDE + 2 * 2 * LAYERS
AT_MISC = AT_CORNER + 2 * 2 * 2
AT_ROWS = AT_MISC + 8
AT_CORE = AT_ROWS + LAYERS
AT_PAIR = AT_CORE + LAYERS
AT_BACK = AT_PAIR + LAYERS * LAYERS


def hop(src, dst, send, recv, target):
    return pltpu.make_async_remote_copy(
        src_ref=src,
        dst_ref=dst,
        send_sem=send,
        recv_sem=recv,
        device_id=target,
        device_id_type=pl.DeviceIdType.MESH,
    )


def greet(targets):
    barrier = pltpu.get_barrier_semaphore()
    for target in targets:
        pl.semaphore_signal(
            barrier, inc=1, device_id=target, device_id_type=pl.DeviceIdType.MESH
        )
    pl.semaphore_wait(barrier, len(targets))


def span(index, size):
    return pl.ds(pl.multiple_of(index * size, size), size)


def row_blocks(whole, deep, columns):
    cut = ROWS_CUT * deep // 8

    def at(f, part=None):
        if part is None:
            return whole.at[span(f, deep), columns]
        start, size = ((0, cut), (cut, deep - cut))[part]
        return whole.at[pl.ds(pl.multiple_of(f * deep + start, 16), size), columns]

    return at


def column_blocks(whole, rows, wide):
    cut = rows // 2 // 16 * 16

    def at(f, part=None):
        start, size = ((0, rows) if part is None else ((0, cut), (cut, rows - cut))[part])
        return whole.at[pl.ds(start, size), span(f, wide)]

    return at


def position(shape):
    return lax.broadcasted_iota(jnp.int32, shape, 0) % SEQ_LEN


def shifted(values, distance, place, fill):
    return jnp.where(place >= distance, pltpu.roll(values, distance, 0), fill)


def rows_conv(values, taps, width, place):
    summed = shifted(values, width - 1, place, 0.0) * taps[0:1, :]
    for j in range(1, width - 1):
        summed = summed + shifted(values, width - 1 - j, place, 0.0) * taps[j : j + 1, :]
    return summed + values * taps[width - 1 : width, :]


def negative_expm1(x):
    near = 1.0 + x * (1.0 / 8.0)
    for n in range(7, 1, -1):
        near = 1.0 + x * (1.0 / n) * near
    return jnp.where(jnp.abs(x) < 0.4, -x * near, 1.0 - jnp.exp(x))


def normed_rows(values, gain):
    factor = lax.rsqrt(jnp.mean(values * values, axis=-1, keepdims=True) + EPS)
    return (values * factor * gain).astype(BF16)


def gelu(x):
    return 0.5 * x * (1.0 + jnp.tanh(0.7978845608028654 * (x + 0.044715 * (x * x * x))))


def layer_kernel(
    tok, gain1, rb, og, ctaps, rmap, imap, rate, pld, mo, gain2, gup, vup, gtaps, vtaps, dn,
    out,
    tok2, bo_all, mo_all, gup_v, vup_v, stage, gu_all, dn_all, taps, gmap, pld_v,
    normed, mix_give, mix_keep, mix_pair, mix_out, mix_in, after, n2, hidden, give, pair, paired, arrive, joint, out_v, part, pld_b,
    sent, got, local,
):
    fs, tp = lax.axis_index("fs"), lax.axis_index("tp")
    z, p = fs // PLANE, fs % PLANE
    y, x = p // 2, p % 2
    px, py = y * 2 + 1 - x, (1 - y) * 2 + x
    inner = ((z + 1) // 2) % 2
    layer = (z, z + 1 - 2 * (z % 2), 2 - z // 2, 3 - 3 * (z // 2))
    lands = (0, 1, 3 - inner, 3 - inner)
    down = (
        ((1 - inner, 1 + z // 2), (2, layer[2])),
        ((inner, 3 * (z // 2)), (3, layer[3])),
    )
    line = [(zz * PLANE + p, tp) for zz in layer]
    x_target, y_target = (z * PLANE + px, tp), (z * PLANE + py, tp)
    core_target = (fs, 1 - tp)
    with jax.named_scope("greet"):
        greet(line[1:] + [x_target, y_target, core_target])

    rows, half = tok.shape
    deep, local_width = rb.shape
    wide = mo.shape[1]
    units = dn.shape[0] // LAYERS
    full, rest = units // LANES, units % LANES
    cw = gmap.shape[1]
    mine_half, their_half, channels = span(tp, half), span(1 - tp, half), span(x, cw)
    heads, head = rmap.shape[:2]
    per = cw // head

    arrays = (
        (row_blocks(bo_all, deep, pl.ds(0, local_width)), rb),
        (row_blocks(bo_all, deep, pl.ds(local_width, local_width)), og),
        (column_blocks(mo_all, mo.shape[0], wide), mo),
        (row_blocks(gu_all, deep, slice(None)), None),
        (column_blocks(dn_all, units, wide), None),
    )

    def piece(a, zz):
        if a < N_SMALL:
            return arrays[a][1]
        return stage.at[zz] if a == 3 else dn.at[span(zz, units), :]

    MIX, UP, DOWN, MIX_Z, MIX_RELAY, UP_Z, DOWN_Z, ROWS, ROWS_RELAY, MISC, PAIR, NEAR, FAR = range(N_SENT)

    def misc_hop(n, source, to, target):
        return hop(source, to, sent.at[MISC], got.at[AT_MISC + n], target)

    def arrival(block, n):
        return hop(block, block, sent.at[MISC], got.at[n], core_target)

    def mixer_part(a, f, h):
        if a < 2:
            columns = pl.ds(pl.multiple_of(a * local_width + h * cw, cw), cw)
            return bo_all.at[span(f, deep), columns]
        return mo_all.at[span(h, cw), span(f, wide)]

    def own_part_of(a, h):
        return mo.at[span(h, cw), :] if a == 2 else arrays[a][1].at[:, span(h, cw)]

    def z_hop(a, source, f, slot, land, to):
        group = (UP_Z, DOWN_Z)[a - N_SMALL] if a >= N_SMALL else MIX_RELAY if slot else MIX_Z
        return hop(source, arrays[a][0](f), sent.at[group], got.at[AT_Z + a * LAYERS + land], line[to])

    def side_at(a, k, kind):
        return AT_SIDE + ((a - N_SMALL) * 2 + kind - 1) * LAYERS + k

    def corner_at(a, late, kind):
        return AT_CORNER + ((a - N_SMALL) * 2 + late) * 2 + kind - 1

    def sides(a, k, of=None, kinds=(1, 2)):
        at = arrays[a][0]
        f = (layer[k] if of is None else of) * PLANE + p
        source = piece(a, z) if of is None and k == 0 else at(f)
        for kind in kinds:
            target = (x_target, y_target)[kind - 1]
            hop(source, at(f), sent.at[UP + a - N_SMALL], got.at[side_at(a, k, kind)], target).start()

    def mixer_sides(a, k):
        copies = []
        f = layer[k] * PLANE + p
        for kind, h, target in ((1, 1 - x, x_target), (2, x, y_target)):
            to = mixer_part(a, f, h)
            source = own_part_of(a, h) if k == 0 else to
            n = AT_MIX + a * LAYERS + k if kind == 1 else AT_MIX_DONE
            copies.append(hop(source, to, sent.at[MIX], got.at[n], target))
        return copies

    def mixer_corner(a, k):
        block = mixer_part(a, layer[k] * PLANE + px, x)
        with jax.named_scope(f"side{a}{k}"):
            arrival(block, AT_MIX + a * LAYERS + k).wait_recv()
        hop(block, block, sent.at[MIX], got.at[AT_MIX_DONE + 1], y_target).start()

    def mixer_done():
        block = bo_all.at[pl.ds(0, N_SMALL * LAYERS * deep // 4), :]
        for n in range(2):
            with jax.named_scope(f"mixer_done{n}"):
                arrival(block, AT_MIX_DONE + n).wait_recv()

    def corners(a, k, of=None, kinds=(1, 2)):
        at = arrays[a][0]
        base = (layer[k] if of is None else of) * PLANE
        late = k == LAYERS - 1 if a == N_SMALL else of is down[1][0][1] or of is down[1][1][1]
        for kind, part, owner, target in ((1, 0, px, y_target), (2, 1, py, x_target)):
            if kind not in kinds:
                continue
            with jax.named_scope(f"side{a}{k if of is None else 9}{kind}"):
                arrival(at(base + owner), side_at(a, k, kind)).wait_recv()
            block = at(base + owner, part)
            hop(block, block, sent.at[UP + a - N_SMALL], got.at[corner_at(a, late, kind)], target).start()

    def corners_done(a, late):
        count = (1 if late else LAYERS - 1) if a == N_SMALL else 2
        for kind in (1, 2):
            if a == N_SMALL:
                block = gu_all.at[pl.ds(0, count * (ROWS_CUT * deep // 8 if kind == 1 else deep - ROWS_CUT * deep // 8)), :]
            else:
                block = dn_all.at[pl.ds(0, units // 2), pl.ds(0, count * wide)]
            with jax.named_scope(f"corner{a}{int(late)}{kind}"):
                arrival(block, corner_at(a, late, kind)).wait_recv()

    def z_done(a, k):
        block = arrays[a][0](layer[k] * PLANE + p)
        with jax.named_scope(f"z{a}{k}"):
            arrival(block, AT_Z + a * LAYERS + k).wait_recv()

    @pl.when(inner == 1)
    def _():
        for a in range(N_SMALL):
            z_hop(a, piece(a, z), fs, 1, 2, 2).start()

    for a in range(N_SMALL):
        z_hop(a, piece(a, z), fs, 0, 1, 1).start()
    mixer_copies = [[c for a in range(N_SMALL) for c in mixer_sides(a, k)] for k in range(LAYERS)]
    for c in mixer_copies[0]:
        c.start()
    tok_swap = misc_hop(0, tok, tok2.at[0, :, mine_half], core_target)

    def tok_hop(n, target):
        piece_rows = pl.ds(n % 2 * (rows // 2), rows // 2)
        block = tok2.at[1, piece_rows, mine_half]
        return misc_hop(1 + n if n < 2 else 0, tok.at[piece_rows, :] if n < 2 else block, block, target)

    tok_x = [tok_hop(n, x_target) for n in range(2)]
    tok_core = [tok_hop(n, core_target) for n in (2, 3)]
    pld_x = misc_hop(3, pld_b.at[0], pld_b.at[1], x_target)
    tok_swap.start()

    own = [
        pltpu.make_async_copy(gup, gup_v, local.at[0]),
        pltpu.make_async_copy(vup, vup_v, local.at[1]),
        pltpu.make_async_copy(tok, tok2.at[0, :, mine_half], local.at[2]),
        pltpu.make_async_copy(pld.at[:, channels], pld_v.at[0], local.at[3]),
        pltpu.make_async_copy(rb, arrays[0][0](fs), local.at[4]),
        pltpu.make_async_copy(og, arrays[1][0](fs), local.at[5]),
        pltpu.make_async_copy(mo, arrays[2][0](fs), local.at[6]),
        pltpu.make_async_copy(piece(4, z), arrays[4][0](fs), local.at[7]),
        pltpu.make_async_copy(pld.at[:, span(1 - x, cw)], pld_v.at[1], local.at[8]),
    ]
    for c in own:
        c.start()

    own[8].wait()
    pld_b[0] = pld_v[1].astype(BF16)
    own[0].wait()
    own[1].wait()

    def arrange(gate, value, zz, store):
        for j in range(full):
            at = zz * units + j * LANES
            store(2 * j * LANES, gate[:, at : at + LANES])
            store((2 * j + 1) * LANES, value[:, at : at + LANES])
        if rest:
            at = zz * units + full * LANES
            store(2 * full * LANES, gate[:, at : at + rest])
            store(2 * full * LANES + rest, value[:, at : at + rest])

    for zz in range(LAYERS):

        def put(at, v, zz=zz):
            stage[zz, :, at : at + v.shape[1]] = v

        def put_taps(at, v, zz=zz):
            taps[zz, 0 : v.shape[0], at : at + v.shape[1]] = v.astype(F32)

        arrange(gup_v, vup_v, zz, put)
        arrange(gtaps, vtaps, zz, put_taps)
    gu_all[span(fs, deep), :] = stage[z]
    dn_all[units:, :] = jnp.zeros((dn_all.shape[0] - units, dn_all.shape[1]), BF16)
    gmap[...] = jnp.zeros(gmap.shape, BF16)
    for c in range(heads // per):
        for h in range(per):
            r = slice(h * head, (h + 1) * head)
            gmap[c, r, h * head : (h + 1) * head] = rmap[c * per + h]
            gmap[c, r, cw + h * head : cw + (h + 1) * head] = imap[c * per + h]

    def relay(k, to, land, slot):
        @pl.when(inner == 1)
        def _():
            for a in range(N_SMALL):
                f = layer[k] * PLANE + p
                z_hop(a, arrays[a][0](f), f, slot, land, to).start()


    def ffn_along_z(a):
        for k in range(1, LAYERS):
            z_hop(a, piece(a, layer[k]), fs, k, lands[k], k).start()

    def mixer_step(k, to, land):
        for a in range(N_SMALL):
            z_done(a, k)
        relay(k, to, land, k + 1)
        for c in mixer_copies[k]:
            c.start()

    def mixer_corners(k):
        for a in range(N_SMALL):
            mixer_corner(a, k)

    mixer_corners(0)
    pld_x.start()
    mixer_step(1, 2, 3)

    @pl.when(inner == 1)
    def _():
        mixer_step(2, 1, 2)

    mixer_corners(1)
    tok_x[0].start()

    @pl.when(inner == 0)
    def _():
        mixer_step(2, 1, 2)
        ffn_along_z(3)

    mixer_corners(2)
    tok_x[1].start()
    mixer_step(3, 1, 3)

    @pl.when(inner == 1)
    def _():
        ffn_along_z(3)

    for n in range(2):
        with jax.named_scope("tok_x"):
            tok_x[n].wait_recv()
        tok_core[n].start()
    for a in range(N_SMALL):
        mixer_corner(a, LAYERS - 1)
    sides(3, 0)

    with jax.named_scope("tokens"):
        arrival(tok2.at[0], AT_MISC).wait_recv()
        pld_x.wait_recv()
    pld_v[1] = pld_b[1].astype(F32)
    with jax.named_scope("tokens"):
        own[2].wait()

    def norm_step(r, _):
        normed[r] = normed_rows(tok2[r].astype(F32), gain1[...].astype(F32)[None, :])
        return 0

    lax.fori_loop(0, 2, norm_step, 0)
    for c in own[3:8]:
        c.wait()
    mixer_done()

    def mixer_rows(r, _):
        place = position((rows, cw))
        branch = jnp.dot(normed[r], bo_all[:, channels], preferred_element_type=F32)
        branch = branch.astype(BF16).astype(F32)
        conv = rows_conv(branch, ctaps[:, channels].astype(F32), ctaps.shape[0], place).astype(BF16)
        gates = jax.nn.sigmoid(jnp.dot(conv, gmap[x], preferred_element_type=F32))
        la = -DECAY_RATE_GAIN * gates[:, :cw] * rate[:, channels] + pld_v[r]
        d = jnp.sqrt(negative_expm1(2.0 * la)) * gates[:, cw:] * conv.astype(F32)
        a = jnp.exp(la)
        step = 1
        while step < SEQ_LEN:
            d = a * shifted(d, step, place, 0.0) + d
            if step * 2 < SEQ_LEN:
                a = a * shifted(a, step, place, 1.0)
            step *= 2
        outgate = jnp.dot(
            normed[r],
            bo_all[:, pl.ds(pl.multiple_of(local_width + x * cw, cw), cw)],
            preferred_element_type=F32,
        )
        outgate = outgate.astype(BF16).astype(F32)
        mixed = (d * gelu(outgate)).astype(BF16)
        mix_give[r] = jnp.dot(mixed, mo_all[channels, their_half], preferred_element_type=F32).astype(BF16)
        mix_keep[r] = jnp.dot(mixed, mo_all[channels, mine_half], preferred_element_type=F32)
        return 0

    def mix_hop(r):
        return misc_hop(4 + r, mix_give.at[r], mix_pair.at[r], core_target)

    with jax.named_scope("mixer1"):
        lax.fori_loop(1, 2, mixer_rows, 0)
    mix_hop(1).start()
    with jax.named_scope("mixer0"):
        lax.fori_loop(0, 1, mixer_rows, 0)
    mix_hop(0).start()
    with jax.named_scope("swap1"):
        mix_hop(1).wait_recv()
    mix_out[...] = (mix_keep[1] + mix_pair[1].astype(F32)).astype(BF16)
    mix_x = misc_hop(6, mix_out, mix_in, x_target)
    mix_x.start()
    ffn_along_z(4)
    z_done(3, 1)
    sides(3, 1)
    corners(3, 0)
    for k in range(2, LAYERS):
        z_done(3, k)
        sides(3, k)
    with jax.named_scope("swap0"):
        mix_hop(0).wait_recv()
    mix_keep[0] = mix_keep[0] + mix_pair[0].astype(F32) + tok2[0, :, mine_half].astype(F32)
    with jax.named_scope("mix_x"):
        mix_x.wait_recv()
    after[:, mine_half] = (mix_keep[0] + mix_in[...].astype(F32)).astype(BF16)
    after_core = misc_hop(7, after.at[:, mine_half], after.at[:, mine_half], core_target)
    after_core.start()
    with jax.named_scope("after"):
        after_core.wait_recv()
    n2[0] = normed_rows(after[...].astype(F32), gain2[...].astype(F32)[None, :])


    def rows_hop(k, land, slot, to):
        return hop(
            n2.at[k, :, mine_half],
            n2.at[land, :, mine_half],
            sent.at[ROWS_RELAY if slot else ROWS],
            got.at[AT_ROWS + land],
            line[to],
        )

    @pl.when(inner == 1)
    def _():
        rows_hop(0, 2, 1, 2).start()

    rows_hop(0, 1, 0, 1).start()

    def rows_arrived(k, to, land):
        with jax.named_scope(f"rows{k}"):
            rows_hop(k, k, 0, 1).wait_recv()

        @pl.when(inner == 1)
        def _():
            rows_hop(k, land, k + 1, to).start()

        core_hop(k).start()

    def core_hop(k):
        block = n2.at[k, :, mine_half]
        return hop(block, block, sent.at[ROWS], got.at[AT_CORE + k], core_target)

    corners(3, 1)
    rows_arrived(1, 2, 3)
    corners(3, 2)

    @pl.when(inner == 1)
    def _():
        rows_arrived(2, 1, 2)

    corners(3, 3)
    z_done(4, 1)
    z_done(4, 2)
    down_a, down_b = down[0]
    for block in down[0]:
        sides(4, *block, kinds=(1,))

    @pl.when(inner == 1)
    def _():
        rows_arrived(3, 1, 3)

    @pl.when(inner == 0)
    def _():
        rows_arrived(2, 1, 2)

    block_rows = PLANE * deep

    def up_dot(k, at, blocks):
        total = None
        for of in blocks:
            where = span(layer[of], block_rows)
            s = jnp.dot(n2[k, :, where], gu_all[where, at], preferred_element_type=F32)
            total = s if total is None else total + s
        return total

    def up_early(k, _):
        with jax.named_scope("up_early"):
            for j in range(0, 2 * units, 4 * LANES):
                at = slice(j, min(j + 4 * LANES, 2 * units))
                part[k - 1, :, at] = up_dot(k, at, range(LAYERS - 1))
        return 0

    def up(k, late):
        place = position((rows, 4 * LANES))
        layer_taps = taps.at[z]
        width = gtaps.shape[0]

        def halves(j, n):
            at = slice(j, j + n)
            if late:
                s = part[k - 1, :, at] + up_dot(k, at, (LAYERS - 1,))
            else:
                s = jnp.dot(n2[k], gu_all[:, at], preferred_element_type=F32)
            return rows_conv(s.astype(BF16).astype(F32), layer_taps[0:width, at], width, place[:, :n])

        j = 0
        while j < 2 * full * LANES:
            n = min(4 * LANES, 2 * full * LANES - j)
            s = halves(j, n)
            for i in range(0, n, 2 * LANES):
                g, v = s[:, i : i + LANES], s[:, i + LANES : i + 2 * LANES]
                h = (j + i) // 2
                hidden[k, :, h : h + LANES] = (g * jax.nn.sigmoid(g) * v).astype(BF16)
            j += n
        if rest:
            s = halves(j, 2 * rest)
            h = s * jax.nn.sigmoid(s) * pltpu.roll(s, rest, 1)
            lane = lax.broadcasted_iota(jnp.int32, h.shape, 1)
            hidden[k, :, full * LANES : (full + 1) * LANES] = jnp.where(lane < rest, h, 0.0).astype(BF16)

    def up_step(k, _):
        with jax.named_scope("up"):
            up(k, False)
        return 0

    def up_late(k, _):
        with jax.named_scope("up_late"):
            up(k, True)
        return 0

    turn = (tp + z // 2) % 2
    quarter = PLANE * wide // 2

    def columns_of(j, mine):
        first, second = down[j // 2][0][1], down[j // 2][1][1]
        side = turn if mine else 1 - turn
        block = first * (1 - side) + second * side
        return block * 2 + (y if j % 2 == 0 else 1 - y)

    def place_of(j):
        return columns_of(j, True) % (half // quarter)

    def pair_hop(j, k):
        return hop(give.at[j, k], pair.at[j, k], sent.at[PAIR], got.at[AT_PAIR + j * LAYERS + k], core_target)

    def to_partner(j, k):
        landing = arrive.at[0, j] if k == 1 else joint.at[j, k - 2]
        group = NEAR if k == 1 else FAR
        return hop(paired.at[j, k], landing, sent.at[group], got.at[AT_BACK + j * LAYERS + k], line[1])

    def to_layer(j, k):
        return hop(joint.at[j, k], arrive.at[1, j], sent.at[FAR], got.at[AT_BACK + j * LAYERS], line[k + 2])

    def part_sums(*parts):
        for j, k in parts:
            given = span(columns_of(j, False), quarter)
            give[j, k] = jnp.dot(hidden[k], dn_all[:, given], preferred_element_type=F32).astype(BF16)
            pair_hop(j, k).start()
        for j, k in parts:
            kept = span(columns_of(j, True), quarter)
            keep = jnp.dot(hidden[k], dn_all[:, kept], preferred_element_type=F32)
            with jax.named_scope(f"pair{j}{k}"):
                pair_hop(j, k).wait_recv()
            paired[j, k] = (keep + pair[j, k].astype(F32)).astype(BF16)
            if k > 1:

                @pl.when(inner == 0)
                def _():
                    to_partner(j, k).start()

            elif k == 1:
                to_partner(j, 1).start()

    def joint_sums(j, k):
        @pl.when(inner == 1)
        def _():
            with jax.named_scope(f"joint{j}{k}"):
                to_partner(j, k + 2).wait_recv()
            joint[j, k] = (joint[j, k].astype(F32) + paired[j, k + 2].astype(F32)).astype(BF16)
            to_layer(j, k).start()

    corners_done(3, False)
    for block in down[0]:
        sides(4, *block, kinds=(2,))
    with jax.named_scope("across12"):
        core_hop(1).wait_recv()
        core_hop(2).wait_recv()
    lax.fori_loop(1, 3, up_early, 0)
    corners_done(3, True)
    lax.fori_loop(1, 3, up_late, 0)
    z_done(4, 3)
    for block in down[0]:
        corners(4, *block, kinds=(1,))
    part_sums((0, 2))
    corners(4, *down_a, kinds=(2,))
    part_sums((0, 1))
    corners(4, *down_b, kinds=(2,))
    for block in down[1]:
        sides(4, *block)

    @pl.when(inner == 0)
    def _():
        rows_arrived(3, 1, 3)

    with jax.named_scope("across3"):
        core_hop(3).wait_recv()
    lax.fori_loop(3, 4, up_step, 0)
    part_sums((0, 3))
    corners_done(4, False)
    part_sums((1, 2), (1, 1), (1, 3))
    joint_sums(0, 0)
    corners(4, *down[1][0])
    corners(4, *down[1][1], kinds=(1,))
    part_sums((2, 3), (2, 2), (2, 1))
    corners(4, *down[1][1], kinds=(2,))
    joint_sums(0, 1)
    joint_sums(1, 0)
    corners_done(4, True)
    part_sums((3, 3), (3, 2), (3, 1))
    joint_sums(1, 1)
    joint_sums(2, 1)
    lax.fori_loop(0, 1, up_step, 0)
    joint_sums(2, 0)
    part_sums((0, 0), (1, 0))
    joint_sums(3, 1)
    joint_sums(3, 0)
    part_sums((2, 0), (3, 0))

    stores = []
    for j in range(LAYERS):
        with jax.named_scope(f"near{j}"):
            to_partner(j, 1).wait_recv()
        with jax.named_scope(f"far{j}"):
            to_layer(j, 0).wait_recv()
        total = paired[j, 0].astype(F32) + arrive[0, j].astype(F32) + arrive[1, j].astype(F32)
        first = pl.multiple_of(tp * half + place_of(j) * quarter, quarter)
        out_v[j] = (after[:, pl.ds(first, quarter)].astype(F32) + total).astype(BF16)
        stores.append(pltpu.make_async_copy(out_v.at[j], out.at[:, span(place_of(j), quarter)], local.at[j]))
        stores[j].start()

    def all_sent(group, block):
        hop(block, block, sent.at[group], got.at[0], core_target).wait_send()

    with jax.named_scope("sent"):
        every = slice(None)
        all_sent(MIX, bo_all.at[pl.ds(0, 3 * N_SMALL * LAYERS * deep // 4), :])
        all_sent(UP, gu_all.at[pl.ds(0, 3 * LAYERS * deep), :])
        all_sent(DOWN, dn_all.at[pl.ds(0, units), pl.ds(0, 3 * LAYERS * wide)])
        all_sent(MIX_Z, bo_all.at[pl.ds(0, N_SMALL * deep // 2), :])
        all_sent(UP_Z, gu_all.at[pl.ds(0, 3 * deep), :])
        all_sent(DOWN_Z, dn_all.at[pl.ds(0, units), pl.ds(0, 3 * wide)])
        all_sent(ROWS, n2.at[pl.ds(0, 2)])
        all_sent(MISC, bo_all.at[pl.ds(0, MISC_QUARTERS * rows * half // bo_all.shape[1] // 4), :])
        all_sent(PAIR, give)
        all_sent(NEAR, arrive.at[0])
        all_sent(FAR, joint)

        @pl.when(inner == 1)
        def _():
            all_sent(MIX_RELAY, bo_all.at[pl.ds(0, LAYERS * N_SMALL * deep // 2), :])
            all_sent(ROWS_RELAY, n2.at[pl.ds(0, 2)])

    with jax.named_scope("stores"):
        for c in stores:
            c.wait()


def fused_layer(
    tokens,
    mixer_norm_gain,
    recurrence_branch_weight,
    output_gate_projection,
    recurrence_conv_taps,
    recurrence_gate_map,
    input_gate_map,
    channel_decay_rate,
    position_log_decay,
    mixer_output_weight,
    feedforward_norm_gain,
    gate_up_weight,
    value_up_weight,
    gate_conv_taps,
    value_conv_taps,
    down_projection_weight,
):
    rows, half = tokens.shape
    deep, local_width = recurrence_branch_weight.shape
    wide = mixer_output_weight.shape[1]
    n_fs = LAYERS * PLANE
    features = 2 * half
    local_units = gate_up_weight.shape[1]
    units = local_units // LAYERS
    padded = -(-units // (2 * LANES)) * 2 * LANES
    cw = local_width // 2
    quarter = PLANE * wide // 2
    dma = pltpu.SemaphoreType.DMA
    scratch = [
        pltpu.VMEM((2, rows, features), BF16),
        pltpu.VMEM((n_fs * deep, 2 * local_width), BF16),
        pltpu.VMEM((local_width, n_fs * wide), BF16),
        pltpu.VMEM((deep, local_units), BF16),
        pltpu.VMEM((deep, local_units), BF16),
        pltpu.VMEM((LAYERS, deep, 2 * units), BF16),
        pltpu.VMEM((n_fs * deep, 2 * units), BF16),
        pltpu.VMEM((padded, n_fs * wide), BF16),
        pltpu.VMEM((LAYERS, 8, 2 * units), F32),
        pltpu.VMEM((local_width // cw, cw, 2 * cw), BF16),
        pltpu.VMEM((2, rows, cw), F32),
        pltpu.VMEM((2, rows, features), BF16),
        pltpu.VMEM((2, rows, half), BF16),
        pltpu.VMEM((2, rows, half), F32),
        pltpu.VMEM((2, rows, half), BF16),
        pltpu.VMEM((rows, half), BF16),
        pltpu.VMEM((rows, half), BF16),
        pltpu.VMEM((rows, features), BF16),
        pltpu.VMEM((LAYERS, rows, features), BF16),
        pltpu.VMEM((LAYERS, rows, padded), BF16),
        pltpu.VMEM((LAYERS, LAYERS, rows, quarter), BF16),
        pltpu.VMEM((LAYERS, LAYERS, rows, quarter), BF16),
        pltpu.VMEM((LAYERS, LAYERS, rows, quarter), BF16),
        pltpu.VMEM((2, LAYERS, rows, quarter), BF16),
        pltpu.VMEM((LAYERS, 2, rows, quarter), BF16),
        pltpu.VMEM((LAYERS, rows, quarter), BF16),
        pltpu.VMEM((2, rows, 2 * units), F32),
        pltpu.VMEM((2, rows, cw), BF16),
        dma((N_SENT,)),
        dma((AT_BACK + LAYERS * LAYERS,)),
        dma((9,)),
    ]
    return pl.pallas_call(
        layer_kernel,
        out_shape=jax.ShapeDtypeStruct((rows, half), BF16),
        in_specs=[ANY, VMEM, ANY, ANY, VMEM, VMEM, VMEM, VMEM, ANY, ANY, VMEM, ANY, ANY, VMEM, VMEM, ANY],
        out_specs=ANY,
        scratch_shapes=scratch,
        compiler_params=pltpu.CompilerParams(
            collective_id=0, has_side_effects=True, vmem_limit_bytes=62 * 2**20
        ),
        name="layer",
    )(
        tokens,
        mixer_norm_gain,
        recurrence_branch_weight,
        output_gate_projection,
        recurrence_conv_taps,
        recurrence_gate_map,
        input_gate_map,
        channel_decay_rate.reshape(1, -1),
        position_log_decay,
        mixer_output_weight,
        feedforward_norm_gain,
        gate_up_weight,
        value_up_weight,
        gate_conv_taps,
        value_conv_taps,
        down_projection_weight,
    )


def solution(mesh):
    placed = (
        P("fs", "tp"),
        P(),
        P("fs", "tp"),
        P("fs", "tp"),
        P(None, "tp"),
        P("tp", None, None),
        P("tp", None, None),
        P("tp"),
        P("fs", "tp"),
        P("tp", "fs"),
        P(),
        P("fs", "tp"),
        P("fs", "tp"),
        P(None, "tp"),
        P(None, "tp"),
        P("tp", "fs"),
    )
    fused = mesh.shape["tp"] == 2 and mesh.shape["fs"] == LAYERS * PLANE
    body = fused_layer if fused else gathered_layer
    return jax.shard_map(
        body, mesh=mesh, in_specs=placed, out_specs=P("fs", "tp"), check_vma=False
    )
```

```python
import functools

import jax
import jax.numpy as jnp
from jax import lax
from jax.experimental import pallas as pl
from jax.experimental.pallas import tpu as pltpu
from jax.sharding import PartitionSpec as P

SEQ_LEN = 64


EPS = 1e-06
DECAY_RATE_GAIN = 8.0


def rms_normed(values, gain):
    wide = values.astype(jnp.float32)
    factor = lax.rsqrt(jnp.mean(wide * wide, axis=-1, keepdims=True) + EPS)
    return (wide * factor * gain.astype(jnp.float32)).astype(jnp.bfloat16)


def causal_conv(values, kernel):
    width = kernel.shape[0]
    row_count, channels = values.shape
    grouped = values.astype(jnp.float32).reshape(row_count // SEQ_LEN, SEQ_LEN, channels)
    padded = jnp.pad(grouped, ((0, 0), (width - 1, 0), (0, 0)))
    summed = padded[:, 0:SEQ_LEN] * kernel[0].astype(jnp.float32)
    for offset in range(1, width):
        summed = summed + padded[:, offset : offset + SEQ_LEN] * kernel[offset].astype(jnp.float32)
    return summed.reshape(row_count, channels)


def combine(left, right):
    first_a, first_b = left
    second_a, second_b = right
    return (first_a * second_a, second_a * first_b + second_b)


def pair_folder(normed, pieces):
    return (
        jnp.dot(normed, pieces[0], preferred_element_type=jnp.float32),
        jnp.dot(normed, pieces[1], preferred_element_type=jnp.float32),
    )


def gathered_layer(
    tokens,
    mixer_norm_gain,
    recurrence_branch_weight,
    output_gate_projection,
    recurrence_conv_taps,
    recurrence_gate_map,
    input_gate_map,
    channel_decay_rate,
    position_log_decay,
    mixer_output_weight,
    feedforward_norm_gain,
    gate_up_weight,
    value_up_weight,
    gate_conv_taps,
    value_conv_taps,
    down_projection_weight,
):
    row_count = tokens.shape[0]
    local_width = recurrence_branch_weight.shape[1]
    local_heads = recurrence_gate_map.shape[0]
    head_size = recurrence_gate_map.shape[1]
    whole_rows = lax.all_gather(tokens, "tp", axis=1, tiled=True)
    normed = rms_normed(whole_rows, mixer_norm_gain)
    branch_sum, outgate_sum = pair_folder(
        normed,
        (
            lax.all_gather(recurrence_branch_weight, "fs", axis=0, tiled=True),
            lax.all_gather(output_gate_projection, "fs", axis=0, tiled=True),
        ),
    )
    branch = branch_sum.astype(jnp.bfloat16)
    outgate = outgate_sum.astype(jnp.bfloat16)
    conv = causal_conv(branch, recurrence_conv_taps).astype(jnp.bfloat16)
    grouped = conv.reshape(row_count, local_heads, head_size)
    recurrence_scan = jax.nn.sigmoid(
        jnp.einsum(
            "rhi,hij->rhj", grouped, recurrence_gate_map, preferred_element_type=jnp.float32
        ).reshape(row_count, local_width)
    )
    inner = jax.nn.sigmoid(
        jnp.einsum(
            "rhi,hij->rhj", grouped, input_gate_map, preferred_element_type=jnp.float32
        ).reshape(row_count, local_width)
    )
    log_alpha = (
        -DECAY_RATE_GAIN * recurrence_scan * channel_decay_rate[None, :] + position_log_decay
    )
    drive = jnp.sqrt(-jnp.expm1(2.0 * log_alpha)) * inner * conv.astype(jnp.float32)
    shape3 = (row_count // SEQ_LEN, SEQ_LEN, local_width)
    unused, state = lax.associative_scan(
        combine, (jnp.exp(log_alpha).reshape(shape3), drive.reshape(shape3)), axis=1
    )
    state = state.reshape(row_count, local_width)
    mixed = (state * jax.nn.gelu(outgate.astype(jnp.float32))).astype(jnp.bfloat16)
    mixer_terms = jnp.dot(
        mixed,
        lax.all_gather(mixer_output_weight, "fs", axis=1, tiled=True),
        preferred_element_type=jnp.float32,
    )
    mixer_terms = mixer_terms.astype(jnp.bfloat16).astype(jnp.float32)
    mixer_whole = lax.psum(mixer_terms.astype(jnp.bfloat16), "tp").astype(jnp.float32)
    whole_after = (whole_rows.astype(jnp.float32) + mixer_whole).astype(jnp.bfloat16)
    normed2 = rms_normed(whole_after, feedforward_norm_gain)
    gate_whole, value_whole = (
        lax.all_gather(gate_up_weight, "fs", axis=0, tiled=True),
        lax.all_gather(value_up_weight, "fs", axis=0, tiled=True),
    )
    gate_sum = jnp.dot(normed2, gate_whole, preferred_element_type=jnp.float32)
    value_sum = jnp.dot(normed2, value_whole, preferred_element_type=jnp.float32)
    gate_half = gate_sum.astype(jnp.bfloat16)
    value_half = value_sum.astype(jnp.bfloat16)
    hidden = (
        jax.nn.silu(causal_conv(gate_half, gate_conv_taps))
        * causal_conv(value_half, value_conv_taps)
    ).astype(jnp.bfloat16)
    channel_terms = jnp.dot(
        hidden,
        lax.all_gather(down_projection_weight, "fs", axis=1, tiled=True),
        preferred_element_type=jnp.float32,
    )
    channel_terms = channel_terms.astype(jnp.bfloat16).astype(jnp.float32)
    channel_share = lax.psum_scatter(
        channel_terms.astype(jnp.bfloat16), "tp", scatter_dimension=1, tiled=True
    ).astype(jnp.float32)
    share_width = channel_share.shape[1]
    residual_share = lax.dynamic_slice_in_dim(
        whole_after, lax.axis_index("tp") * share_width, share_width, 1
    )
    return (residual_share.astype(jnp.float32) + channel_share).astype(jnp.bfloat16)


PLANE = 4
LAYERS = 4
LANES = 128
ANY = pl.BlockSpec(memory_space=pl.ANY)
VMEM = pl.BlockSpec(memory_space=pltpu.VMEM)
F32, BF16 = jnp.float32, jnp.bfloat16
N_SMALL, N_BIG = 3, 5
ROWS_CUT = 6
MISC_QUARTERS = 29
N_SENT = 13
AT_Z = 0
AT_MIX = AT_Z + N_BIG * LAYERS
AT_MIX_DONE = AT_MIX + N_SMALL * LAYERS
AT_SIDE = AT_MIX_DONE + 2
AT_CORNER = AT_SIDE + 2 * 2 * LAYERS
AT_MISC = AT_CORNER + 2 * 2 * 2
AT_ROWS = AT_MISC + 8
AT_CORE = AT_ROWS + LAYERS
AT_PAIR = AT_CORE + LAYERS
AT_BACK = AT_PAIR + LAYERS * LAYERS


def hop(src, dst, send, recv, target):
    return pltpu.make_async_remote_copy(
        src_ref=src,
        dst_ref=dst,
        send_sem=send,
        recv_sem=recv,
        device_id=target,
        device_id_type=pl.DeviceIdType.MESH,
    )


def greet(targets):
    barrier = pltpu.get_barrier_semaphore()
    for target in targets:
        pl.semaphore_signal(
            barrier, inc=1, device_id=target, device_id_type=pl.DeviceIdType.MESH
        )
    pl.semaphore_wait(barrier, len(targets))


def span(index, size):
    return pl.ds(pl.multiple_of(index * size, size), size)


def row_blocks(whole, deep, columns):
    cut = ROWS_CUT * deep // 8

    def at(f, part=None):
        if part is None:
            return whole.at[span(f, deep), columns]
        start, size = ((0, cut), (cut, deep - cut))[part]
        return whole.at[pl.ds(pl.multiple_of(f * deep + start, 16), size), columns]

    return at


def column_blocks(whole, rows, wide):
    cut = rows // 2 // 16 * 16

    def at(f, part=None):
        start, size = ((0, rows) if part is None else ((0, cut), (cut, rows - cut))[part])
        return whole.at[pl.ds(start, size), span(f, wide)]

    return at


def position(shape):
    return lax.broadcasted_iota(jnp.int32, shape, 0) % SEQ_LEN


def shifted(values, distance, place, fill):
    return jnp.where(place >= distance, pltpu.roll(values, distance, 0), fill)


def rows_conv(values, taps, width, place):
    summed = shifted(values, width - 1, place, 0.0) * taps[0:1, :]
    for j in range(1, width - 1):
        summed = summed + shifted(values, width - 1 - j, place, 0.0) * taps[j : j + 1, :]
    return summed + values * taps[width - 1 : width, :]


def negative_expm1(x):
    near = 1.0 + x * (1.0 / 8.0)
    for n in range(7, 1, -1):
        near = 1.0 + x * (1.0 / n) * near
    return jnp.where(jnp.abs(x) < 0.4, -x * near, 1.0 - jnp.exp(x))


def normed_rows(values, gain):
    factor = lax.rsqrt(jnp.mean(values * values, axis=-1, keepdims=True) + EPS)
    return (values * factor * gain).astype(BF16)


def gelu(x):
    return 0.5 * x * (1.0 + jnp.tanh(0.7978845608028654 * (x + 0.044715 * (x * x * x))))


def layer_kernel(
    tok, gain1, rb, og, ctaps, rmap, imap, rate, pld, mo, gain2, gup, vup, gtaps, vtaps, dn,
    out,
    tok2, bo_all, mo_all, gup_v, vup_v, stage, gu_all, dn_all, taps, gmap, pld_v,
    normed, mix_give, mix_keep, mix_pair, mix_out, mix_in, after, n2, hidden, give, pair, paired, arrive, joint, out_v, part, pld_b,
    sent, got, local,
):
    fs, tp = lax.axis_index("fs"), lax.axis_index("tp")
    z, p = fs // PLANE, fs % PLANE
    y, x = p // 2, p % 2
    px, py = y * 2 + 1 - x, (1 - y) * 2 + x
    inner = ((z + 1) // 2) % 2
    layer = (z, z + 1 - 2 * (z % 2), 2 - z // 2, 3 - 3 * (z // 2))
    lands = (0, 1, 3 - inner, 3 - inner)
    down = (
        ((1 - inner, 1 + z // 2), (2, layer[2])),
        ((inner, 3 * (z // 2)), (3, layer[3])),
    )
    line = [(zz * PLANE + p, tp) for zz in layer]
    x_target, y_target = (z * PLANE + px, tp), (z * PLANE + py, tp)
    core_target = (fs, 1 - tp)
    with jax.named_scope("greet"):
        greet(line[1:] + [x_target, y_target, core_target])

    rows, half = tok.shape
    deep, local_width = rb.shape
    wide = mo.shape[1]
    units = dn.shape[0] // LAYERS
    full, rest = units // LANES, units % LANES
    cw = gmap.shape[1]
    mine_half, their_half, channels = span(tp, half), span(1 - tp, half), span(x, cw)
    heads, head = rmap.shape[:2]
    per = cw // head

    arrays = (
        (row_blocks(bo_all, deep, pl.ds(0, local_width)), rb),
        (row_blocks(bo_all, deep, pl.ds(local_width, local_width)), og),
        (column_blocks(mo_all, mo.shape[0], wide), mo),
        (row_blocks(gu_all, deep, slice(None)), None),
        (column_blocks(dn_all, units, wide), None),
    )

    def piece(a, zz):
        if a < N_SMALL:
            return arrays[a][1]
        return stage.at[zz] if a == 3 else dn.at[span(zz, units), :]

    MIX, UP, DOWN, MIX_Z, MIX_RELAY, UP_Z, DOWN_Z, ROWS, ROWS_RELAY, MISC, PAIR, NEAR, FAR = range(N_SENT)

    def misc_hop(n, source, to, target):
        return hop(source, to, sent.at[MISC], got.at[AT_MISC + n], target)

    def arrival(block, n):
        return hop(block, block, sent.at[MISC], got.at[n], core_target)

    def mixer_part(a, f, h):
        if a < 2:
            columns = pl.ds(pl.multiple_of(a * local_width + h * cw, cw), cw)
            return bo_all.at[span(f, deep), columns]
        return mo_all.at[span(h, cw), span(f, wide)]

    def own_part_of(a, h):
        return mo.at[span(h, cw), :] if a == 2 else arrays[a][1].at[:, span(h, cw)]

    def z_hop(a, source, f, slot, land, to):
        group = (UP_Z, DOWN_Z)[a - N_SMALL] if a >= N_SMALL else MIX_RELAY if slot else MIX_Z
        return hop(source, arrays[a][0](f), sent.at[group], got.at[AT_Z + a * LAYERS + land], line[to])

    def side_at(a, k, kind):
        return AT_SIDE + ((a - N_SMALL) * 2 + kind - 1) * LAYERS + k

    def corner_at(a, late, kind):
        return AT_CORNER + ((a - N_SMALL) * 2 + late) * 2 + kind - 1

    def sides(a, k, of=None, kinds=(1, 2)):
        at = arrays[a][0]
        f = (layer[k] if of is None else of) * PLANE + p
        source = piece(a, z) if of is None and k == 0 else at(f)
        for kind in kinds:
            target = (x_target, y_target)[kind - 1]
            hop(source, at(f), sent.at[UP + a - N_SMALL], got.at[side_at(a, k, kind)], target).start()

    def mixer_sides(a, k):
        copies = []
        f = layer[k] * PLANE + p
        for kind, h, target in ((1, 1 - x, x_target), (2, x, y_target)):
            to = mixer_part(a, f, h)
            source = own_part_of(a, h) if k == 0 else to
            n = AT_MIX + a * LAYERS + k if kind == 1 else AT_MIX_DONE
            copies.append(hop(source, to, sent.at[MIX], got.at[n], target))
        return copies

    def mixer_corner(a, k):
        block = mixer_part(a, layer[k] * PLANE + px, x)
        with jax.named_scope(f"side{a}{k}"):
            arrival(block, AT_MIX + a * LAYERS + k).wait_recv()
        hop(block, block, sent.at[MIX], got.at[AT_MIX_DONE + 1], y_target).start()

    def mixer_done():
        block = bo_all.at[pl.ds(0, N_SMALL * LAYERS * deep // 4), :]
        for n in range(2):
            with jax.named_scope(f"mixer_done{n}"):
                arrival(block, AT_MIX_DONE + n).wait_recv()

    def corners(a, k, of=None, kinds=(1, 2)):
        at = arrays[a][0]
        base = (layer[k] if of is None else of) * PLANE
        late = k == LAYERS - 1 if a == N_SMALL else of is down[1][0][1] or of is down[1][1][1]
        for kind, part, owner, target in ((1, 0, px, y_target), (2, 1, py, x_target)):
            if kind not in kinds:
                continue
            with jax.named_scope(f"side{a}{k if of is None else 9}{kind}"):
                arrival(at(base + owner), side_at(a, k, kind)).wait_recv()
            block = at(base + owner, part)
            hop(block, block, sent.at[UP + a - N_SMALL], got.at[corner_at(a, late, kind)], target).start()

    def corners_done(a, late):
        count = (1 if late else LAYERS - 1) if a == N_SMALL else 2
        for kind in (1, 2):
            if a == N_SMALL:
                block = gu_all.at[pl.ds(0, count * (ROWS_CUT * deep // 8 if kind == 1 else deep - ROWS_CUT * deep // 8)), :]
            else:
                block = dn_all.at[pl.ds(0, units // 2), pl.ds(0, count * wide)]
            with jax.named_scope(f"corner{a}{int(late)}{kind}"):
                arrival(block, corner_at(a, late, kind)).wait_recv()

    def z_done(a, k):
        block = arrays[a][0](layer[k] * PLANE + p)
        with jax.named_scope(f"z{a}{k}"):
            arrival(block, AT_Z + a * LAYERS + k).wait_recv()

    @pl.when(inner == 1)
    def _():
        for a in range(N_SMALL):
            z_hop(a, piece(a, z), fs, 1, 2, 2).start()

    for a in range(N_SMALL):
        z_hop(a, piece(a, z), fs, 0, 1, 1).start()
    mixer_copies = [[c for a in range(N_SMALL) for c in mixer_sides(a, k)] for k in range(LAYERS)]
    for c in mixer_copies[0]:
        c.start()
    tok_swap = misc_hop(0, tok, tok2.at[0, :, mine_half], core_target)

    def tok_hop(n, target):
        piece_rows = pl.ds(n % 2 * (rows // 2), rows // 2)
        block = tok2.at[1, piece_rows, mine_half]
        return misc_hop(1 + n if n < 2 else 0, tok.at[piece_rows, :] if n < 2 else block, block, target)

    tok_x = [tok_hop(n, x_target) for n in range(2)]
    tok_core = [tok_hop(n, core_target) for n in (2, 3)]
    pld_x = misc_hop(3, pld_b.at[0], pld_b.at[1], x_target)
    tok_swap.start()

    own = [
        pltpu.make_async_copy(gup, gup_v, local.at[0]),
        pltpu.make_async_copy(vup, vup_v, local.at[1]),
        pltpu.make_async_copy(tok, tok2.at[0, :, mine_half], local.at[2]),
        pltpu.make_async_copy(pld.at[:, channels], pld_v.at[0], local.at[3]),
        pltpu.make_async_copy(rb, arrays[0][0](fs), local.at[4]),
        pltpu.make_async_copy(og, arrays[1][0](fs), local.at[5]),
        pltpu.make_async_copy(mo, arrays[2][0](fs), local.at[6]),
        pltpu.make_async_copy(piece(4, z), arrays[4][0](fs), local.at[7]),
        pltpu.make_async_copy(pld.at[:, span(1 - x, cw)], pld_v.at[1], local.at[8]),
    ]
    for c in own:
        c.start()

    own[8].wait()
    pld_b[0] = pld_v[1].astype(BF16)
    own[0].wait()
    own[1].wait()

    def arrange(gate, value, zz, store):
        for j in range(full):
            at = zz * units + j * LANES
            store(2 * j * LANES, gate[:, at : at + LANES])
            store((2 * j + 1) * LANES, value[:, at : at + LANES])
        if rest:
            at = zz * units + full * LANES
            store(2 * full * LANES, gate[:, at : at + rest])
            store(2 * full * LANES + rest, value[:, at : at + rest])

    for zz in range(LAYERS):

        def put(at, v, zz=zz):
            stage[zz, :, at : at + v.shape[1]] = v

        def put_taps(at, v, zz=zz):
            taps[zz, 0 : v.shape[0], at : at + v.shape[1]] = v.astype(F32)

        arrange(gup_v, vup_v, zz, put)
        arrange(gtaps, vtaps, zz, put_taps)
    gu_all[span(fs, deep), :] = stage[z]
    dn_all[units:, :] = jnp.zeros((dn_all.shape[0] - units, dn_all.shape[1]), BF16)
    gmap[...] = jnp.zeros(gmap.shape, BF16)
    for c in range(heads // per):
        for h in range(per):
            r = slice(h * head, (h + 1) * head)
            gmap[c, r, h * head : (h + 1) * head] = rmap[c * per + h]
            gmap[c, r, cw + h * head : cw + (h + 1) * head] = imap[c * per + h]

    def relay(k, to, land, slot):
        @pl.when(inner == 1)
        def _():
            for a in range(N_SMALL):
                f = layer[k] * PLANE + p
                z_hop(a, arrays[a][0](f), f, slot, land, to).start()


    def ffn_along_z(a):
        for k in range(1, LAYERS):
            z_hop(a, piece(a, layer[k]), fs, k, lands[k], k).start()

    def mixer_step(k, to, land):
        for a in range(N_SMALL):
            z_done(a, k)
        relay(k, to, land, k + 1)
        for c in mixer_copies[k]:
            c.start()

    def mixer_corners(k):
        for a in range(N_SMALL):
            mixer_corner(a, k)

    mixer_corners(0)
    pld_x.start()
    mixer_step(1, 2, 3)

    @pl.when(inner == 1)
    def _():
        mixer_step(2, 1, 2)

    mixer_corners(1)
    tok_x[0].start()

    @pl.when(inner == 0)
    def _():
        mixer_step(2, 1, 2)
        ffn_along_z(3)

    mixer_corners(2)
    tok_x[1].start()
    mixer_step(3, 1, 3)

    @pl.when(inner == 1)
    def _():
        ffn_along_z(3)

    for n in range(2):
        with jax.named_scope("tok_x"):
            tok_x[n].wait_recv()
        tok_core[n].start()
    for a in range(N_SMALL):
        mixer_corner(a, LAYERS - 1)
    sides(3, 0)

    with jax.named_scope("tokens"):
        arrival(tok2.at[0], AT_MISC).wait_recv()
        pld_x.wait_recv()
    pld_v[1] = pld_b[1].astype(F32)
    with jax.named_scope("tokens"):
        own[2].wait()

    def norm_step(r, _):
        normed[r] = normed_rows(tok2[r].astype(F32), gain1[...].astype(F32)[None, :])
        return 0

    lax.fori_loop(0, 2, norm_step, 0)
    for c in own[3:8]:
        c.wait()
    mixer_done()

    def mixer_rows(r, _):
        place = position((rows, cw))
        branch = jnp.dot(normed[r], bo_all[:, channels], preferred_element_type=F32)
        branch = branch.astype(BF16).astype(F32)
        conv = rows_conv(branch, ctaps[:, channels].astype(F32), ctaps.shape[0], place).astype(BF16)
        gates = jax.nn.sigmoid(jnp.dot(conv, gmap[x], preferred_element_type=F32))
        la = -DECAY_RATE_GAIN * gates[:, :cw] * rate[:, channels] + pld_v[r]
        d = jnp.sqrt(negative_expm1(2.0 * la)) * gates[:, cw:] * conv.astype(F32)
        a = jnp.exp(la)
        step = 1
        while step < SEQ_LEN:
            d = a * shifted(d, step, place, 0.0) + d
            if step * 2 < SEQ_LEN:
                a = a * shifted(a, step, place, 1.0)
            step *= 2
        outgate = jnp.dot(
            normed[r],
            bo_all[:, pl.ds(pl.multiple_of(local_width + x * cw, cw), cw)],
            preferred_element_type=F32,
        )
        outgate = outgate.astype(BF16).astype(F32)
        mixed = (d * gelu(outgate)).astype(BF16)
        mix_give[r] = jnp.dot(mixed, mo_all[channels, their_half], preferred_element_type=F32).astype(BF16)
        mix_keep[r] = jnp.dot(mixed, mo_all[channels, mine_half], preferred_element_type=F32)
        return 0

    def mix_hop(r):
        return misc_hop(4 + r, mix_give.at[r], mix_pair.at[r], core_target)

    with jax.named_scope("mixer1"):
        lax.fori_loop(1, 2, mixer_rows, 0)
    mix_hop(1).start()
    with jax.named_scope("mixer0"):
        lax.fori_loop(0, 1, mixer_rows, 0)
    mix_hop(0).start()
    with jax.named_scope("swap1"):
        mix_hop(1).wait_recv()
    mix_out[...] = (mix_keep[1] + mix_pair[1].astype(F32)).astype(BF16)
    mix_x = misc_hop(6, mix_out, mix_in, x_target)
    mix_x.start()
    ffn_along_z(4)
    z_done(3, 1)
    sides(3, 1)
    corners(3, 0)
    for k in range(2, LAYERS):
        z_done(3, k)
        sides(3, k)
    with jax.named_scope("swap0"):
        mix_hop(0).wait_recv()
    mix_keep[0] = mix_keep[0] + mix_pair[0].astype(F32) + tok2[0, :, mine_half].astype(F32)
    with jax.named_scope("mix_x"):
        mix_x.wait_recv()
    after[:, mine_half] = (mix_keep[0] + mix_in[...].astype(F32)).astype(BF16)
    after_core = misc_hop(7, after.at[:, mine_half], after.at[:, mine_half], core_target)
    after_core.start()
    with jax.named_scope("after"):
        after_core.wait_recv()
    n2[0] = normed_rows(after[...].astype(F32), gain2[...].astype(F32)[None, :])


    def rows_hop(k, land, slot, to):
        return hop(
            n2.at[k, :, mine_half],
            n2.at[land, :, mine_half],
            sent.at[ROWS_RELAY if slot else ROWS],
            got.at[AT_ROWS + land],
            line[to],
        )

    @pl.when(inner == 1)
    def _():
        rows_hop(0, 2, 1, 2).start()

    rows_hop(0, 1, 0, 1).start()

    def rows_arrived(k, to, land):
        with jax.named_scope(f"rows{k}"):
            rows_hop(k, k, 0, 1).wait_recv()

        @pl.when(inner == 1)
        def _():
            rows_hop(k, land, k + 1, to).start()

        core_hop(k).start()

    def core_hop(k):
        block = n2.at[k, :, mine_half]
        return hop(block, block, sent.at[ROWS], got.at[AT_CORE + k], core_target)

    corners(3, 1)
    rows_arrived(1, 2, 3)
    corners(3, 2)

    @pl.when(inner == 1)
    def _():
        rows_arrived(2, 1, 2)

    corners(3, 3)
    z_done(4, 1)
    z_done(4, 2)
    down_a, down_b = down[0]
    for block in down[0]:
        sides(4, *block, kinds=(1,))

    @pl.when(inner == 1)
    def _():
        rows_arrived(3, 1, 3)

    @pl.when(inner == 0)
    def _():
        rows_arrived(2, 1, 2)

    block_rows = PLANE * deep

    def up_dot(k, at, blocks):
        total = None
        for of in blocks:
            where = span(layer[of], block_rows)
            s = jnp.dot(n2[k, :, where], gu_all[where, at], preferred_element_type=F32)
            total = s if total is None else total + s
        return total

    def up_early(k, _):
        with jax.named_scope("up_early"):
            for j in range(0, 2 * units, 4 * LANES):
                at = slice(j, min(j + 4 * LANES, 2 * units))
                part[k - 1, :, at] = up_dot(k, at, range(LAYERS - 1))
        return 0

    def up(k, late):
        place = position((rows, 4 * LANES))
        layer_taps = taps.at[z]
        width = gtaps.shape[0]

        def halves(j, n):
            at = slice(j, j + n)
            if late:
                s = part[k - 1, :, at] + up_dot(k, at, (LAYERS - 1,))
            else:
                s = jnp.dot(n2[k], gu_all[:, at], preferred_element_type=F32)
            return rows_conv(s.astype(BF16).astype(F32), layer_taps[0:width, at], width, place[:, :n])

        j = 0
        while j < 2 * full * LANES:
            n = min(4 * LANES, 2 * full * LANES - j)
            s = halves(j, n)
            for i in range(0, n, 2 * LANES):
                g, v = s[:, i : i + LANES], s[:, i + LANES : i + 2 * LANES]
                h = (j + i) // 2
                hidden[k, :, h : h + LANES] = (g * jax.nn.sigmoid(g) * v).astype(BF16)
            j += n
        if rest:
            s = halves(j, 2 * rest)
            h = s * jax.nn.sigmoid(s) * pltpu.roll(s, rest, 1)
            lane = lax.broadcasted_iota(jnp.int32, h.shape, 1)
            hidden[k, :, full * LANES : (full + 1) * LANES] = jnp.where(lane < rest, h, 0.0).astype(BF16)

    def up_step(k, _):
        with jax.named_scope("up"):
            up(k, False)
        return 0

    def up_late(k, _):
        with jax.named_scope("up_late"):
            up(k, True)
        return 0

    turn = (tp + z // 2) % 2
    quarter = PLANE * wide // 2

    def columns_of(j, mine):
        first, second = down[j // 2][0][1], down[j // 2][1][1]
        side = turn if mine else 1 - turn
        block = first * (1 - side) + second * side
        return block * 2 + (y if j % 2 == 0 else 1 - y)

    def place_of(j):
        return columns_of(j, True) % (half // quarter)

    def pair_hop(j, k):
        return hop(give.at[j, k], pair.at[j, k], sent.at[PAIR], got.at[AT_PAIR + j * LAYERS + k], core_target)

    def to_partner(j, k):
        landing = arrive.at[0, j] if k == 1 else joint.at[j, k - 2]
        group = NEAR if k == 1 else FAR
        return hop(paired.at[j, k], landing, sent.at[group], got.at[AT_BACK + j * LAYERS + k], line[1])

    def to_layer(j, k):
        return hop(joint.at[j, k], arrive.at[1, j], sent.at[FAR], got.at[AT_BACK + j * LAYERS], line[k + 2])

    def part_sums(*parts):
        for j, k in parts:
            given = span(columns_of(j, False), quarter)
            give[j, k] = jnp.dot(hidden[k], dn_all[:, given], preferred_element_type=F32).astype(BF16)
            pair_hop(j, k).start()
        for j, k in parts:
            kept = span(columns_of(j, True), quarter)
            keep = jnp.dot(hidden[k], dn_all[:, kept], preferred_element_type=F32)
            with jax.named_scope(f"pair{j}{k}"):
                pair_hop(j, k).wait_recv()
            paired[j, k] = (keep + pair[j, k].astype(F32)).astype(BF16)
            if k > 1:

                @pl.when(inner == 0)
                def _():
                    to_partner(j, k).start()

            elif k == 1:
                to_partner(j, 1).start()

    def joint_sums(j, k):
        @pl.when(inner == 1)
        def _():
            with jax.named_scope(f"joint{j}{k}"):
                to_partner(j, k + 2).wait_recv()
            joint[j, k] = (joint[j, k].astype(F32) + paired[j, k + 2].astype(F32)).astype(BF16)
            to_layer(j, k).start()

    corners_done(3, False)
    for block in down[0]:
        sides(4, *block, kinds=(2,))
    with jax.named_scope("across12"):
        core_hop(1).wait_recv()
        core_hop(2).wait_recv()
    lax.fori_loop(1, 3, up_early, 0)
    corners_done(3, True)
    lax.fori_loop(1, 3, up_late, 0)
    z_done(4, 3)
    for block in down[0]:
        corners(4, *block, kinds=(1,))
    part_sums((0, 2))
    corners(4, *down_a, kinds=(2,))
    part_sums((0, 1))
    corners(4, *down_b, kinds=(2,))
    for block in down[1]:
        sides(4, *block)

    @pl.when(inner == 0)
    def _():
        rows_arrived(3, 1, 3)

    with jax.named_scope("across3"):
        core_hop(3).wait_recv()
    lax.fori_loop(3, 4, up_step, 0)
    part_sums((0, 3))
    corners_done(4, False)
    part_sums((1, 2), (1, 1), (1, 3))
    joint_sums(0, 0)
    corners(4, *down[1][0])
    corners(4, *down[1][1], kinds=(1,))
    part_sums((2, 3), (2, 2), (2, 1))
    corners(4, *down[1][1], kinds=(2,))
    joint_sums(0, 1)
    joint_sums(1, 0)
    corners_done(4, True)
    part_sums((3, 2), (3, 3), (3, 1))
    joint_sums(1, 1)
    joint_sums(2, 1)
    lax.fori_loop(0, 1, up_step, 0)
    joint_sums(2, 0)
    part_sums((0, 0), (1, 0))
    joint_sums(3, 0)
    joint_sums(3, 1)
    part_sums((2, 0), (3, 0))

    stores = []
    for j in range(LAYERS):
        with jax.named_scope(f"near{j}"):
            to_partner(j, 1).wait_recv()
        with jax.named_scope(f"far{j}"):
            to_layer(j, 0).wait_recv()
        total = paired[j, 0].astype(F32) + arrive[0, j].astype(F32) + arrive[1, j].astype(F32)
        first = pl.multiple_of(tp * half + place_of(j) * quarter, quarter)
        out_v[j] = (after[:, pl.ds(first, quarter)].astype(F32) + total).astype(BF16)
        stores.append(pltpu.make_async_copy(out_v.at[j], out.at[:, span(place_of(j), quarter)], local.at[j]))
        stores[j].start()

    def all_sent(group, block):
        hop(block, block, sent.at[group], got.at[0], core_target).wait_send()

    with jax.named_scope("sent"):
        every = slice(None)
        all_sent(MIX, bo_all.at[pl.ds(0, 3 * N_SMALL * LAYERS * deep // 4), :])
        all_sent(UP, gu_all.at[pl.ds(0, 3 * LAYERS * deep), :])
        all_sent(DOWN, dn_all.at[pl.ds(0, units), pl.ds(0, 3 * LAYERS * wide)])
        all_sent(MIX_Z, bo_all.at[pl.ds(0, N_SMALL * deep // 2), :])
        all_sent(UP_Z, gu_all.at[pl.ds(0, 3 * deep), :])
        all_sent(DOWN_Z, dn_all.at[pl.ds(0, units), pl.ds(0, 3 * wide)])
        all_sent(ROWS, n2.at[pl.ds(0, 2)])
        all_sent(MISC, bo_all.at[pl.ds(0, MISC_QUARTERS * rows * half // bo_all.shape[1] // 4), :])
        all_sent(PAIR, give)
        all_sent(NEAR, arrive.at[0])
        all_sent(FAR, joint)

        @pl.when(inner == 1)
        def _():
            all_sent(MIX_RELAY, bo_all.at[pl.ds(0, LAYERS * N_SMALL * deep // 2), :])
            all_sent(ROWS_RELAY, n2.at[pl.ds(0, 2)])

    with jax.named_scope("stores"):
        for c in stores:
            c.wait()


def fused_layer(
    tokens,
    mixer_norm_gain,
    recurrence_branch_weight,
    output_gate_projection,
    recurrence_conv_taps,
    recurrence_gate_map,
    input_gate_map,
    channel_decay_rate,
    position_log_decay,
    mixer_output_weight,
    feedforward_norm_gain,
    gate_up_weight,
    value_up_weight,
    gate_conv_taps,
    value_conv_taps,
    down_projection_weight,
):
    rows, half = tokens.shape
    deep, local_width = recurrence_branch_weight.shape
    wide = mixer_output_weight.shape[1]
    n_fs = LAYERS * PLANE
    features = 2 * half
    local_units = gate_up_weight.shape[1]
    units = local_units // LAYERS
    padded = -(-units // (2 * LANES)) * 2 * LANES
    cw = local_width // 2
    quarter = PLANE * wide // 2
    dma = pltpu.SemaphoreType.DMA
    scratch = [
        pltpu.VMEM((2, rows, features), BF16),
        pltpu.VMEM((n_fs * deep, 2 * local_width), BF16),
        pltpu.VMEM((local_width, n_fs * wide), BF16),
        pltpu.VMEM((deep, local_units), BF16),
        pltpu.VMEM((deep, local_units), BF16),
        pltpu.VMEM((LAYERS, deep, 2 * units), BF16),
        pltpu.VMEM((n_fs * deep, 2 * units), BF16),
        pltpu.VMEM((padded, n_fs * wide), BF16),
        pltpu.VMEM((LAYERS, 8, 2 * units), F32),
        pltpu.VMEM((local_width // cw, cw, 2 * cw), BF16),
        pltpu.VMEM((2, rows, cw), F32),
        pltpu.VMEM((2, rows, features), BF16),
        pltpu.VMEM((2, rows, half), BF16),
        pltpu.VMEM((2, rows, half), F32),
        pltpu.VMEM((2, rows, half), BF16),
        pltpu.VMEM((rows, half), BF16),
        pltpu.VMEM((rows, half), BF16),
        pltpu.VMEM((rows, features), BF16),
        pltpu.VMEM((LAYERS, rows, features), BF16),
        pltpu.VMEM((LAYERS, rows, padded), BF16),
        pltpu.VMEM((LAYERS, LAYERS, rows, quarter), BF16),
        pltpu.VMEM((LAYERS, LAYERS, rows, quarter), BF16),
        pltpu.VMEM((LAYERS, LAYERS, rows, quarter), BF16),
        pltpu.VMEM((2, LAYERS, rows, quarter), BF16),
        pltpu.VMEM((LAYERS, 2, rows, quarter), BF16),
        pltpu.VMEM((LAYERS, rows, quarter), BF16),
        pltpu.VMEM((2, rows, 2 * units), F32),
        pltpu.VMEM((2, rows, cw), BF16),
        dma((N_SENT,)),
        dma((AT_BACK + LAYERS * LAYERS,)),
        dma((9,)),
    ]
    return pl.pallas_call(
        layer_kernel,
        out_shape=jax.ShapeDtypeStruct((rows, half), BF16),
        in_specs=[ANY, VMEM, ANY, ANY, VMEM, VMEM, VMEM, VMEM, ANY, ANY, VMEM, ANY, ANY, VMEM, VMEM, ANY],
        out_specs=ANY,
        scratch_shapes=scratch,
        compiler_params=pltpu.CompilerParams(
            collective_id=0, has_side_effects=True, vmem_limit_bytes=62 * 2**20
        ),
        name="layer",
    )(
        tokens,
        mixer_norm_gain,
        recurrence_branch_weight,
        output_gate_projection,
        recurrence_conv_taps,
        recurrence_gate_map,
        input_gate_map,
        channel_decay_rate.reshape(1, -1),
        position_log_decay,
        mixer_output_weight,
        feedforward_norm_gain,
        gate_up_weight,
        value_up_weight,
        gate_conv_taps,
        value_conv_taps,
        down_projection_weight,
    )


def solution(mesh):
    placed = (
        P("fs", "tp"),
        P(),
        P("fs", "tp"),
        P("fs", "tp"),
        P(None, "tp"),
        P("tp", None, None),
        P("tp", None, None),
        P("tp"),
        P("fs", "tp"),
        P("tp", "fs"),
        P(),
        P("fs", "tp"),
        P("fs", "tp"),
        P(None, "tp"),
        P(None, "tp"),
        P("tp", "fs"),
    )
    fused = mesh.shape["tp"] == 2 and mesh.shape["fs"] == LAYERS * PLANE
    body = fused_layer if fused else gathered_layer
    return jax.shard_map(
        body, mesh=mesh, in_specs=placed, out_specs=P("fs", "tp"), check_vma=False
    )
```
